256 devices in a mesh: sp: 64 (over z, y, core), tp: 4 (over x).
Axes of the slice: x: 4, y: 4, z: 8, core: 2. Of those that a mesh axis runs over, the one named last changes fastest.
Arguments:
- tokens: bfloat16 [4, 24576, 2048], P(None, 'sp'), may hold values from -21 to 21
- query_weight: bfloat16 [2048, 1024], P(None, 'tp'), may hold values from -0.125 to 0.125
- key_weight: bfloat16 [2048, 1024], P(None, 'tp'), may hold values from -0.125 to 0.125
- value_weight: bfloat16 [2048, 1024], P(None, 'tp'), may hold values from -0.125 to 0.125
- out_gain: float32 [1024], replicated, may hold values from 0.1 to 1.9
- out_weight: bfloat16 [1024, 2048], P(None, 'tp'), may hold values from -0.1875 to 0.1875
Outputs:
- mixed_out: bfloat16 [4, 24576, 2048], P(None, 'sp', 'tp')
- total_log: float32 [4, 8, 24576], P(None, 'tp', 'sp')
The draws below stay inside these ranges and needn't reach their ends.
All inputs are finite; a program needn't handle non-finite values.
Results may differ from the reference program's by a relative error of at most 0.0098.
Values may be sent and summed in bfloat16 or wider, within the bound.
A program may use at most 128 MiB of HBM per device.

```python
import jax
import jax.numpy as jnp
from jax import lax

D = 2048
HEADS = 8
HEAD_DIM = 128
REACH = 64
SEQS = 4
TOK_DEV = 384
TOKENS = 24576


def draw_tokens(key, part):
    dims = (SEQS, TOKENS, D)
    return jnp.clip(jax.random.normal(key, dims, jnp.float32), -6.0, 6.0).astype(jnp.bfloat16)


def block_levels(rng, shape, cuts, least, high):
    factor_of, own = 1.0, jax.random.fold_in(rng, 6)
    for axis_at, blocks in cuts:
        heights = jnp.exp(jax.random.uniform(jax.random.fold_in(own, axis_at), (blocks,), jnp.float32, least / len(cuts), high / len(cuts)))
        factor_of = factor_of * jnp.repeat(heights, shape[axis_at] // blocks).reshape([-1 if axis == axis_at else 1 for axis in range(len(shape))])
    return factor_of


def bell_draw(rng, shape, deviation, bound, cuts=(), kind=jnp.bfloat16):
    entries = jax.random.normal(rng, shape, jnp.float32) * deviation
    if len(cuts) > 0:
        entries = block_levels(rng, shape, cuts, -0.22, 0.18) * entries
    return jnp.clip(entries, min=-bound, max=bound).astype(kind)


def setup_inputs(seed: int = 0) -> dict:
    arg_keys = jax.random.split(jax.random.key(seed), 7)
    tokens = draw_tokens(jax.random.fold_in(arg_keys[6], 71), 0)
    query_weight = bell_draw(arg_keys[1], (D, HEADS * HEAD_DIM), D ** -0.5, 0.125, ((1, 4),))
    key_weight = bell_draw(arg_keys[2], (D, HEADS * HEAD_DIM), D ** -0.5, 0.125, ((1, 4),))
    value_weight = bell_draw(arg_keys[3], (D, HEADS * HEAD_DIM), D ** -0.5, 0.125, ((1, 4),))
    out_gain = jnp.clip(1.0 + 0.18 * jax.random.normal(arg_keys[4], (HEADS * HEAD_DIM,), jnp.float32), 0.1, 1.9)
    out_weight = bell_draw(arg_keys[5], (HEADS * HEAD_DIM, D), (HEADS * HEAD_DIM) ** -0.5, 0.1875, ((1, 4),))
    return {"tokens": tokens, "query_weight": query_weight, "key_weight": key_weight, "value_weight": value_weight, "out_gain": out_gain, "out_weight": out_weight}


DILATIONS = (1, 4, 16)
ROPE_BASE = 10000.0
MASK_FILL = -1e+30
NORM_FLOOR = 1e-06

def rotate(projected, positions):
    in_shape = projected.shape
    heads_view = projected.reshape(in_shape[0], in_shape[1], -1, HEAD_DIM)
    half_dim = HEAD_DIM // 2
    frequency = ROPE_BASE ** (-jnp.arange(half_dim, dtype=jnp.float32) / half_dim)
    angles = positions.astype(jnp.float32)[:, None] * frequency[None, :]
    cosine = jnp.cos(angles)[None, :, None, :]
    sine_part = jnp.sin(angles)[None, :, None, :]
    lower_half = heads_view[..., :half_dim]
    upper_half = heads_view[..., half_dim:]
    turned = jnp.concatenate([lower_half * cosine - upper_half * sine_part, upper_half * cosine + lower_half * sine_part], axis=-1)
    return turned.reshape(in_shape)

def band_attend(queries, extended, dilation, offset, total_len):
    seq_count, length, channels = queries.shape
    head_count = channels // HEAD_DIM
    reach_span = REACH * dilation
    query_rows = length // dilation
    key_rows = query_rows + 2 * REACH
    shaped_q = queries.reshape(seq_count, query_rows, dilation, head_count, HEAD_DIM).astype(jnp.float32)
    shaped_k = extended[:, :, :channels].reshape(seq_count, key_rows, dilation, head_count, HEAD_DIM).astype(jnp.float32)
    shaped_v = extended[:, :, channels:].reshape(seq_count, key_rows, dilation, head_count, HEAD_DIM).astype(jnp.float32)
    scores = jnp.einsum('sarhe,sbrhe->srhab', shaped_q, shaped_k)
    query_row = jnp.arange(query_rows, dtype=jnp.int32)[:, None]
    key_row = jnp.arange(key_rows, dtype=jnp.int32)[None, :]
    inband = (key_row >= query_row) & (key_row <= query_row + 2 * REACH)
    residue = jnp.arange(dilation, dtype=jnp.int32)[:, None, None]
    key_pos = offset - reach_span + key_row[None] * dilation + residue
    allowed = inband[None] & (key_pos >= 0) & (key_pos < total_len)
    scores = jnp.where(allowed[None, :, None], scores * HEAD_DIM ** (-0.5), MASK_FILL)
    maximum = lax.optimization_barrier(jnp.max(scores, axis=-1, keepdims=True))
    exp_scores = jnp.exp(scores - maximum)
    weight_sum = lax.optimization_barrier(jnp.sum(exp_scores, axis=-1, keepdims=True))
    probs = lax.optimization_barrier(exp_scores.astype(jnp.bfloat16)).astype(jnp.float32)
    branch = jnp.einsum('srhab,sbrhe->sarhe', probs, shaped_v)
    branch = branch / jnp.transpose(weight_sum, (0, 3, 1, 2, 4))
    branch = branch.reshape(seq_count, length, head_count, HEAD_DIM)
    log_sum = (maximum + jnp.log(weight_sum))[..., 0]
    log_sum = jnp.transpose(log_sum, (0, 2, 3, 1)).reshape(seq_count, head_count, length)
    return (branch, log_sum)

def combine(branch_out, branch_log):
    logs = jnp.stack(branch_log, 0)
    peak = lax.optimization_barrier(jnp.max(logs, axis=0))
    total_log = peak + jnp.log(lax.optimization_barrier(jnp.sum(jnp.exp(logs - peak[None]), axis=0)))
    shares = jnp.exp(logs - total_log[None])
    shares = jnp.transpose(shares, (0, 1, 3, 2))[..., None]
    merged = lax.optimization_barrier(jnp.sum(shares * jnp.stack(branch_out, 0), axis=0))
    seq_count, length, head_count, head_dim = merged.shape
    return (merged.reshape(seq_count, length, head_count * head_dim).astype(jnp.bfloat16), total_log)

def reference(tokens, query_weight, key_weight, value_weight, out_gain, out_weight):
    flat_rows = tokens.reshape(SEQS * TOKENS, D)
    positions = jnp.arange(TOKENS, dtype=jnp.int32)

    def project(weight):
        return jnp.dot(flat_rows, weight, preferred_element_type=jnp.float32).reshape(SEQS, TOKENS, -1)
    queries = rotate(project(query_weight), positions).astype(jnp.bfloat16)
    key_rows = rotate(project(key_weight), positions).astype(jnp.bfloat16)
    values = project(value_weight).astype(jnp.bfloat16)
    wide_span = REACH * DILATIONS[2]
    stacked = jnp.pad(jnp.concatenate([key_rows, values], axis=2), ((0, 0), (wide_span, wide_span), (0, 0)))

    def one_block(block_index):
        row_start = (block_index * TOK_DEV).astype(jnp.int32)
        block_q = lax.dynamic_slice_in_dim(queries, row_start, TOK_DEV, 1)
        branch_out = []
        branch_log = []
        for dilation in DILATIONS:
            reach_span = REACH * dilation
            extended = lax.dynamic_slice_in_dim(stacked, row_start + wide_span - reach_span, TOK_DEV + 2 * reach_span, 1)
            branch, log_sum = band_attend(block_q, extended, dilation, row_start, TOKENS)
            branch_out.append(branch)
            branch_log.append(log_sum)
        return combine(branch_out, branch_log)
    merged, total_log = lax.map(one_block, jnp.arange(TOKENS // TOK_DEV, dtype=jnp.int32))
    merged = jnp.transpose(merged, (1, 0, 2, 3)).reshape(SEQS, TOKENS, HEADS * HEAD_DIM)
    total_log = jnp.transpose(total_log, (1, 2, 0, 3)).reshape(SEQS, HEADS, TOKENS)
    lifted = merged.astype(jnp.float32)
    square = lax.optimization_barrier(jnp.mean(lifted * lifted, axis=-1))
    scaled = (lifted * out_gain.astype(jnp.float32)).astype(jnp.bfloat16)
    projected = jnp.dot(scaled.reshape(SEQS * TOKENS, HEADS * HEAD_DIM), out_weight, preferred_element_type=jnp.float32).reshape(SEQS, TOKENS, D)
    mixed_out = (projected * lax.rsqrt(square + NORM_FLOOR)[..., None]).astype(jnp.bfloat16)
    return (mixed_out, total_log)
```

```python
import functools

import jax
import jax.numpy as jnp
from jax import lax
from jax.experimental import pallas as pl
from jax.experimental.pallas import tpu as pltpu
from jax.sharding import PartitionSpec as P

HEAD_DIM = 128
REACH = 64
ROPE_BASE = 10000.0
MASK_FILL = -1e30
NORM_FLOOR = 1e-6
LOG2E = 1.4426950408889634
SCALE = HEAD_DIM ** (-0.5)
RATE = SCALE * LOG2E

TOK = 384
CHIP = 2 * TOK
BLK = 256
WIDE = 1024
HALO = WIDE // BLK
OWN = CHIP // BLK
NBLK = 2 * HALO + OWN
ROWS = NBLK * BLK
MESH = pl.DeviceIdType.MESH
F32 = jnp.float32
BF16 = jnp.bfloat16


def dot_nt(a, b):
    return lax.dot_general(a, b, (((1,), (1,)), ((), ())), preferred_element_type=F32)


def dot(a, b):
    return jnp.dot(a, b, preferred_element_type=F32)


def attend(queries, keys, values, bias):
    scores = dot_nt(queries, keys) + bias
    peak = jnp.max(scores, axis=-1, keepdims=True)
    probs = jnp.exp2((scores - peak) * RATE)
    total = jnp.sum(probs, axis=-1, keepdims=True)
    return dot(probs.astype(BF16), values), peak, total


def iota(shape, dim):
    return lax.broadcasted_iota(jnp.int32, shape, dim)


def kernel(chips, tps, seqs, tokens, wq, wk, wv, gain, wo, cos, sin, out, logs,
           tok_v, wq_v, wk_v, wv_v, wo_v, kvown, qown, kvbuf, qbuf, kvp, qp, perm,
           bias1, bias4, bias16, acc1, peak1, sum1, mperm, lperm, mnat, lnat, lrx, mg, out_v,
           in_sem, loc_sem, kv_send, kv_recv, x_send, x_recv, l_send, l_recv, x_loc, out_sem):
    sp, tp = lax.axis_index("sp"), lax.axis_index("tp")
    chip, core = sp // 2, sp % 2

    loads = [pltpu.make_async_copy(wk, wk_v, in_sem.at[0]),
             pltpu.make_async_copy(tokens.at[0], tok_v.at[0], in_sem.at[4]),
             pltpu.make_async_copy(wv, wv_v, in_sem.at[1]),
             pltpu.make_async_copy(wq, wq_v, in_sem.at[2])]
    for s in range(1, seqs):
        loads.append(pltpu.make_async_copy(tokens.at[s], tok_v.at[s], in_sem.at[4 + s]))
    loads.append(pltpu.make_async_copy(wo, wo_v, in_sem.at[3]))
    for load in loads:
        load.start()

    barrier = pltpu.get_barrier_semaphore()
    partners = [(2 * chip + 1 - core, tp)]
    for step in (1, -1, 2, -2):
        for c in range(2):
            partners.append((2 * ((chip + chips + step) % chips) + c, tp))
    for dx in range(1, tps):
        for c in range(2):
            partners.append((2 * chip + c, (tp + dx) % tps))
    for partner in partners:
        pl.semaphore_signal(barrier, inc=1, device_id=partner, device_id_type=MESH)

    def row_of(at, size):
        return pl.ds(pl.multiple_of(at, 128), size)

    def remote(src, dst, send, recv, device):
        return pltpu.make_async_remote_copy(src_ref=src, dst_ref=dst, send_sem=send, recv_sem=recv,
                                            device_id=device, device_id_type=MESH)

    def kv_sends(s):
        after, before = (chip + 1) % chips, (chip + chips - 1) % chips
        far = (chip + chips + 4 * core - 2) % chips
        copies = []
        for h in range(2):
            copies.append(remote(kvown.at[s, h], kvbuf.at[s, row_of(BLK + TOK * core, TOK)],
                                 kv_send.at[s, h], kv_recv.at[s, 1 + core], (2 * after + h, tp)))
            copies.append(remote(kvown.at[s, h], kvbuf.at[s, row_of(WIDE + CHIP + TOK * core, TOK)],
                                 kv_send.at[s, 2 + h], kv_recv.at[s, 3 + core], (2 * before + h, tp)))
        for h in range(2):
            copies.append(remote(kvown.at[s, h, row_of(128 * core, BLK)],
                                 kvbuf.at[s, row_of((ROWS - BLK) * (1 - core), BLK)],
                                 kv_send.at[s, 4 + h], kv_recv.at[s, 6 - core], (2 * far + h, tp)))
        copies.append(remote(kvown.at[s, 1 - core], kvbuf.at[s, row_of(WIDE + TOK * core, TOK)],
                             kv_send.at[s, 6], kv_recv.at[s, 0], (2 * chip + 1 - core, tp)))
        return copies

    def q_send(s):
        return remote(qown.at[s, 1 - core], qbuf.at[s, row_of(TOK * core, TOK)],
                      kv_send.at[s, 7], kv_recv.at[s, 7], (2 * chip + 1 - core, tp))

    def local_copies(s):
        return [pltpu.make_async_copy(kvown.at[s, core], kvbuf.at[s, row_of(WIDE + TOK * core, TOK)], loc_sem.at[s, 0]),
                pltpu.make_async_copy(qown.at[s, core], qbuf.at[s, row_of(TOK * core, TOK)], loc_sem.at[s, 1])]

    def kv_arrivals(s):
        starts = [(WIDE + TOK * (1 - core), TOK), (BLK, TOK), (BLK + TOK, TOK),
                  (WIDE + CHIP, TOK), (WIDE + CHIP + TOK, TOK), (0, BLK), (ROWS - BLK, BLK)]
        waits = [remote(kvown.at[s, 0, pl.ds(0, size)], kvbuf.at[s, row_of(at, size)], kv_send.at[s, 0],
                        kv_recv.at[s, i], (2 * chip + 1 - core, tp)) for i, (at, size) in enumerate(starts)]
        waits.append(remote(qown.at[s, 0], qbuf.at[s, row_of(TOK * (1 - core), TOK)], kv_send.at[s, 0],
                            kv_recv.at[s, 7], (2 * chip + 1 - core, tp)))
        return waits

    head = 2 * tp + core

    def column_of(h):
        return pl.ds(pl.multiple_of(h * HEAD_DIM, HEAD_DIM), HEAD_DIM)

    def x_sends(s):
        copies = []
        for dx in range(1, tps):
            for c in range(2):
                copies.append(remote(mnat.at[s, pl.ds(TOK * c, TOK)], mg.at[s, :, column_of(head)],
                                     x_send.at[s, 2 * dx + c], x_recv.at[s, head], (2 * chip + c, (tp + dx) % tps)))
        copies.append(remote(mnat.at[s, row_of(TOK * (1 - core), TOK)], mg.at[s, :, column_of(head)],
                             x_send.at[s, 0], x_recv.at[s, head], (2 * chip + 1 - core, tp)))
        copies.append(remote(lnat.at[s, 1 - core], lrx.at[s], l_send.at[s], l_recv.at[s], (2 * chip + 1 - core, tp)))
        return copies

    def x_local(s):
        return pltpu.make_async_copy(mnat.at[s, row_of(TOK * core, TOK)], mg.at[s, :, column_of(head)], x_loc.at[s])

    def x_arrivals(s):
        waits = []
        for o in range(1, 2 * tps):
            other = (head + o) % (2 * tps)
            waits.append(remote(mnat.at[s, pl.ds(0, TOK)], mg.at[s, :, column_of(other)], x_send.at[s, 0],
                                x_recv.at[s, other], (2 * chip + 1 - core, tp)))
        waits.append(remote(lnat.at[s, 0], lrx.at[s], l_send.at[s], l_recv.at[s], (2 * chip + 1 - core, tp)))
        return waits

    row, col = iota((BLK, BLK), 0), iota((BLK, BLK), 1)
    perm[...] = jnp.where(col == (row % 16) * 16 + row // 16, 1.0, 0.0).astype(BF16)
    first = chip * CHIP
    limit = chips * CHIP
    for b in range(OWN):
        row, col = iota((BLK, BLK + 2 * REACH), 0), iota((BLK, BLK + 2 * REACH), 1)
        gap = (row % 16) * 16 + row // 16 - (col - REACH)
        at = first + b * BLK - REACH + col
        good = (gap >= -REACH) & (gap <= REACH) & (at >= 0) & (at < limit)
        bias1[b] = jnp.where(good, 0.0, MASK_FILL)
        row, col = iota((64, 192), 0), iota((64, 192), 1)
        gap = (row % 16) * 4 + row // 16 - ((col // 64 - 1) * 64 + (col % 16) * 4 + (col % 64) // 16)
        at = first + (b + col // 64 - 1) * BLK
        good = (gap >= -REACH) & (gap <= REACH) & (at >= 0) & (at < limit)
        bias4[b] = jnp.where(good, 0.0, MASK_FILL)
    row, col = iota((16 * OWN, 16 * NBLK), 0), iota((16 * OWN, 16 * NBLK), 1)
    gap = row - (col - 16 * HALO)
    at = first + (col // 16 - HALO) * BLK
    good = (gap >= -REACH) & (gap <= REACH) & (at >= 0) & (at < limit)
    bias16[...] = jnp.where(good, 0.0, MASK_FILL)

    def turned(x):
        return (x * cos[...] + pltpu.roll(x, HEAD_DIM // 2, 1) * sin[...]).astype(BF16)

    def project(s, _):
        pltpu.make_async_copy(tokens.at[s], tok_v.at[s], in_sem.at[4 + s]).wait()

        @pl.when(s == 0)
        def _():
            loads[0].wait()
        keys = dot(tok_v[s], wk_v[...])
        for h in range(2):
            kvown[s, h, :, :HEAD_DIM] = turned(keys[:, h * HEAD_DIM:(h + 1) * HEAD_DIM])

        @pl.when(s == 0)
        def _():
            loads[2].wait()
        values = dot(tok_v[s], wv_v[...])
        for h in range(2):
            kvown[s, h, :, HEAD_DIM:] = values[:, h * HEAD_DIM:(h + 1) * HEAD_DIM].astype(BF16)

        @pl.when(s == 0)
        def _():
            pl.semaphore_wait(barrier, len(partners))
        for copy in kv_sends(s):
            copy.start()
        local_copies(s)[0].start()

        @pl.when(s == 0)
        def _():
            loads[3].wait()
        queries = dot(tok_v[s], wq_v[...])
        for h in range(2):
            qown[s, h] = turned(queries[:, h * HEAD_DIM:(h + 1) * HEAD_DIM])
        q_send(s).start()
        local_copies(s)[1].start()
        return 0

    lax.fori_loop(0, seqs, project, 0)
    loads[-1].wait()

    def attention(s):
        for copy in local_copies(s):
            copy.wait()
        for copy in kv_arrivals(s):
            copy.wait_recv()

        def put_in_order(b, _):
            block = kvbuf[s, pl.ds(pl.multiple_of(b * BLK, BLK), BLK), :]
            kvp[b] = dot(perm[...], block).astype(BF16).reshape(4, 4, 16, 2 * HEAD_DIM)
            return 0
        lax.fori_loop(0, NBLK, put_in_order, 0)
        for b in range(OWN):
            block = dot(perm[...], qbuf[s, pl.ds(b * BLK, BLK), :]).astype(BF16)
            qp[b] = block.reshape(4, 4, 16, HEAD_DIM)
            near = pl.ds(WIDE + b * BLK - REACH, BLK + 2 * REACH)
            acc, peak, total = attend(block, kvbuf[s, near, :HEAD_DIM], kvbuf[s, near, HEAD_DIM:], bias1[b])
            acc1[b] = acc.reshape(4, 4, 16, HEAD_DIM)
            peak1[b] = jnp.broadcast_to(peak, (BLK, HEAD_DIM)).reshape(4, 4, 16, HEAD_DIM)
            sum1[b] = jnp.broadcast_to(total, (BLK, HEAD_DIM)).reshape(4, 4, 16, HEAD_DIM)

        def residue(r, _):
            middle = []
            for b in range(OWN):
                keys = kvp[b + HALO - 1:b + HALO + 2, :, r, :, :HEAD_DIM].reshape(192, HEAD_DIM)
                values = kvp[b + HALO - 1:b + HALO + 2, :, r, :, HEAD_DIM:].reshape(192, HEAD_DIM)
                middle.append(attend(qp[b, :, r].reshape(64, HEAD_DIM), keys, values, bias4[b]))
            for a in range(4):
                keys = kvp[:, a, r, :, :HEAD_DIM].reshape(16 * NBLK, HEAD_DIM)
                values = kvp[:, a, r, :, HEAD_DIM:].reshape(16 * NBLK, HEAD_DIM)
                wide = attend(qp[:, a, r].reshape(16 * OWN, HEAD_DIM), keys, values, bias16[...])
                for b in range(OWN):
                    near = (acc1[b, a, r], peak1[b, a, r], sum1[b, a, r])
                    mid = tuple(x[a * 16:(a + 1) * 16] for x in middle[b])
                    far = tuple(x[b * 16:(b + 1) * 16] for x in wide)
                    peak = jnp.maximum(jnp.maximum(near[1], mid[1]), far[1])
                    merged, total = 0.0, 0.0
                    for acc_g, peak_g, sum_g in (near, mid, far):
                        share = jnp.exp2((peak_g - peak) * RATE)
                        merged = merged + share * acc_g
                        total = total + share * sum_g
                    mperm[b, a, r] = (merged / total).astype(BF16)
                    lperm[b, a, r] = peak * SCALE + jnp.log(total)
            return 0
        lax.fori_loop(0, 4, residue, 0)
        for b in range(OWN):
            block = dot(perm[...], mperm[b].reshape(BLK, HEAD_DIM)).astype(BF16)
            mnat[s, pl.ds(b * BLK, BLK), :] = block
            column = lperm[b].reshape(BLK, HEAD_DIM)
            for half in range(2):
                hit = perm[:, half * 128:(half + 1) * 128].astype(F32)
                line = jnp.sum(jnp.where(hit > 0.5, column, 0.0), axis=0, keepdims=True)
                piece = 2 * b + half
                lnat[s, piece // 3, piece % 3:piece % 3 + 1, :] = line
        for copy in x_sends(s):
            copy.start()
        x_local(s).start()

    def finish(s):
        x_local(s).wait()
        for copy in x_arrivals(s):
            copy.wait_recv()
        lifted = mg[s].astype(F32)
        square = jnp.mean(lifted * lifted, axis=-1, keepdims=True)
        scaled = (lifted * gain[...]).astype(BF16)
        projected = dot(scaled, wo_v[...])
        out_v[s] = (projected * lax.rsqrt(square + NORM_FLOOR)).astype(BF16)
        pltpu.make_async_copy(out_v.at[s], out.at[s], out_sem.at[s]).start()
        mine, theirs = lnat[s, core], lrx[s]
        upper = jnp.where(core == 0, mine, theirs)
        lower = jnp.where(core == 0, theirs, mine)
        for piece in range(3):
            lanes = pl.ds(piece * 128, 128)
            logs[s, 0:1, lanes] = upper[piece:piece + 1]
            logs[s, 1:2, lanes] = lower[piece:piece + 1]

    def stage(s, _):
        attention(s)

        @pl.when(s > 0)
        def _():
            finish(s - 1)
        return 0

    lax.fori_loop(0, seqs, stage, 0)
    finish(seqs - 1)

    def drain(s, _):
        for copy in kv_sends(s):
            copy.wait_send()
        q_send(s).wait_send()
        for copy in x_sends(s):
            copy.wait_send()
        pltpu.make_async_copy(out_v.at[s], out.at[s], out_sem.at[s]).wait()
        return 0
    lax.fori_loop(0, seqs, drain, 0)


def shards(chips, tps, tokens, query_weight, key_weight, value_weight, out_gain, out_weight):
    seqs, length, model_dim = tokens.shape
    channels, out_cols = out_weight.shape
    positions = lax.axis_index("sp") * length + jnp.arange(length, dtype=jnp.int32)
    half_dim = HEAD_DIM // 2
    frequency = ROPE_BASE ** (-jnp.arange(half_dim, dtype=F32) / half_dim)
    angles = positions.astype(F32)[:, None] * frequency[None, :]
    cosine, sine = jnp.cos(angles), jnp.sin(angles)
    cosine = jnp.concatenate([cosine, cosine], axis=1)
    sine = jnp.concatenate([-sine, sine], axis=1)
    any_spec = pl.BlockSpec(memory_space=pl.ANY)
    vmem = pl.BlockSpec(memory_space=pltpu.VMEM)
    dma = pltpu.SemaphoreType.DMA
    grid4 = (OWN, 4, 4, 16, HEAD_DIM)
    return pl.pallas_call(
        functools.partial(kernel, chips, tps, seqs),
        out_shape=(jax.ShapeDtypeStruct((seqs, length, out_cols), BF16),
                   jax.ShapeDtypeStruct((seqs, 2, length), F32)),
        in_specs=[any_spec, any_spec, any_spec, any_spec, vmem, any_spec, vmem, vmem],
        out_specs=(any_spec, vmem),
        scratch_shapes=[
            pltpu.VMEM((seqs, TOK, model_dim), BF16),
            pltpu.VMEM((model_dim, 256), BF16),
            pltpu.VMEM((model_dim, 256), BF16),
            pltpu.VMEM((model_dim, 256), BF16),
            pltpu.VMEM((channels, out_cols), BF16),
            pltpu.VMEM((seqs, 2, TOK, 256), BF16),
            pltpu.VMEM((seqs, 2, TOK, 128), BF16),
            pltpu.VMEM((seqs, ROWS, 256), BF16),
            pltpu.VMEM((seqs, CHIP, 128), BF16),
            pltpu.VMEM((NBLK, 4, 4, 16, 256), BF16),
            pltpu.VMEM(grid4, BF16),
            pltpu.VMEM((BLK, BLK), BF16),
            pltpu.VMEM((OWN, BLK, BLK + 2 * REACH), F32),
            pltpu.VMEM((OWN, 64, 192), F32),
            pltpu.VMEM((16 * OWN, 16 * NBLK), F32),
            pltpu.VMEM(grid4, F32),
            pltpu.VMEM(grid4, F32),
            pltpu.VMEM(grid4, F32),
            pltpu.VMEM(grid4, BF16),
            pltpu.VMEM(grid4, F32),
            pltpu.VMEM((seqs, CHIP, 128), BF16),
            pltpu.VMEM((seqs, 2, 3, 128), F32),
            pltpu.VMEM((seqs, 3, 128), F32),
            pltpu.VMEM((seqs, TOK, channels), BF16),
            pltpu.VMEM((seqs, TOK, out_cols), BF16),
            dma((4 + seqs,)),
            dma((seqs, 2)),
            dma((seqs, 8)),
            dma((seqs, 8)),
            dma((seqs, 8)),
            dma((seqs, 8)),
            dma((seqs,)),
            dma((seqs,)),
            dma((seqs,)),
            dma((seqs,)),
        ],
        compiler_params=pltpu.CompilerParams(
            collective_id=0, has_side_effects=True, vmem_limit_bytes=60 * 1024 * 1024
        ),
    )(tokens, query_weight, key_weight, value_weight, out_gain.reshape(1, channels), out_weight, cosine, sine)


def solution(mesh):
    return jax.shard_map(
        functools.partial(shards, mesh.shape["sp"] // 2, mesh.shape["tp"]),
        mesh=mesh,
        in_specs=(
            P(None, "sp", None),
            P(None, "tp"),
            P(None, "tp"),
            P(None, "tp"),
            P(),
            P(None, "tp"),
        ),
        out_specs=(P(None, "sp", "tp"), P(None, "tp", "sp")),
        check_vma=False,
    )
```

```python
import functools

import jax
import jax.numpy as jnp
from jax import lax
from jax.experimental import pallas as pl
from jax.experimental.pallas import tpu as pltpu
from jax.sharding import PartitionSpec as P

HEAD_DIM = 128
REACH = 64
ROPE_BASE = 10000.0
MASK_FILL = -1e30
NORM_FLOOR = 1e-6
LOG2E = 1.4426950408889634
SCALE = HEAD_DIM ** (-0.5)
RATE = SCALE * LOG2E

TOK = 384
CHIP = 2 * TOK
BLK = 256
WIDE = 1024
HALO = WIDE // BLK
OWN = CHIP // BLK
NBLK = 2 * HALO + OWN
ROWS = NBLK * BLK
MESH = pl.DeviceIdType.MESH
F32 = jnp.float32
BF16 = jnp.bfloat16


def dot_nt(a, b):
    return lax.dot_general(a, b, (((1,), (1,)), ((), ())), preferred_element_type=F32)


def dot(a, b):
    return jnp.dot(a, b, preferred_element_type=F32)


def softened(scores):
    peak = jnp.max(scores, axis=-1, keepdims=True)
    probs = jnp.exp2((scores - peak) * RATE)
    return probs.astype(BF16), peak, jnp.sum(probs, axis=-1, keepdims=True)


def pipelined(jobs):
    ahead = jobs[0][0]()
    for i, (_, finish) in enumerate(jobs):
        now = ahead
        if i + 1 < len(jobs):
            ahead = jobs[i + 1][0]()
        finish(now)


def joined(parts):
    peak = functools.reduce(jnp.maximum, [part[1] for part in parts])
    merged, total = 0.0, 0.0
    for acc_g, peak_g, sum_g in parts:
        share = jnp.exp2((peak_g - peak) * RATE)
        merged = merged + share * acc_g
        total = total + share * sum_g
    return merged, peak, total


def iota(shape, dim):
    return lax.broadcasted_iota(jnp.int32, shape, dim)


def kernel(chips, tps, seqs, tokens, wq, wk, wv, gain, wo, cos, sin, out, logs,
           tok_v, wq_v, wk_v, wv_v, wo_v, kvown, qown, kvbuf, qbuf, kvp, qp, perm,
           bias1, bias4, bias16, acc1, peak1, sum1, mperm, lperm, mnat, lnat, lrx, mg, out_v,
           in_sem, loc_sem, kv_send, kv_recv, x_send, x_recv, l_send, l_recv, x_loc, out_sem):
    sp, tp = lax.axis_index("sp"), lax.axis_index("tp")
    chip, core = sp // 2, sp % 2

    loads = [pltpu.make_async_copy(wk, wk_v, in_sem.at[0]),
             pltpu.make_async_copy(tokens.at[0], tok_v.at[0], in_sem.at[4]),
             pltpu.make_async_copy(wv, wv_v, in_sem.at[1]),
             pltpu.make_async_copy(wq, wq_v, in_sem.at[2])]
    for s in range(1, seqs):
        loads.append(pltpu.make_async_copy(tokens.at[s], tok_v.at[s], in_sem.at[4 + s]))
    loads.append(pltpu.make_async_copy(wo, wo_v, in_sem.at[3]))
    for load in loads:
        load.start()

    barrier = pltpu.get_barrier_semaphore()
    partners = [(2 * chip + 1 - core, tp)]
    for step in (1, -1):
        for c in range(2):
            partners.append((2 * ((chip + chips + step) % chips) + c, tp))
    for dx in range(1, tps):
        for c in range(2):
            partners.append((2 * chip + c, (tp + dx) % tps))
    for partner in partners:
        pl.semaphore_signal(barrier, inc=1, device_id=partner, device_id_type=MESH)

    def row_of(at, size):
        return pl.ds(pl.multiple_of(at, 128), size)

    def remote(src, dst, send, recv, device):
        return pltpu.make_async_remote_copy(src_ref=src, dst_ref=dst, send_sem=send, recv_sem=recv,
                                            device_id=device, device_id_type=MESH)

    after, before = (chip + 1) % chips, (chip + chips - 1) % chips

    def near_sends(s):
        copies = []
        for piece, (src, at, size) in enumerate(((128 * core, 512 * core, BLK), (BLK * (1 - core), BLK + 128 * core, 128))):
            for h in range(2):
                for way, (base, to) in enumerate(((BLK, after), (WIDE + CHIP, before))):
                    copies.append(remote(kvown.at[s, h, row_of(src, size)], kvbuf.at[s, row_of(base + at, size)],
                                         kv_send.at[s, 4 * piece + 2 * h + way],
                                         kv_recv.at[s, 4 * way + 2 * piece + core], (2 * to + h, tp)))
        return copies

    def far_sends(s):
        return [remote(kvbuf.at[s, pl.ds(WIDE - BLK, BLK)], kvbuf.at[s, pl.ds(0, BLK)],
                       kv_send.at[s, 8], kv_recv.at[s, 8], (2 * after + core, tp)),
                remote(kvbuf.at[s, pl.ds(WIDE + CHIP, BLK)], kvbuf.at[s, pl.ds(ROWS - BLK, BLK)],
                       kv_send.at[s, 9], kv_recv.at[s, 9], (2 * before + core, tp))]

    def own_sends(s):
        return [remote(kvown.at[s, 1 - core], kvbuf.at[s, row_of(WIDE + TOK * core, TOK)],
                       kv_send.at[s, 10], kv_recv.at[s, 10], (2 * chip + 1 - core, tp)),
                remote(qown.at[s, 1 - core], qbuf.at[s, row_of(TOK * core, TOK)],
                       kv_send.at[s, 11], kv_recv.at[s, 11], (2 * chip + 1 - core, tp))]

    def local_copies(s):
        return [pltpu.make_async_copy(kvown.at[s, core], kvbuf.at[s, row_of(WIDE + TOK * core, TOK)], loc_sem.at[s, 0]),
                pltpu.make_async_copy(qown.at[s, core], qbuf.at[s, row_of(TOK * core, TOK)], loc_sem.at[s, 1])]

    def near_arrival(s, way, piece, c):
        at, size = ((512 * c, BLK), (BLK + 128 * c, 128))[piece]
        at += (BLK, WIDE + CHIP)[way]
        return remote(kvown.at[s, 0, pl.ds(0, size)], kvbuf.at[s, pl.ds(at, size)], kv_send.at[s, 0],
                      kv_recv.at[s, 4 * way + 2 * piece + c], (2 * chip + 1 - core, tp))

    def own_arrivals(s):
        return [remote(kvown.at[s, 0], kvbuf.at[s, row_of(WIDE + TOK * (1 - core), TOK)], kv_send.at[s, 0],
                       kv_recv.at[s, 10], (2 * chip + 1 - core, tp)),
                remote(qown.at[s, 0], qbuf.at[s, row_of(TOK * (1 - core), TOK)], kv_send.at[s, 0],
                       kv_recv.at[s, 11], (2 * chip + 1 - core, tp))]

    head = 2 * tp + core

    def column_of(h):
        return pl.ds(pl.multiple_of(h * HEAD_DIM, HEAD_DIM), HEAD_DIM)

    def x_sends(s):
        copies = []
        for dx in range(1, tps):
            for c in range(2):
                copies.append(remote(mnat.at[s, pl.ds(TOK * c, TOK)], mg.at[s, :, column_of(head)],
                                     x_send.at[s, 2 * dx + c], x_recv.at[s, head], (2 * chip + c, (tp + dx) % tps)))
        copies.append(remote(mnat.at[s, row_of(TOK * (1 - core), TOK)], mg.at[s, :, column_of(head)],
                             x_send.at[s, 0], x_recv.at[s, head], (2 * chip + 1 - core, tp)))
        copies.append(remote(lnat.at[s, 1 - core], lrx.at[s], l_send.at[s], l_recv.at[s], (2 * chip + 1 - core, tp)))
        return copies

    def x_local(s):
        return pltpu.make_async_copy(mnat.at[s, row_of(TOK * core, TOK)], mg.at[s, :, column_of(head)], x_loc.at[s])

    def x_arrivals(s):
        waits = []
        for o in range(1, 2 * tps):
            other = (head + o) % (2 * tps)
            waits.append(remote(mnat.at[s, pl.ds(0, TOK)], mg.at[s, :, column_of(other)], x_send.at[s, 0],
                                x_recv.at[s, other], (2 * chip + 1 - core, tp)))
        waits.append(remote(lnat.at[s, 0], lrx.at[s], l_send.at[s], l_recv.at[s], (2 * chip + 1 - core, tp)))
        return waits

    def turned(x):
        return (x * cos[...] + pltpu.roll(x, HEAD_DIM // 2, 1) * sin[...]).astype(BF16)

    def project(s, _):
        pltpu.make_async_copy(tokens.at[s], tok_v.at[s], in_sem.at[4 + s]).wait()

        @pl.when(s == 0)
        def _():
            loads[0].wait()
        keys = dot(tok_v[s], wk_v[...])
        for h in range(2):
            kvown[s, h, :, :HEAD_DIM] = turned(keys[:, h * HEAD_DIM:(h + 1) * HEAD_DIM])

        @pl.when(s == 0)
        def _():
            loads[2].wait()
        values = dot(tok_v[s], wv_v[...])
        for h in range(2):
            kvown[s, h, :, HEAD_DIM:] = values[:, h * HEAD_DIM:(h + 1) * HEAD_DIM].astype(BF16)

        @pl.when(s == 0)
        def _():
            pl.semaphore_wait(barrier, len(partners))
            for copy in near_sends(0):
                copy.start()
        own_sends(s)[0].start()
        local_copies(s)[0].start()

        @pl.when(s == 0)
        def _():
            loads[3].wait()
        queries = dot(tok_v[s], wq_v[...])
        for h in range(2):
            qown[s, h] = turned(queries[:, h * HEAD_DIM:(h + 1) * HEAD_DIM])
        own_sends(s)[1].start()
        local_copies(s)[1].start()
        return 0

    lax.fori_loop(0, seqs, project, 0)
    loads[-1].wait()

    row, col = iota((BLK, BLK), 0), iota((BLK, BLK), 1)
    perm[...] = jnp.where(col == (row % 16) * 16 + row // 16, 1.0, 0.0).astype(BF16)
    first = chip * CHIP
    limit = chips * CHIP
    for b in range(OWN):
        row, col = iota((BLK, BLK + 2 * REACH), 0), iota((BLK, BLK + 2 * REACH), 1)
        gap = (row % 16) * 16 + row // 16 - (col - REACH)
        at = first + b * BLK - REACH + col
        good = (gap >= -REACH) & (gap <= REACH) & (at >= 0) & (at < limit)
        bias1[b] = jnp.where(good, 0.0, MASK_FILL)
        row, col = iota((64, 192), 0), iota((64, 192), 1)
        gap = (row % 16) * 4 + row // 16 - ((col // 64 - 1) * 64 + (col % 16) * 4 + (col % 64) // 16)
        at = first + (b + col // 64 - 1) * BLK
        good = (gap >= -REACH) & (gap <= REACH) & (at >= 0) & (at < limit)
        bias4[b] = jnp.where(good, 0.0, MASK_FILL)
    row, col = iota((16 * OWN, 16 * NBLK), 0), iota((16 * OWN, 16 * NBLK), 1)
    gap = row - (col - 16 * HALO)
    at = first + (col // 16 - HALO) * BLK
    good = (gap >= -REACH) & (gap <= REACH) & (at >= 0) & (at < limit)
    bias16[...] = jnp.where(good, 0.0, MASK_FILL)


    def put_in_order(s, blocks):
        for b in blocks:
            kvp[b] = dot(perm[...], kvbuf[s, pl.ds(b * BLK, BLK), :]).astype(BF16).reshape(4, 4, 16, 2 * HEAD_DIM)

    def near(s):
        for b in range(OWN):
            block = dot(perm[...], qbuf[s, pl.ds(b * BLK, BLK), :]).astype(BF16)
            qp[b] = block.reshape(4, 4, 16, HEAD_DIM)
        put_in_order(s, range(1, NBLK - 1))
        jobs, done = [], {}

        def narrow(b, half):
            around = pl.ds(WIDE + b * BLK - REACH, BLK + 2 * REACH)

            def scores():
                queries = qp[b, 2 * half:2 * half + 2].reshape(128, HEAD_DIM)
                return dot_nt(queries, kvbuf[s, around, :HEAD_DIM]) + bias1[b, half * 128:(half + 1) * 128]

            def finish(scores):
                probs, peak, total = softened(scores)
                done[b, half] = dot(probs, kvbuf[s, around, HEAD_DIM:]), peak, total
            return scores, finish

        def middle(b):
            def scores():
                every = []
                for r in range(4):
                    keys = kvp[b + HALO - 1:b + HALO + 2, :, r, :, :HEAD_DIM].reshape(192, HEAD_DIM)
                    every.append(dot_nt(qp[b, :, r].reshape(64, HEAD_DIM), keys) + bias4[b])
                return every

            def finish(every):
                soft = [softened(scores) for scores in every]
                accs = []
                for r in range(4):
                    values = kvp[b + HALO - 1:b + HALO + 2, :, r, :, HEAD_DIM:].reshape(192, HEAD_DIM)
                    accs.append(dot(soft[r][0], values))
                for a in range(4):
                    for r in range(4):
                        at = (a % 2) * 64 + r * 16
                        one = tuple(x[at:at + 16] for x in done[b, a // 2])
                        two = tuple(x[a * 16:(a + 1) * 16] for x in (accs[r],) + soft[r][1:])
                        acc, peak, total = joined((one, two))
                        acc1[b, a, r] = acc
                        peak1[b, a, r] = jnp.broadcast_to(peak, (16, HEAD_DIM))
                        sum1[b, a, r] = jnp.broadcast_to(total, (16, HEAD_DIM))
            return scores, finish

        for b in range(OWN):
            jobs += [narrow(b, 0), narrow(b, 1), middle(b)]
        pipelined(jobs)

    def far(s):
        put_in_order(s, (0, NBLK - 1))

        def wide(r):
            def scores():
                every = []
                for a in range(4):
                    keys = kvp[:, a, r, :, :HEAD_DIM].reshape(16 * NBLK, HEAD_DIM)
                    every.append(dot_nt(qp[:, a, r].reshape(16 * OWN, HEAD_DIM), keys) + bias16[...])
                return every

            def finish(every):
                soft = [softened(scores) for scores in every]
                accs = []
                for a in range(4):
                    values = kvp[:, a, r, :, HEAD_DIM:].reshape(16 * NBLK, HEAD_DIM)
                    accs.append(dot(soft[a][0], values))
                for a in range(4):
                    for b in range(OWN):
                        one = (acc1[b, a, r], peak1[b, a, r], sum1[b, a, r])
                        two = tuple(x[b * 16:(b + 1) * 16] for x in (accs[a],) + soft[a][1:])
                        merged, peak, total = joined((one, two))
                        mperm[b, a, r] = (merged / total).astype(BF16)
                        lperm[b, a, r] = peak * SCALE + jnp.log(total)
            return scores, finish

        pipelined([wide(r) for r in range(4)])
        for b in range(OWN):
            mnat[s, pl.ds(b * BLK, BLK), :] = dot(perm[...], mperm[b].reshape(BLK, HEAD_DIM)).astype(BF16)
        for copy in x_sends(s)[:-1]:
            copy.start()
        x_local(s).start()
        for b in range(OWN):
            column = lperm[b].reshape(BLK, HEAD_DIM)
            for half in range(2):
                hit = perm[:, half * 128:(half + 1) * 128].astype(F32)
                line = jnp.sum(jnp.where(hit > 0.5, column, 0.0), axis=0, keepdims=True)
                piece = 2 * b + half
                lnat[s, piece // 3, piece % 3:piece % 3 + 1, :] = line
        x_sends(s)[-1].start()

    def finish(s):
        x_local(s).wait()
        for copy in x_arrivals(s):
            copy.wait_recv()
        lifted = mg[s].astype(F32)
        square = jnp.mean(lifted * lifted, axis=-1, keepdims=True)
        scaled = (lifted * gain[...]).astype(BF16)
        projected = dot(scaled, wo_v[...])
        out_v[s] = (projected * lax.rsqrt(square + NORM_FLOOR)).astype(BF16)
        pltpu.make_async_copy(out_v.at[s], out.at[s], out_sem.at[s]).start()
        mine, theirs = lnat[s, core], lrx[s]
        upper = jnp.where(core == 0, mine, theirs)
        lower = jnp.where(core == 0, theirs, mine)
        for piece in range(3):
            lanes = pl.ds(piece * 128, 128)
            logs[s, 0:1, lanes] = upper[piece:piece + 1]
            logs[s, 1:2, lanes] = lower[piece:piece + 1]

    def stage(s, _):
        near_arrival(s, 0, 0, 1).wait_recv()
        near_arrival(s, 1, 0, 0).wait_recv()
        for copy in far_sends(s):
            copy.start()

        @pl.when(s + 1 < seqs)
        def _():
            for copy in near_sends(s + 1):
                copy.start()

        for copy in local_copies(s):
            copy.wait()
        for copy in own_arrivals(s):
            copy.wait_recv()
        near_arrival(s, 0, 0, 0).wait_recv()
        near_arrival(s, 1, 0, 1).wait_recv()
        for way in range(2):
            for c in range(2):
                near_arrival(s, way, 1, c).wait_recv()
        near(s)
        for copy in far_sends(s):
            copy.wait_recv()
        far(s)

        @pl.when(s > 0)
        def _():
            finish(s - 1)
        return 0

    lax.fori_loop(0, seqs, stage, 0)
    finish(seqs - 1)

    def drain(s, _):
        for copy in near_sends(s) + far_sends(s) + own_sends(s):
            copy.wait_send()
        for copy in x_sends(s):
            copy.wait_send()
        pltpu.make_async_copy(out_v.at[s], out.at[s], out_sem.at[s]).wait()
        return 0
    lax.fori_loop(0, seqs, drain, 0)


def shards(chips, tps, tokens, query_weight, key_weight, value_weight, out_gain, out_weight):
    seqs, length, model_dim = tokens.shape
    channels, out_cols = out_weight.shape
    positions = lax.axis_index("sp") * length + jnp.arange(length, dtype=jnp.int32)
    half_dim = HEAD_DIM // 2
    frequency = ROPE_BASE ** (-jnp.arange(half_dim, dtype=F32) / half_dim)
    angles = positions.astype(F32)[:, None] * frequency[None, :]
    cosine, sine = jnp.cos(angles), jnp.sin(angles)
    cosine = jnp.concatenate([cosine, cosine], axis=1)
    sine = jnp.concatenate([-sine, sine], axis=1)
    any_spec = pl.BlockSpec(memory_space=pl.ANY)
    vmem = pl.BlockSpec(memory_space=pltpu.VMEM)
    dma = pltpu.SemaphoreType.DMA
    grid4 = (OWN, 4, 4, 16, HEAD_DIM)
    return pl.pallas_call(
        functools.partial(kernel, chips, tps, seqs),
        out_shape=(jax.ShapeDtypeStruct((seqs, length, out_cols), BF16),
                   jax.ShapeDtypeStruct((seqs, 2, length), F32)),
        in_specs=[any_spec, any_spec, any_spec, any_spec, vmem, any_spec, vmem, vmem],
        out_specs=(any_spec, vmem),
        scratch_shapes=[
            pltpu.VMEM((seqs, TOK, model_dim), BF16),
            pltpu.VMEM((model_dim, 256), BF16),
            pltpu.VMEM((model_dim, 256), BF16),
            pltpu.VMEM((model_dim, 256), BF16),
            pltpu.VMEM((channels, out_cols), BF16),
            pltpu.VMEM((seqs, 2, TOK, 256), BF16),
            pltpu.VMEM((seqs, 2, TOK, 128), BF16),
            pltpu.VMEM((seqs, ROWS, 256), BF16),
            pltpu.VMEM((seqs, CHIP, 128), BF16),
            pltpu.VMEM((NBLK, 4, 4, 16, 256), BF16),
            pltpu.VMEM(grid4, BF16),
            pltpu.VMEM((BLK, BLK), BF16),
            pltpu.VMEM((OWN, BLK, BLK + 2 * REACH), F32),
            pltpu.VMEM((OWN, 64, 192), F32),
            pltpu.VMEM((16 * OWN, 16 * NBLK), F32),
            pltpu.VMEM(grid4, F32),
            pltpu.VMEM(grid4, F32),
            pltpu.VMEM(grid4, F32),
            pltpu.VMEM(grid4, BF16),
            pltpu.VMEM(grid4, F32),
            pltpu.VMEM((seqs, CHIP, 128), BF16),
            pltpu.VMEM((seqs, 2, 3, 128), F32),
            pltpu.VMEM((seqs, 3, 128), F32),
            pltpu.VMEM((seqs, TOK, channels), BF16),
            pltpu.VMEM((seqs, TOK, out_cols), BF16),
            dma((4 + seqs,)),
            dma((seqs, 2)),
            dma((seqs, 12)),
            dma((seqs, 12)),
            dma((seqs, 8)),
            dma((seqs, 8)),
            dma((seqs,)),
            dma((seqs,)),
            dma((seqs,)),
            dma((seqs,)),
        ],
        compiler_params=pltpu.CompilerParams(
            collective_id=0, has_side_effects=True, vmem_limit_bytes=60 * 1024 * 1024
        ),
    )(tokens, query_weight, key_weight, value_weight, out_gain.reshape(1, channels), out_weight, cosine, sine)


def solution(mesh):
    return jax.shard_map(
        functools.partial(shards, mesh.shape["sp"] // 2, mesh.shape["tp"]),
        mesh=mesh,
        in_specs=(
            P(None, "sp", None),
            P(None, "tp"),
            P(None, "tp"),
            P(None, "tp"),
            P(),
            P(None, "tp"),
        ),
        out_specs=(P(None, "sp", "tp"), P(None, "tp", "sp")),
        check_vma=False,
    )
```

```python
import functools

import jax
import jax.numpy as jnp
from jax import lax
from jax.experimental import pallas as pl
from jax.experimental.pallas import tpu as pltpu
from jax.sharding import PartitionSpec as P

HEAD_DIM = 128
REACH = 64
ROPE_BASE = 10000.0
MASK_FILL = -1e30
NORM_FLOOR = 1e-6
LOG2E = 1.4426950408889634
SCALE = HEAD_DIM ** (-0.5)
RATE = SCALE * LOG2E

TOK = 384
CHIP = 2 * TOK
BLK = 256
WIDE = 1024
HALO = WIDE // BLK
OWN = CHIP // BLK
NBLK = 2 * HALO + OWN
ROWS = NBLK * BLK
MESH = pl.DeviceIdType.MESH
F32 = jnp.float32
BF16 = jnp.bfloat16


def dot_nt(a, b):
    return lax.dot_general(a, b, (((1,), (1,)), ((), ())), preferred_element_type=F32)


def dot(a, b):
    return jnp.dot(a, b, preferred_element_type=F32)


def softened(scores):
    peak = jnp.max(scores, axis=-1, keepdims=True)
    probs = jnp.exp2((scores - peak) * RATE)
    return probs.astype(BF16), peak, jnp.sum(probs, axis=-1, keepdims=True)


def pipelined(jobs):
    ahead = jobs[0][0]()
    for i, (_, finish) in enumerate(jobs):
        now = ahead
        if i + 1 < len(jobs):
            ahead = jobs[i + 1][0]()
        finish(now)


def joined(parts):
    peak = functools.reduce(jnp.maximum, [part[1] for part in parts])
    merged, total = 0.0, 0.0
    for acc_g, peak_g, sum_g in parts:
        share = jnp.exp2((peak_g - peak) * RATE)
        merged = merged + share * acc_g
        total = total + share * sum_g
    return merged, peak, total


def iota(shape, dim):
    return lax.broadcasted_iota(jnp.int32, shape, dim)


def kernel(chips, tps, seqs, tokens, wq, wk, wv, gain, wo, frequency, out, logs,
           cos, sin, tok_v, wq_v, wk_v, wv_v, wo_v, kvown, qown, kvbuf, qbuf, kvp, qp, perm,
           bias1, bias4, bias16, acc1, peak1, sum1, mperm, lperm, mnat, lnat, lrx, mg, out_v,
           in_sem, loc_sem, kv_send, kv_recv, x_send, x_recv, l_send, l_recv, x_loc, out_sem):
    sp, tp = lax.axis_index("sp"), lax.axis_index("tp")
    chip, core = sp // 2, sp % 2

    loads = [pltpu.make_async_copy(wk, wk_v, in_sem.at[0]),
             pltpu.make_async_copy(tokens.at[0], tok_v.at[0], in_sem.at[4]),
             pltpu.make_async_copy(wv, wv_v, in_sem.at[1]),
             pltpu.make_async_copy(wq, wq_v, in_sem.at[2])]
    for s in range(1, seqs):
        loads.append(pltpu.make_async_copy(tokens.at[s], tok_v.at[s], in_sem.at[4 + s]))
    loads.append(pltpu.make_async_copy(wo, wo_v, in_sem.at[3]))
    for load in loads:
        load.start()

    barrier = pltpu.get_barrier_semaphore()
    partners = [(2 * chip + 1 - core, tp)]
    for dx in range(1, tps):
        for c in range(2):
            partners.append((2 * chip + c, (tp + dx) % tps))
    has_left, has_right = chip > 0, chip < chips - 1
    has_far_left, has_far_right = chip > 1, chip < chips - 2
    after, before = jnp.minimum(chip + 1, chips - 1), jnp.maximum(chip - 1, 0)
    for partner in partners:
        pl.semaphore_signal(barrier, inc=1, device_id=partner, device_id_type=MESH)
    for has, neighbour in ((has_left, before), (has_right, after)):
        @pl.when(has)
        def _():
            for c in range(2):
                pl.semaphore_signal(barrier, inc=1, device_id=(2 * neighbour + c, tp), device_id_type=MESH)

    angles = (sp * TOK + iota((TOK, HEAD_DIM), 0)).astype(F32) * frequency[...]
    cos[...] = jnp.cos(angles)
    sine = jnp.sin(angles)
    sin[...] = jnp.where(iota((TOK, HEAD_DIM), 1) < HEAD_DIM // 2, -sine, sine)

    def row_of(at, size):
        return pl.ds(pl.multiple_of(at, 128), size)

    def remote(src, dst, send, recv, device):
        return pltpu.make_async_remote_copy(src_ref=src, dst_ref=dst, send_sem=send, recv_sem=recv,
                                            device_id=device, device_id_type=MESH)


    def near_sends(s, way):
        copies = []
        base, to = ((BLK, after), (WIDE + CHIP, before))[way]
        for piece, (src, at, size) in enumerate(((128 * core, 512 * core, BLK), (BLK * (1 - core), BLK + 128 * core, 128))):
            for h in range(2):
                copies.append(remote(kvown.at[s, h, row_of(src, size)], kvbuf.at[s, row_of(base + at, size)],
                                     kv_send.at[s, 4 * piece + 2 * h + way],
                                     kv_recv.at[s, 4 * way + 2 * piece + core], (2 * to + h, tp)))
        return copies

    def far_send(s, way):
        src, dst, to = ((WIDE - BLK, 0, after), (WIDE + CHIP, ROWS - BLK, before))[way]
        return remote(kvbuf.at[s, pl.ds(src, BLK)], kvbuf.at[s, pl.ds(dst, BLK)],
                      kv_send.at[s, 8 + way], kv_recv.at[s, 8 + way], (2 * to + core, tp))

    sends_to = (has_right, has_left)
    hears_from = (has_left, has_right)
    hears_far = (has_far_left, has_far_right)

    def start_near(s):
        for way in range(2):
            @pl.when(sends_to[way])
            def _():
                for copy in near_sends(s, way):
                    copy.start()

    def own_sends(s):
        return [remote(kvown.at[s, 1 - core], kvbuf.at[s, row_of(WIDE + TOK * core, TOK)],
                       kv_send.at[s, 10], kv_recv.at[s, 10], (2 * chip + 1 - core, tp)),
                remote(qown.at[s, 1 - core], qbuf.at[s, row_of(TOK * core, TOK)],
                       kv_send.at[s, 11], kv_recv.at[s, 11], (2 * chip + 1 - core, tp))]

    def local_copies(s):
        return [pltpu.make_async_copy(kvown.at[s, core], kvbuf.at[s, row_of(WIDE + TOK * core, TOK)], loc_sem.at[s, 0]),
                pltpu.make_async_copy(qown.at[s, core], qbuf.at[s, row_of(TOK * core, TOK)], loc_sem.at[s, 1])]

    def near_arrival(s, way, piece, c):
        at, size = ((512 * c, BLK), (BLK + 128 * c, 128))[piece]
        at += (BLK, WIDE + CHIP)[way]
        return remote(kvown.at[s, 0, pl.ds(0, size)], kvbuf.at[s, pl.ds(at, size)], kv_send.at[s, 0],
                      kv_recv.at[s, 4 * way + 2 * piece + c], (2 * chip + 1 - core, tp))

    def own_arrivals(s):
        return [remote(kvown.at[s, 0], kvbuf.at[s, row_of(WIDE + TOK * (1 - core), TOK)], kv_send.at[s, 0],
                       kv_recv.at[s, 10], (2 * chip + 1 - core, tp)),
                remote(qown.at[s, 0], qbuf.at[s, row_of(TOK * (1 - core), TOK)], kv_send.at[s, 0],
                       kv_recv.at[s, 11], (2 * chip + 1 - core, tp))]

    head = 2 * tp + core

    def column_of(h):
        return pl.ds(pl.multiple_of(h * HEAD_DIM, HEAD_DIM), HEAD_DIM)

    def x_sends(s):
        copies = []
        for dx in range(1, tps):
            for c in range(2):
                copies.append(remote(mnat.at[s, pl.ds(TOK * c, TOK)], mg.at[s, :, column_of(head)],
                                     x_send.at[s, 2 * dx + c], x_recv.at[s, head], (2 * chip + c, (tp + dx) % tps)))
        copies.append(remote(mnat.at[s, row_of(TOK * (1 - core), TOK)], mg.at[s, :, column_of(head)],
                             x_send.at[s, 0], x_recv.at[s, head], (2 * chip + 1 - core, tp)))
        copies.append(remote(lnat.at[s, 1 - core], lrx.at[s], l_send.at[s], l_recv.at[s], (2 * chip + 1 - core, tp)))
        return copies

    def x_local(s):
        return pltpu.make_async_copy(mnat.at[s, row_of(TOK * core, TOK)], mg.at[s, :, column_of(head)], x_loc.at[s])

    def x_arrivals(s):
        waits = []
        for o in range(1, 2 * tps):
            other = (head + o) % (2 * tps)
            waits.append(remote(mnat.at[s, pl.ds(0, TOK)], mg.at[s, :, column_of(other)], x_send.at[s, 0],
                                x_recv.at[s, other], (2 * chip + 1 - core, tp)))
        waits.append(remote(lnat.at[s, 0], lrx.at[s], l_send.at[s], l_recv.at[s], (2 * chip + 1 - core, tp)))
        return waits

    def turned(x):
        return (x * cos[...] + pltpu.roll(x, HEAD_DIM // 2, 1) * sin[...]).astype(BF16)

    def project(s, _):
        pltpu.make_async_copy(tokens.at[s], tok_v.at[s], in_sem.at[4 + s]).wait()

        @pl.when(s == 0)
        def _():
            loads[0].wait()
        keys = dot(tok_v[s], wk_v[...])
        for h in range(2):
            kvown[s, h, :, :HEAD_DIM] = turned(keys[:, h * HEAD_DIM:(h + 1) * HEAD_DIM])

        @pl.when(s == 0)
        def _():
            loads[2].wait()
        values = dot(tok_v[s], wv_v[...])
        for h in range(2):
            kvown[s, h, :, HEAD_DIM:] = values[:, h * HEAD_DIM:(h + 1) * HEAD_DIM].astype(BF16)

        @pl.when(s == 0)
        def _():
            pl.semaphore_wait(barrier, len(partners) + 2 * (jnp.where(has_left, 1, 0) + jnp.where(has_right, 1, 0)))
            start_near(0)
        own_sends(s)[0].start()
        local_copies(s)[0].start()

        @pl.when(s == 0)
        def _():
            loads[3].wait()
        queries = dot(tok_v[s], wq_v[...])
        for h in range(2):
            qown[s, h] = turned(queries[:, h * HEAD_DIM:(h + 1) * HEAD_DIM])
        own_sends(s)[1].start()
        local_copies(s)[1].start()
        return 0

    lax.fori_loop(0, seqs, project, 0)
    loads[-1].wait()

    row, col = iota((BLK, BLK), 0), iota((BLK, BLK), 1)
    perm[...] = jnp.where(col == (row % 16) * 16 + row // 16, 1.0, 0.0).astype(BF16)
    first = chip * CHIP
    limit = chips * CHIP
    for b in range(OWN):
        row, col = iota((BLK, BLK + 2 * REACH), 0), iota((BLK, BLK + 2 * REACH), 1)
        gap = (row % 16) * 16 + row // 16 - (col - REACH)
        at = first + b * BLK - REACH + col
        good = (gap >= -REACH) & (gap <= REACH) & (at >= 0) & (at < limit)
        bias1[b] = jnp.where(good, 0.0, MASK_FILL)
        row, col = iota((64, 192), 0), iota((64, 192), 1)
        gap = (row % 16) * 4 + row // 16 - ((col // 64 - 1) * 64 + (col % 16) * 4 + (col % 64) // 16)
        at = first + (b + col // 64 - 1) * BLK
        good = (gap >= -REACH) & (gap <= REACH) & (at >= 0) & (at < limit)
        bias4[b] = jnp.where(good, 0.0, MASK_FILL)
    row, col = iota((16 * OWN, 16 * NBLK), 0), iota((16 * OWN, 16 * NBLK), 1)
    gap = row - (col - 16 * HALO)
    at = first + (col // 16 - HALO) * BLK
    good = (gap >= -REACH) & (gap <= REACH) & (at >= 0) & (at < limit)
    bias16[...] = jnp.where(good, 0.0, MASK_FILL)


    def put_in_order(s, blocks):
        for b in blocks:
            kvp[b] = dot(perm[...], kvbuf[s, pl.ds(b * BLK, BLK), :]).astype(BF16).reshape(4, 4, 16, 2 * HEAD_DIM)

    def near(s):
        for b in range(OWN):
            block = dot(perm[...], qbuf[s, pl.ds(b * BLK, BLK), :]).astype(BF16)
            qp[b] = block.reshape(4, 4, 16, HEAD_DIM)
        put_in_order(s, range(1, NBLK - 1))
        jobs, done = [], {}

        def narrow(b, half):
            around = pl.ds(WIDE + b * BLK - REACH, BLK + 2 * REACH)

            def scores():
                queries = qp[b, 2 * half:2 * half + 2].reshape(128, HEAD_DIM)
                return dot_nt(queries, kvbuf[s, around, :HEAD_DIM]) + bias1[b, half * 128:(half + 1) * 128]

            def finish(scores):
                probs, peak, total = softened(scores)
                done[b, half] = dot(probs, kvbuf[s, around, HEAD_DIM:]), peak, total
            return scores, finish

        def middle(b):
            def scores():
                every = []
                for r in range(4):
                    keys = kvp[b + HALO - 1:b + HALO + 2, :, r, :, :HEAD_DIM].reshape(192, HEAD_DIM)
                    every.append(dot_nt(qp[b, :, r].reshape(64, HEAD_DIM), keys) + bias4[b])
                return every

            def finish(every):
                soft = [softened(scores) for scores in every]
                accs = []
                for r in range(4):
                    values = kvp[b + HALO - 1:b + HALO + 2, :, r, :, HEAD_DIM:].reshape(192, HEAD_DIM)
                    accs.append(dot(soft[r][0], values))
                for a in range(4):
                    for r in range(4):
                        at = (a % 2) * 64 + r * 16
                        one = tuple(x[at:at + 16] for x in done[b, a // 2])
                        two = tuple(x[a * 16:(a + 1) * 16] for x in (accs[r],) + soft[r][1:])
                        acc, peak, total = joined((one, two))
                        acc1[b, a, r] = acc
                        peak1[b, a, r] = jnp.broadcast_to(peak, (16, HEAD_DIM))
                        sum1[b, a, r] = jnp.broadcast_to(total, (16, HEAD_DIM))
            return scores, finish

        for b in range(OWN):
            jobs += [narrow(b, 0), narrow(b, 1), middle(b)]
        pipelined(jobs)

    def far(s):
        put_in_order(s, (0, NBLK - 1))

        def wide(r):
            def scores():
                every = []
                for a in range(4):
                    keys = kvp[:, a, r, :, :HEAD_DIM].reshape(16 * NBLK, HEAD_DIM)
                    every.append(dot_nt(qp[:, a, r].reshape(16 * OWN, HEAD_DIM), keys) + bias16[...])
                return every

            def finish(every):
                soft = [softened(scores) for scores in every]
                accs = []
                for a in range(4):
                    values = kvp[:, a, r, :, HEAD_DIM:].reshape(16 * NBLK, HEAD_DIM)
                    accs.append(dot(soft[a][0], values))
                for a in range(4):
                    for b in range(OWN):
                        one = (acc1[b, a, r], peak1[b, a, r], sum1[b, a, r])
                        two = tuple(x[b * 16:(b + 1) * 16] for x in (accs[a],) + soft[a][1:])
                        merged, peak, total = joined((one, two))
                        mperm[b, a, r] = (merged / total).astype(BF16)
                        lperm[b, a, r] = peak * SCALE + jnp.log(total)
            return scores, finish

        pipelined([wide(r) for r in range(4)])
        for b in range(OWN):
            mnat[s, pl.ds(b * BLK, BLK), :] = dot(perm[...], mperm[b].reshape(BLK, HEAD_DIM)).astype(BF16)
        for copy in x_sends(s)[:-1]:
            copy.start()
        x_local(s).start()
        for b in range(OWN):
            column = lperm[b].reshape(BLK, HEAD_DIM)
            for half in range(2):
                hit = perm[:, half * 128:(half + 1) * 128].astype(F32)
                line = jnp.sum(jnp.where(hit > 0.5, column, 0.0), axis=0, keepdims=True)
                piece = 2 * b + half
                lnat[s, piece // 3, piece % 3:piece % 3 + 1, :] = line
        x_sends(s)[-1].start()

    def finish(s):
        x_local(s).wait()
        for copy in x_arrivals(s):
            copy.wait_recv()
        lifted = mg[s].astype(F32)
        square = jnp.mean(lifted * lifted, axis=-1, keepdims=True)
        scaled = (lifted * gain[...]).astype(BF16)
        projected = dot(scaled, wo_v[...])
        out_v[s] = (projected * lax.rsqrt(square + NORM_FLOOR)).astype(BF16)
        pltpu.make_async_copy(out_v.at[s], out.at[s], out_sem.at[s]).start()
        mine, theirs = lnat[s, core], lrx[s]
        upper = jnp.where(core == 0, mine, theirs)
        lower = jnp.where(core == 0, theirs, mine)
        for piece in range(3):
            lanes = pl.ds(piece * 128, 128)
            logs[s, 0:1, lanes] = upper[piece:piece + 1]
            logs[s, 1:2, lanes] = lower[piece:piece + 1]

    for has, at, size in ((has_left, BLK, CHIP), (has_far_left, 0, BLK),
                          (has_right, WIDE + CHIP, CHIP), (has_far_right, ROWS - BLK, BLK)):
        @pl.when(jnp.logical_not(has))
        def _():
            def clear(s, _):
                kvbuf[s, pl.ds(at, size), :] = jnp.zeros((size, 2 * HEAD_DIM), BF16)
                return 0
            lax.fori_loop(0, seqs, clear, 0)

    def stage(s, _):
        for way in range(2):
            @pl.when(hears_from[way])
            def _():
                near_arrival(s, way, 0, 1 - way).wait_recv()

            @pl.when(jnp.logical_and(hears_from[way], sends_to[way]))
            def _():
                far_send(s, way).start()

        @pl.when(s + 1 < seqs)
        def _():
            start_near(s + 1)

        for copy in local_copies(s):
            copy.wait()
        for copy in own_arrivals(s):
            copy.wait_recv()
        for way in range(2):
            @pl.when(hears_from[way])
            def _():
                near_arrival(s, way, 0, way).wait_recv()
                for c in range(2):
                    near_arrival(s, way, 1, c).wait_recv()
        near(s)
        for way in range(2):
            @pl.when(hears_far[way])
            def _():
                far_send(s, way).wait_recv()
        far(s)

        @pl.when(s > 0)
        def _():
            finish(s - 1)
        return 0

    lax.fori_loop(0, seqs, stage, 0)
    finish(seqs - 1)

    def drain(s, _):
        for copy in own_sends(s):
            copy.wait_send()
        for way in range(2):
            @pl.when(sends_to[way])
            def _():
                for copy in near_sends(s, way):
                    copy.wait_send()

            @pl.when(jnp.logical_and(hears_from[way], sends_to[way]))
            def _():
                far_send(s, way).wait_send()
        for copy in x_sends(s):
            copy.wait_send()
        pltpu.make_async_copy(out_v.at[s], out.at[s], out_sem.at[s]).wait()
        return 0
    lax.fori_loop(0, seqs, drain, 0)


def shards(chips, tps, tokens, query_weight, key_weight, value_weight, out_gain, out_weight):
    seqs, length, model_dim = tokens.shape
    channels, out_cols = out_weight.shape
    half_dim = HEAD_DIM // 2
    frequency = ROPE_BASE ** (-jnp.arange(half_dim, dtype=F32) / half_dim)
    frequency = jnp.concatenate([frequency, frequency]).reshape(1, HEAD_DIM)
    any_spec = pl.BlockSpec(memory_space=pl.ANY)
    vmem = pl.BlockSpec(memory_space=pltpu.VMEM)
    dma = pltpu.SemaphoreType.DMA
    grid4 = (OWN, 4, 4, 16, HEAD_DIM)
    return pl.pallas_call(
        functools.partial(kernel, chips, tps, seqs),
        out_shape=(pltpu.VMEM((seqs, length, out_cols), BF16),
                   jax.ShapeDtypeStruct((seqs, 2, length), F32)),
        in_specs=[any_spec, any_spec, any_spec, any_spec, vmem, any_spec, vmem],
        out_specs=(any_spec, vmem),
        scratch_shapes=[
            pltpu.VMEM((TOK, HEAD_DIM), F32),
            pltpu.VMEM((TOK, HEAD_DIM), F32),
            pltpu.VMEM((seqs, TOK, model_dim), BF16),
            pltpu.VMEM((model_dim, 256), BF16),
            pltpu.VMEM((model_dim, 256), BF16),
            pltpu.VMEM((model_dim, 256), BF16),
            pltpu.VMEM((channels, out_cols), BF16),
            pltpu.VMEM((seqs, 2, TOK, 256), BF16),
            pltpu.VMEM((seqs, 2, TOK, 128), BF16),
            pltpu.VMEM((seqs, ROWS, 256), BF16),
            pltpu.VMEM((seqs, CHIP, 128), BF16),
            pltpu.VMEM((NBLK, 4, 4, 16, 256), BF16),
            pltpu.VMEM(grid4, BF16),
            pltpu.VMEM((BLK, BLK), BF16),
            pltpu.VMEM((OWN, BLK, BLK + 2 * REACH), F32),
            pltpu.VMEM((OWN, 64, 192), F32),
            pltpu.VMEM((16 * OWN, 16 * NBLK), F32),
            pltpu.VMEM(grid4, F32),
            pltpu.VMEM(grid4, F32),
            pltpu.VMEM(grid4, F32),
            pltpu.VMEM(grid4, BF16),
            pltpu.VMEM(grid4, F32),
            pltpu.VMEM((seqs, CHIP, 128), BF16),
            pltpu.VMEM((seqs, 2, 3, 128), F32),
            pltpu.VMEM((seqs, 3, 128), F32),
            pltpu.VMEM((seqs, TOK, channels), BF16),
            pltpu.VMEM((seqs, TOK, out_cols), BF16),
            dma((4 + seqs,)),
            dma((seqs, 2)),
            dma((seqs, 12)),
            dma((seqs, 12)),
            dma((seqs, 8)),
            dma((seqs, 8)),
            dma((seqs,)),
            dma((seqs,)),
            dma((seqs,)),
            dma((seqs,)),
        ],
        compiler_params=pltpu.CompilerParams(
            collective_id=0, has_side_effects=True, vmem_limit_bytes=62 * 1024 * 1024
        ),
    )(tokens, query_weight, key_weight, value_weight, out_gain.reshape(1, channels), out_weight, frequency)


def solution(mesh):
    return jax.shard_map(
        functools.partial(shards, mesh.shape["sp"] // 2, mesh.shape["tp"]),
        mesh=mesh,
        in_specs=(
            P(None, "sp", None),
            P(None, "tp"),
            P(None, "tp"),
            P(None, "tp"),
            P(),
            P(None, "tp"),
        ),
        out_specs=(P(None, "sp", "tp"), P(None, "tp", "sp")),
        check_vma=False,
    )
```

```python
import functools

import jax
import jax.numpy as jnp
from jax import lax
from jax.experimental import pallas as pl
from jax.experimental.pallas import tpu as pltpu
from jax.sharding import PartitionSpec as P

HEAD_DIM = 128
REACH = 64
ROPE_BASE = 10000.0
MASK_FILL = -1e30
NORM_FLOOR = 1e-6
LOG2E = 1.4426950408889634
SCALE = HEAD_DIM ** (-0.5)
RATE = SCALE * LOG2E

TOK = 384
CHIP = 2 * TOK
BLK = 256
WIDE = 1024
HALO = WIDE // BLK
OWN = CHIP // BLK
NBLK = 2 * HALO + OWN
ROWS = NBLK * BLK
MESH = pl.DeviceIdType.MESH
F32 = jnp.float32
BF16 = jnp.bfloat16


def dot_nt(a, b):
    return lax.dot_general(a, b, (((1,), (1,)), ((), ())), preferred_element_type=F32)


def dot(a, b):
    return jnp.dot(a, b, preferred_element_type=F32)


def softened(scores):
    peak = jnp.max(scores, axis=-1, keepdims=True)
    probs = jnp.exp2((scores - peak) * RATE)
    return probs.astype(BF16), peak, jnp.sum(probs, axis=-1, keepdims=True)


def pipelined(jobs):
    ahead = jobs[0][0]()
    for i, (_, finish) in enumerate(jobs):
        now = ahead
        if i + 1 < len(jobs):
            ahead = jobs[i + 1][0]()
        finish(now)


def joined(parts):
    peak = functools.reduce(jnp.maximum, [part[1] for part in parts])
    merged, total = 0.0, 0.0
    for acc_g, peak_g, sum_g in parts:
        share = jnp.exp2((peak_g - peak) * RATE)
        merged = merged + share * acc_g
        total = total + share * sum_g
    return merged, peak, total


def iota(shape, dim):
    return lax.broadcasted_iota(jnp.int32, shape, dim)


def kernel(chips, tps, seqs, tokens, wq, wk, wv, gain, wo, frequency, out, logs,
           cos, sin, tok_v, wq_v, wk_v, wv_v, wo_v, kvown, qown, kvbuf, qbuf, kvp, qp, perm,
           bias1, bias4, bias_mid, bias_out, acc1, peak1, sum1, mperm, lperm, mnat, lnat, lrx, mg, out_v,
           in_sem, loc_sem, kv_send, kv_recv, x_send, x_recv, l_send, l_recv, x_loc, out_sem):
    sp, tp = lax.axis_index("sp"), lax.axis_index("tp")
    chip, core = sp // 2, sp % 2

    loads = [pltpu.make_async_copy(wk, wk_v, in_sem.at[0]),
             pltpu.make_async_copy(tokens.at[0], tok_v.at[0], in_sem.at[4]),
             pltpu.make_async_copy(wv, wv_v, in_sem.at[1]),
             pltpu.make_async_copy(wq, wq_v, in_sem.at[2])]
    for s in range(1, seqs):
        loads.append(pltpu.make_async_copy(tokens.at[s], tok_v.at[s], in_sem.at[4 + s]))
    loads.append(pltpu.make_async_copy(wo, wo_v, in_sem.at[3]))
    for load in loads[:3]:
        load.start()

    barrier = pltpu.get_barrier_semaphore()
    partners = [(2 * chip + 1 - core, tp)]
    for dx in range(1, tps):
        for c in range(2):
            partners.append((2 * chip + c, (tp + dx) % tps))
    has_left, has_right = chip > 0, chip < chips - 1
    has_far_left, has_far_right = chip > 1, chip < chips - 2
    after, before = jnp.minimum(chip + 1, chips - 1), jnp.maximum(chip - 1, 0)
    for partner in partners:
        pl.semaphore_signal(barrier, inc=1, device_id=partner, device_id_type=MESH)
    for has, neighbour in ((has_left, before), (has_right, after)):
        @pl.when(has)
        def _():
            for c in range(2):
                pl.semaphore_signal(barrier, inc=1, device_id=(2 * neighbour + c, tp), device_id_type=MESH)

    angles = (sp * TOK + iota((TOK, HEAD_DIM), 0)).astype(F32) * frequency[...]
    cos[...] = jnp.cos(angles)
    sine = jnp.sin(angles)
    sin[...] = jnp.where(iota((TOK, HEAD_DIM), 1) < HEAD_DIM // 2, -sine, sine)

    def row_of(at, size):
        return pl.ds(pl.multiple_of(at, 128), size)

    def remote(src, dst, send, recv, device):
        return pltpu.make_async_remote_copy(src_ref=src, dst_ref=dst, send_sem=send, recv_sem=recv,
                                            device_id=device, device_id_type=MESH)


    def near_sends(s, way):
        copies = []
        base, to = ((BLK, after), (WIDE + CHIP, before))[way]
        for piece, (src, at, size) in enumerate(((128 * core, 512 * core, BLK), (BLK * (1 - core), BLK + 128 * core, 128))):
            for h in range(2):
                copies.append(remote(kvown.at[s, h, row_of(src, size)], kvbuf.at[s, row_of(base + at, size)],
                                     kv_send.at[s, 4 * piece + 2 * h + way],
                                     kv_recv.at[s, 4 * way + 2 * piece + core], (2 * to + h, tp)))
        return copies

    def far_send(s, way):
        src, dst, to = ((WIDE - BLK, 0, after), (WIDE + CHIP, ROWS - BLK, before))[way]
        return remote(kvbuf.at[s, pl.ds(src, BLK)], kvbuf.at[s, pl.ds(dst, BLK)],
                      kv_send.at[s, 8 + way], kv_recv.at[s, 8 + way], (2 * to + core, tp))

    sends_to = (has_right, has_left)
    hears_from = (has_left, has_right)
    hears_far = (has_far_left, has_far_right)

    def start_near(s):
        for way in range(2):
            @pl.when(sends_to[way])
            def _():
                for copy in near_sends(s, way):
                    copy.start()

    def own_sends(s):
        return [remote(kvown.at[s, 1 - core], kvbuf.at[s, row_of(WIDE + TOK * core, TOK)],
                       kv_send.at[s, 10], kv_recv.at[s, 10], (2 * chip + 1 - core, tp)),
                remote(qown.at[s, 1 - core], qbuf.at[s, row_of(TOK * core, TOK)],
                       kv_send.at[s, 11], kv_recv.at[s, 11], (2 * chip + 1 - core, tp))]

    def local_copies(s):
        return [pltpu.make_async_copy(kvown.at[s, core], kvbuf.at[s, row_of(WIDE + TOK * core, TOK)], loc_sem.at[s, 0]),
                pltpu.make_async_copy(qown.at[s, core], qbuf.at[s, row_of(TOK * core, TOK)], loc_sem.at[s, 1])]

    def near_arrival(s, way, piece, c):
        at, size = ((512 * c, BLK), (BLK + 128 * c, 128))[piece]
        at += (BLK, WIDE + CHIP)[way]
        return remote(kvown.at[s, 0, pl.ds(0, size)], kvbuf.at[s, pl.ds(at, size)], kv_send.at[s, 0],
                      kv_recv.at[s, 4 * way + 2 * piece + c], (2 * chip + 1 - core, tp))

    def own_arrivals(s):
        return [remote(kvown.at[s, 0], kvbuf.at[s, row_of(WIDE + TOK * (1 - core), TOK)], kv_send.at[s, 0],
                       kv_recv.at[s, 10], (2 * chip + 1 - core, tp)),
                remote(qown.at[s, 0], qbuf.at[s, row_of(TOK * (1 - core), TOK)], kv_send.at[s, 0],
                       kv_recv.at[s, 11], (2 * chip + 1 - core, tp))]

    head = 2 * tp + core

    def column_of(h):
        return pl.ds(pl.multiple_of(h * HEAD_DIM, HEAD_DIM), HEAD_DIM)

    def piece_of(piece, c):
        return ((BLK * (1 - c), 128), (128 * c, BLK))[piece]

    def x_sends(s, piece):
        copies = []
        for dx in [tps // 2] + [d for d in range(1, tps) if d != tps // 2]:
            for c in range(2) if tps > 1 else ():
                at, size = piece_of(piece, c)
                copies.append(remote(mnat.at[s, pl.ds(TOK * c + at, size)], mg.at[s, pl.ds(at, size), column_of(head)],
                                     x_send.at[s, 8 * piece + 2 * dx + c], x_recv.at[s, 8 * piece + head],
                                     (2 * chip + c, (tp + dx) % tps)))
        at, size = piece_of(piece, 1 - core)
        copies.append(remote(mnat.at[s, row_of(TOK * (1 - core) + at, size)], mg.at[s, row_of(at, size), column_of(head)],
                             x_send.at[s, 8 * piece], x_recv.at[s, 8 * piece + head], (2 * chip + 1 - core, tp)))
        return copies

    def log_send(s):
        return remote(lnat.at[s, 1 - core], lrx.at[s], l_send.at[s], l_recv.at[s], (2 * chip + 1 - core, tp))

    def x_local(s):
        return pltpu.make_async_copy(mnat.at[s, row_of(TOK * core, TOK)], mg.at[s, :, column_of(head)], x_loc.at[s])

    def x_arrivals(s):
        waits = []
        for piece in range(2):
            at, size = piece_of(piece, core)
            for o in range(1, 2 * tps):
                other = (head + o) % (2 * tps)
                waits.append(remote(mnat.at[s, pl.ds(0, size)], mg.at[s, row_of(at, size), column_of(other)],
                                    x_send.at[s, 0], x_recv.at[s, 8 * piece + other], (2 * chip + 1 - core, tp)))
        return waits

    def turned(x):
        return (x * cos[...] + pltpu.roll(x, HEAD_DIM // 2, 1) * sin[...]).astype(BF16)

    def project(s, _):
        pltpu.make_async_copy(tokens.at[s], tok_v.at[s], in_sem.at[4 + s]).wait()

        @pl.when(s == 0)
        def _():
            loads[0].wait()
            loads[2].wait()
            for load in loads[3:]:
                load.start()
        keys = dot(tok_v[s], wk_v[...])
        for h in range(2):
            kvown[s, h, :, :HEAD_DIM] = turned(keys[:, h * HEAD_DIM:(h + 1) * HEAD_DIM])

        values = dot(tok_v[s], wv_v[...])
        for h in range(2):
            kvown[s, h, :, HEAD_DIM:] = values[:, h * HEAD_DIM:(h + 1) * HEAD_DIM].astype(BF16)

        @pl.when(s == 0)
        def _():
            pl.semaphore_wait(barrier, len(partners) + 2 * (jnp.where(has_left, 1, 0) + jnp.where(has_right, 1, 0)))
            start_near(0)
        own_sends(s)[0].start()
        local_copies(s)[0].start()

        @pl.when(s == 0)
        def _():
            loads[3].wait()
        queries = dot(tok_v[s], wq_v[...])
        for h in range(2):
            qown[s, h] = turned(queries[:, h * HEAD_DIM:(h + 1) * HEAD_DIM])
        own_sends(s)[1].start()
        local_copies(s)[1].start()
        return 0

    lax.fori_loop(0, seqs, project, 0)
    loads[-1].wait()

    row, col = iota((BLK, BLK), 0), iota((BLK, BLK), 1)
    perm[...] = jnp.where(col == (row % 16) * 16 + row // 16, 1.0, 0.0).astype(BF16)
    first = chip * CHIP
    limit = chips * CHIP
    for b in range(OWN):
        row, col = iota((BLK, BLK + 2 * REACH), 0), iota((BLK, BLK + 2 * REACH), 1)
        gap = (row % 16) * 16 + row // 16 - (col - REACH)
        at = first + b * BLK - REACH + col
        good = (gap >= -REACH) & (gap <= REACH) & (at >= 0) & (at < limit)
        bias1[b] = jnp.where(good, 0.0, MASK_FILL)
        row, col = iota((64, 192), 0), iota((64, 192), 1)
        gap = (row % 16) * 4 + row // 16 - ((col // 64 - 1) * 64 + (col % 16) * 4 + (col % 64) // 16)
        at = first + (b + col // 64 - 1) * BLK
        good = (gap >= -REACH) & (gap <= REACH) & (at >= 0) & (at < limit)
        bias4[b] = jnp.where(good, 0.0, MASK_FILL)
    for ref, q_blocks, k_blocks in ((bias_mid, (1,), range(1, NBLK - 1)), (bias_out, (0, 2), range(NBLK))):
        dims = (16 * len(q_blocks), 16 * len(k_blocks))
        row, col = iota(dims, 0), iota(dims, 1)
        q_at = row % 16 + 16 * (q_blocks[0] + 2 * (row // 16))
        block = col // 16 + k_blocks[0] - HALO
        gap = q_at - (col % 16 + 16 * block)
        at = first + block * BLK
        good = (gap >= -REACH) & (gap <= REACH) & (at >= 0) & (at < limit)
        ref[...] = jnp.where(good, 0.0, MASK_FILL)

    def put_in_order(s, blocks):
        for b in blocks:
            kvp[b] = dot(perm[...], kvbuf[s, pl.ds(b * BLK, BLK), :]).astype(BF16).reshape(4, 4, 16, 2 * HEAD_DIM)

    def near(s):
        for b in range(OWN):
            block = dot(perm[...], qbuf[s, pl.ds(b * BLK, BLK), :]).astype(BF16)
            qp[b] = block.reshape(4, 4, 16, HEAD_DIM)
        put_in_order(s, range(1, NBLK - 1))
        jobs, done = [], {}

        def narrow(b, half):
            around = pl.ds(WIDE + b * BLK - REACH, BLK + 2 * REACH)

            def scores():
                queries = qp[b, 2 * half:2 * half + 2].reshape(128, HEAD_DIM)
                return dot_nt(queries, kvbuf[s, around, :HEAD_DIM]) + bias1[b, half * 128:(half + 1) * 128]

            def finish(scores):
                probs, peak, total = softened(scores)
                done[b, half] = dot(probs, kvbuf[s, around, HEAD_DIM:]), peak, total
            return scores, finish

        def middle(b):
            def scores():
                every = []
                for r in range(4):
                    keys = kvp[b + HALO - 1:b + HALO + 2, :, r, :, :HEAD_DIM].reshape(192, HEAD_DIM)
                    every.append(dot_nt(qp[b, :, r].reshape(64, HEAD_DIM), keys) + bias4[b])
                return every

            def finish(every):
                soft = [softened(scores) for scores in every]
                accs = []
                for r in range(4):
                    values = kvp[b + HALO - 1:b + HALO + 2, :, r, :, HEAD_DIM:].reshape(192, HEAD_DIM)
                    accs.append(dot(soft[r][0], values))
                for a in range(4):
                    for r in range(4):
                        at = (a % 2) * 64 + r * 16
                        one = tuple(x[at:at + 16] for x in done[b, a // 2])
                        two = tuple(x[a * 16:(a + 1) * 16] for x in (accs[r],) + soft[r][1:])
                        acc, peak, total = joined((one, two))
                        acc1[b, a, r] = acc
                        peak1[b, a, r] = jnp.broadcast_to(peak, (16, HEAD_DIM))
                        sum1[b, a, r] = jnp.broadcast_to(total, (16, HEAD_DIM))
            return scores, finish

        pipelined([narrow(1, 0), narrow(1, 1), middle(1)] + [wide(r, (1,), range(1, NBLK - 1), bias_mid) for r in range(4)])
        in_order(s, 1)
        for copy in x_sends(s, 0):
            copy.start()
        for b in (0, 2):
            jobs += [narrow(b, 0), narrow(b, 1), middle(b)]
        pipelined(jobs)

    def wide(r, q_blocks, k_blocks, bias):
        keys_in = slice(k_blocks[0], k_blocks[-1] + 1)

        def scores():
            every = []
            for a in range(4):
                keys = kvp[keys_in, a, r, :, :HEAD_DIM].reshape(16 * len(k_blocks), HEAD_DIM)
                queries = jnp.concatenate([qp[b, a, r] for b in q_blocks], axis=0)
                every.append(dot_nt(queries, keys) + bias[...])
            return every

        def finish(every):
            soft = [softened(scores) for scores in every]
            accs = []
            for a in range(4):
                values = kvp[keys_in, a, r, :, HEAD_DIM:].reshape(16 * len(k_blocks), HEAD_DIM)
                accs.append(dot(soft[a][0], values))
            for a in range(4):
                for i, b in enumerate(q_blocks):
                    one = (acc1[b, a, r], peak1[b, a, r], sum1[b, a, r])
                    two = tuple(x[i * 16:(i + 1) * 16] for x in (accs[a],) + soft[a][1:])
                    merged, peak, total = joined((one, two))
                    mperm[b, a, r] = (merged / total).astype(BF16)
                    lperm[b, a, r] = peak * SCALE + jnp.log(total)
        return scores, finish

    def in_order(s, b):
        mnat[s, pl.ds(b * BLK, BLK), :] = dot(perm[...], mperm[b].reshape(BLK, HEAD_DIM)).astype(BF16)

    def far(s):
        put_in_order(s, (0, NBLK - 1))
        pipelined([wide(r, (0, 2), range(NBLK), bias_out) for r in range(4)])
        for b in (0, 2):
            in_order(s, b)
        for copy in x_sends(s, 1):
            copy.start()
        x_local(s).start()
        for b in range(OWN):
            column = lperm[b].reshape(BLK, HEAD_DIM)
            for half in range(2):
                hit = perm[:, half * 128:(half + 1) * 128].astype(F32)
                line = jnp.sum(jnp.where(hit > 0.5, column, 0.0), axis=0, keepdims=True)
                piece = 2 * b + half
                lnat[s, piece // 3, piece % 3:piece % 3 + 1, :] = line
        log_send(s).start()

    def finish(s):
        x_local(s).wait()
        for copy in x_arrivals(s):
            copy.wait_recv()
        log_send(s).wait_recv()
        lifted = mg[s].astype(F32)
        square = jnp.mean(lifted * lifted, axis=-1, keepdims=True)
        scaled = (lifted * gain[...]).astype(BF16)
        projected = dot(scaled, wo_v[...])
        out_v[s] = (projected * lax.rsqrt(square + NORM_FLOOR)).astype(BF16)
        pltpu.make_async_copy(out_v.at[s], out.at[s], out_sem.at[s]).start()
        mine, theirs = lnat[s, core], lrx[s]
        upper = jnp.where(core == 0, mine, theirs)
        lower = jnp.where(core == 0, theirs, mine)
        for piece in range(3):
            lanes = pl.ds(piece * 128, 128)
            logs[s, 0:1, lanes] = upper[piece:piece + 1]
            logs[s, 1:2, lanes] = lower[piece:piece + 1]

    for has, at, size in ((has_left, BLK, CHIP), (has_far_left, 0, BLK),
                          (has_right, WIDE + CHIP, CHIP), (has_far_right, ROWS - BLK, BLK)):
        @pl.when(jnp.logical_not(has))
        def _():
            def clear(s, _):
                kvbuf[s, pl.ds(at, size), :] = jnp.zeros((size, 2 * HEAD_DIM), BF16)
                return 0
            lax.fori_loop(0, seqs, clear, 0)

    def stage(s, _):
        for way in range(2):
            @pl.when(hears_from[way])
            def _():
                near_arrival(s, way, 0, 1 - way).wait_recv()

            @pl.when(jnp.logical_and(hears_from[way], sends_to[way]))
            def _():
                far_send(s, way).start()

        @pl.when(s + 1 < seqs)
        def _():
            start_near(s + 1)

        for copy in local_copies(s):
            copy.wait()
        for copy in own_arrivals(s):
            copy.wait_recv()
        for way in range(2):
            @pl.when(hears_from[way])
            def _():
                near_arrival(s, way, 0, way).wait_recv()
                for c in range(2):
                    near_arrival(s, way, 1, c).wait_recv()
        near(s)
        for way in range(2):
            @pl.when(hears_far[way])
            def _():
                far_send(s, way).wait_recv()
        far(s)

        @pl.when(s > 0)
        def _():
            finish(s - 1)
        return 0

    lax.fori_loop(0, seqs, stage, 0)
    finish(seqs - 1)

    def drain(s, _):
        for copy in own_sends(s):
            copy.wait_send()
        for way in range(2):
            @pl.when(sends_to[way])
            def _():
                for copy in near_sends(s, way):
                    copy.wait_send()

            @pl.when(jnp.logical_and(hears_from[way], sends_to[way]))
            def _():
                far_send(s, way).wait_send()
        for copy in x_sends(s, 0) + x_sends(s, 1):
            copy.wait_send()
        log_send(s).wait_send()
        pltpu.make_async_copy(out_v.at[s], out.at[s], out_sem.at[s]).wait()
        return 0
    lax.fori_loop(0, seqs, drain, 0)


def shards(chips, tps, tokens, query_weight, key_weight, value_weight, out_gain, out_weight):
    seqs, length, model_dim = tokens.shape
    channels, out_cols = out_weight.shape
    half_dim = HEAD_DIM // 2
    frequency = ROPE_BASE ** (-(jnp.arange(HEAD_DIM) % half_dim).astype(F32) / half_dim)
    frequency = frequency.reshape(1, HEAD_DIM)
    any_spec = pl.BlockSpec(memory_space=pl.ANY)
    vmem = pl.BlockSpec(memory_space=pltpu.VMEM)
    dma = pltpu.SemaphoreType.DMA
    grid4 = (OWN, 4, 4, 16, HEAD_DIM)
    return pl.pallas_call(
        functools.partial(kernel, chips, tps, seqs),
        out_shape=(pltpu.VMEM((seqs, length, out_cols), BF16),
                   jax.ShapeDtypeStruct((seqs, 2, length), F32)),
        in_specs=[any_spec, any_spec, any_spec, any_spec, vmem, any_spec, vmem],
        out_specs=(any_spec, vmem),
        scratch_shapes=[
            pltpu.VMEM((TOK, HEAD_DIM), F32),
            pltpu.VMEM((TOK, HEAD_DIM), F32),
            pltpu.VMEM((seqs, TOK, model_dim), BF16),
            pltpu.VMEM((model_dim, 256), BF16),
            pltpu.VMEM((model_dim, 256), BF16),
            pltpu.VMEM((model_dim, 256), BF16),
            pltpu.VMEM((channels, out_cols), BF16),
            pltpu.VMEM((seqs, 2, TOK, 256), BF16),
            pltpu.VMEM((seqs, 2, TOK, 128), BF16),
            pltpu.VMEM((seqs, ROWS, 256), BF16),
            pltpu.VMEM((seqs, CHIP, 128), BF16),
            pltpu.VMEM((NBLK, 4, 4, 16, 256), BF16),
            pltpu.VMEM(grid4, BF16),
            pltpu.VMEM((BLK, BLK), BF16),
            pltpu.VMEM((OWN, BLK, BLK + 2 * REACH), F32),
            pltpu.VMEM((OWN, 64, 192), F32),
            pltpu.VMEM((16, 16 * (NBLK - 2)), F32),
            pltpu.VMEM((32, 16 * NBLK), F32),
            pltpu.VMEM(grid4, F32),
            pltpu.VMEM(grid4, F32),
            pltpu.VMEM(grid4, F32),
            pltpu.VMEM(grid4, BF16),
            pltpu.VMEM(grid4, F32),
            pltpu.VMEM((seqs, CHIP, 128), BF16),
            pltpu.VMEM((seqs, 2, 3, 128), F32),
            pltpu.VMEM((seqs, 3, 128), F32),
            pltpu.VMEM((seqs, TOK, channels), BF16),
            pltpu.VMEM((seqs, TOK, out_cols), BF16),
            dma((4 + seqs,)),
            dma((seqs, 2)),
            dma((seqs, 12)),
            dma((seqs, 12)),
            dma((seqs, 16)),
            dma((seqs, 16)),
            dma((seqs,)),
            dma((seqs,)),
            dma((seqs,)),
            dma((seqs,)),
        ],
        compiler_params=pltpu.CompilerParams(
            collective_id=0, has_side_effects=True, vmem_limit_bytes=62 * 1024 * 1024
        ),
    )(tokens, query_weight, key_weight, value_weight, out_gain.reshape(1, channels), out_weight, frequency)


def solution(mesh):
    return jax.shard_map(
        functools.partial(shards, mesh.shape["sp"] // 2, mesh.shape["tp"]),
        mesh=mesh,
        in_specs=(
            P(None, "sp", None),
            P(None, "tp"),
            P(None, "tp"),
            P(None, "tp"),
            P(),
            P(None, "tp"),
        ),
        out_specs=(P(None, "sp", "tp"), P(None, "tp", "sp")),
        check_vma=False,
    )
```

```python
import functools
import math

import jax
import jax.numpy as jnp
from jax import lax
from jax.experimental import pallas as pl
from jax.experimental.pallas import tpu as pltpu
from jax.sharding import PartitionSpec as P

HEAD_DIM = 128
REACH = 64
ROPE_BASE = 10000.0
MASK_FILL = -1e30
NORM_FLOOR = 1e-6
LOG2E = 1.4426950408889634
SCALE = HEAD_DIM ** (-0.5)
RATE = SCALE * LOG2E

TOK = 384
CHIP = 2 * TOK
BLK = 256
WIDE = 1024
HALO = WIDE // BLK
OWN = CHIP // BLK
NBLK = 2 * HALO + OWN
ROWS = NBLK * BLK
MESH = pl.DeviceIdType.MESH
F32 = jnp.float32
BF16 = jnp.bfloat16


def dot_nt(a, b):
    return lax.dot_general(a, b, (((1,), (1,)), ((), ())), preferred_element_type=F32)


def dot(a, b):
    return jnp.dot(a, b, preferred_element_type=F32)


def softened(scores):
    peak = jnp.max(scores, axis=-1, keepdims=True)
    probs = jnp.exp2((scores - peak) * RATE)
    return probs.astype(BF16), peak, jnp.sum(probs, axis=-1, keepdims=True)


def pipelined(jobs):
    ahead = jobs[0][0]()
    for i, (_, finish) in enumerate(jobs):
        now = ahead
        if i + 1 < len(jobs):
            ahead = jobs[i + 1][0]()
        finish(now)


def joined(parts):
    peak = functools.reduce(jnp.maximum, [part[1] for part in parts])
    merged, total = 0.0, 0.0
    for acc_g, peak_g, sum_g in parts:
        share = jnp.exp2((peak_g - peak) * RATE)
        merged = merged + share * acc_g
        total = total + share * sum_g
    return merged, peak, total


def iota(shape, dim):
    return lax.broadcasted_iota(jnp.int32, shape, dim)


def kernel(chips, tps, seqs, tokens, wq, wk, wv, gain_in, wo, out, logs,
           cos, sin, gain, tok_v, wq_v, wkv_v, wo_v, kvown, qown, kvbuf, qbuf, kvp, qp, perm,
           bias1, bias4, bias_mid, bias_out, acc1, peak1, sum1, mperm, lperm, mnat, lnat, lrx, mg, out_v,
           in_sem, loc_sem, kv_send, kv_recv, x_send, x_recv, l_send, l_recv, x_loc, out_sem):
    sp, tp = lax.axis_index("sp"), lax.axis_index("tp")
    chip, core = sp // 2, sp % 2

    def token_load(s):
        return pltpu.make_async_copy(tokens.at[s], tok_v.at[s], in_sem.at[s])

    def pair_loads(h):
        lanes = pl.ds(h * HEAD_DIM, HEAD_DIM)
        return [pltpu.make_async_copy(w.at[:, lanes], wkv_v.at[h, :, pl.ds(i * HEAD_DIM, HEAD_DIM)],
                                      in_sem.at[seqs + 2 * h + i]) for i, w in enumerate((wk, wv))]

    query_load = pltpu.make_async_copy(wq, wq_v, in_sem.at[seqs + 4])
    last_loads = [pltpu.make_async_copy(wo, wo_v, in_sem.at[seqs + 5]),
                  pltpu.make_async_copy(gain_in, gain, in_sem.at[seqs + 6])]
    token_load(0).start()
    for load in pair_loads(0) + pair_loads(1):
        load.start()

    barrier = pltpu.get_barrier_semaphore()
    partners = [(2 * chip + 1 - core, tp)]
    for dx in range(1, tps):
        for c in range(2):
            partners.append((2 * chip + c, (tp + dx) % tps))
    has_left, has_right = chip > 0, chip < chips - 1
    has_far_left, has_far_right = chip > 1, chip < chips - 2
    after, before = jnp.minimum(chip + 1, chips - 1), jnp.maximum(chip - 1, 0)
    for partner in partners:
        pl.semaphore_signal(barrier, inc=1, device_id=partner, device_id_type=MESH)
    for has, neighbour in ((has_left, before), (has_right, after)):
        @pl.when(has)
        def _():
            for c in range(2):
                pl.semaphore_signal(barrier, inc=1, device_id=(2 * neighbour + c, tp), device_id_type=MESH)

    pair = iota((1, HEAD_DIM), 1) % (HEAD_DIM // 2)
    frequency = jnp.exp2(pair.astype(F32) * (-math.log2(ROPE_BASE) / (HEAD_DIM // 2)))
    angles = (sp * TOK + iota((TOK, HEAD_DIM), 0)).astype(F32) * frequency
    cos[...] = jnp.cos(angles)
    sine = jnp.sin(angles)
    sin[...] = jnp.where(iota((TOK, HEAD_DIM), 1) < HEAD_DIM // 2, -sine, sine)

    def row_of(at, size):
        return pl.ds(pl.multiple_of(at, 128), size)

    def remote(src, dst, send, recv, device):
        return pltpu.make_async_remote_copy(src_ref=src, dst_ref=dst, send_sem=send, recv_sem=recv,
                                            device_id=device, device_id_type=MESH)


    def near_sends(s, way):
        copies = []
        base, to = ((BLK, after), (WIDE + CHIP, before))[way]
        for piece, (src, at, size) in enumerate(((128 * core, 512 * core, BLK), (BLK * (1 - core), BLK + 128 * core, 128))):
            for h in range(2):
                copies.append(remote(kvown.at[s, h, row_of(src, size)], kvbuf.at[s, row_of(base + at, size)],
                                     kv_send.at[s, 4 * piece + 2 * h + way],
                                     kv_recv.at[s, 4 * way + 2 * piece + core], (2 * to + h, tp)))
        return copies

    def far_send(s, way):
        src, dst, to = ((WIDE - BLK, 0, after), (WIDE + CHIP, ROWS - BLK, before))[way]
        return remote(kvbuf.at[s, pl.ds(src, BLK)], kvbuf.at[s, pl.ds(dst, BLK)],
                      kv_send.at[s, 8 + way], kv_recv.at[s, 8 + way], (2 * to + core, tp))

    sends_to = (has_right, has_left)
    hears_from = (has_left, has_right)
    hears_far = (has_far_left, has_far_right)

    def start_near(s, which=slice(0, 4)):
        for way in range(2):
            @pl.when(sends_to[way])
            def _():
                for copy in near_sends(s, way)[which]:
                    copy.start()

    def own_sends(s):
        return [remote(kvown.at[s, 1 - core], kvbuf.at[s, row_of(WIDE + TOK * core, TOK)],
                       kv_send.at[s, 10], kv_recv.at[s, 10], (2 * chip + 1 - core, tp)),
                remote(qown.at[s, 1 - core], qbuf.at[s, row_of(TOK * core, TOK)],
                       kv_send.at[s, 11], kv_recv.at[s, 11], (2 * chip + 1 - core, tp))]

    def local_copies(s):
        return [pltpu.make_async_copy(kvown.at[s, core], kvbuf.at[s, row_of(WIDE + TOK * core, TOK)], loc_sem.at[s, 0]),
                pltpu.make_async_copy(qown.at[s, core], qbuf.at[s, row_of(TOK * core, TOK)], loc_sem.at[s, 1])]

    def near_arrival(s, way, piece, c):
        at, size = ((512 * c, BLK), (BLK + 128 * c, 128))[piece]
        at += (BLK, WIDE + CHIP)[way]
        return remote(kvown.at[s, 0, pl.ds(0, size)], kvbuf.at[s, pl.ds(at, size)], kv_send.at[s, 0],
                      kv_recv.at[s, 4 * way + 2 * piece + c], (2 * chip + 1 - core, tp))

    def own_arrivals(s):
        return [remote(kvown.at[s, 0], kvbuf.at[s, row_of(WIDE + TOK * (1 - core), TOK)], kv_send.at[s, 0],
                       kv_recv.at[s, 10], (2 * chip + 1 - core, tp)),
                remote(qown.at[s, 0], qbuf.at[s, row_of(TOK * (1 - core), TOK)], kv_send.at[s, 0],
                       kv_recv.at[s, 11], (2 * chip + 1 - core, tp))]

    head = 2 * tp + core

    def column_of(h):
        return pl.ds(pl.multiple_of(h * HEAD_DIM, HEAD_DIM), HEAD_DIM)

    def piece_of(piece, c):
        return ((BLK * (1 - c), 128), (128 * c, BLK))[piece]

    def x_sends(s, piece):
        copies = []
        for dx in [tps // 2] + [d for d in range(1, tps) if d != tps // 2]:
            for c in range(2) if tps > 1 else ():
                at, size = piece_of(piece, c)
                copies.append(remote(mnat.at[s, pl.ds(TOK * c + at, size)], mg.at[s, pl.ds(at, size), column_of(head)],
                                     x_send.at[s, 8 * piece + 2 * dx + c], x_recv.at[s, 8 * piece + head],
                                     (2 * chip + c, (tp + dx) % tps)))
        at, size = piece_of(piece, 1 - core)
        copies.append(remote(mnat.at[s, row_of(TOK * (1 - core) + at, size)], mg.at[s, row_of(at, size), column_of(head)],
                             x_send.at[s, 8 * piece], x_recv.at[s, 8 * piece + head], (2 * chip + 1 - core, tp)))
        return copies

    def log_send(s):
        return remote(lnat.at[s, 1 - core], lrx.at[s], l_send.at[s], l_recv.at[s], (2 * chip + 1 - core, tp))

    def x_local(s):
        return pltpu.make_async_copy(mnat.at[s, row_of(TOK * core, TOK)], mg.at[s, :, column_of(head)], x_loc.at[s])

    def x_arrivals(s):
        waits = []
        for piece in range(2):
            at, size = piece_of(piece, core)
            for o in range(1, 2 * tps):
                other = (head + o) % (2 * tps)
                waits.append(remote(mnat.at[s, pl.ds(0, size)], mg.at[s, row_of(at, size), column_of(other)],
                                    x_send.at[s, 0], x_recv.at[s, 8 * piece + other], (2 * chip + 1 - core, tp)))
        return waits

    def turned(x):
        return (x * cos[...] + pltpu.roll(x, HEAD_DIM // 2, 1) * sin[...]).astype(BF16)

    def project(s, _):
        token_load(s).wait()
        for h in range(2):
            @pl.when(s == 0)
            def _():
                for load in pair_loads(h):
                    load.wait()
                if h == 1:
                    for t in range(1, seqs):
                        token_load(t).start()
                    for load in last_loads:
                        load.start()
                else:
                    query_load.start()
            both = dot(tok_v[s], wkv_v[h])
            kvown[s, h, :, :HEAD_DIM] = turned(both[:, :HEAD_DIM])
            kvown[s, h, :, HEAD_DIM:] = both[:, HEAD_DIM:].astype(BF16)

            @pl.when(s == 0)
            def _():
                if h == 0:
                    pl.semaphore_wait(barrier, len(partners) + 2 * (jnp.where(has_left, 1, 0) + jnp.where(has_right, 1, 0)))
                    start_near(0, slice(0, 1))
                else:
                    start_near(0, slice(1, 4))
        own_sends(s)[0].start()
        local_copies(s)[0].start()

        @pl.when(s == 0)
        def _():
            query_load.wait()
        queries = dot(tok_v[s], wq_v[...])
        for h in range(2):
            qown[s, h] = turned(queries[:, h * HEAD_DIM:(h + 1) * HEAD_DIM])
        own_sends(s)[1].start()
        local_copies(s)[1].start()
        return 0

    lax.fori_loop(0, seqs, project, 0)
    for load in last_loads:
        load.wait()

    row, col = iota((BLK, BLK), 0), iota((BLK, BLK), 1)
    perm[...] = jnp.where(col == (row % 16) * 16 + row // 16, 1.0, 0.0).astype(BF16)
    first = chip * CHIP
    limit = chips * CHIP
    for b in range(OWN):
        row, col = iota((BLK, BLK + 2 * REACH), 0), iota((BLK, BLK + 2 * REACH), 1)
        gap = (row % 16) * 16 + row // 16 - (col - REACH)
        at = first + b * BLK - REACH + col
        good = (gap >= -REACH) & (gap <= REACH) & (at >= 0) & (at < limit)
        bias1[b] = jnp.where(good, 0.0, MASK_FILL)
        row, col = iota((64, 192), 0), iota((64, 192), 1)
        gap = (row % 16) * 4 + row // 16 - ((col // 64 - 1) * 64 + (col % 16) * 4 + (col % 64) // 16)
        at = first + (b + col // 64 - 1) * BLK
        good = (gap >= -REACH) & (gap <= REACH) & (at >= 0) & (at < limit)
        bias4[b] = jnp.where(good, 0.0, MASK_FILL)
    for ref, q_blocks, k_blocks in ((bias_mid, (1,), range(1, NBLK - 1)), (bias_out, (0, 2), range(NBLK))):
        dims = (16 * len(q_blocks), 16 * len(k_blocks))
        row, col = iota(dims, 0), iota(dims, 1)
        q_at = row % 16 + 16 * (q_blocks[0] + 2 * (row // 16))
        block = col // 16 + k_blocks[0] - HALO
        gap = q_at - (col % 16 + 16 * block)
        at = first + block * BLK
        good = (gap >= -REACH) & (gap <= REACH) & (at >= 0) & (at < limit)
        ref[...] = jnp.where(good, 0.0, MASK_FILL)

    def put_in_order(s, blocks):
        for b in blocks:
            kvp[b] = dot(perm[...], kvbuf[s, pl.ds(b * BLK, BLK), :]).astype(BF16).reshape(4, 4, 16, 2 * HEAD_DIM)

    def near(s):
        for b in range(OWN):
            block = dot(perm[...], qbuf[s, pl.ds(b * BLK, BLK), :]).astype(BF16)
            qp[b] = block.reshape(4, 4, 16, HEAD_DIM)
        put_in_order(s, range(1, NBLK - 1))
        jobs, done = [], {}

        def narrow(b, half):
            around = pl.ds(WIDE + b * BLK - REACH, BLK + 2 * REACH)

            def scores():
                queries = qp[b, 2 * half:2 * half + 2].reshape(128, HEAD_DIM)
                return dot_nt(queries, kvbuf[s, around, :HEAD_DIM]) + bias1[b, half * 128:(half + 1) * 128]

            def finish(scores):
                probs, peak, total = softened(scores)
                done[b, half] = dot(probs, kvbuf[s, around, HEAD_DIM:]), peak, total
            return scores, finish

        def middle(b):
            def scores():
                every = []
                for r in range(4):
                    keys = kvp[b + HALO - 1:b + HALO + 2, :, r, :, :HEAD_DIM].reshape(192, HEAD_DIM)
                    every.append(dot_nt(qp[b, :, r].reshape(64, HEAD_DIM), keys) + bias4[b])
                return every

            def finish(every):
                soft = [softened(scores) for scores in every]
                accs = []
                for r in range(4):
                    values = kvp[b + HALO - 1:b + HALO + 2, :, r, :, HEAD_DIM:].reshape(192, HEAD_DIM)
                    accs.append(dot(soft[r][0], values))
                for a in range(4):
                    for r in range(4):
                        at = (a % 2) * 64 + r * 16
                        one = tuple(x[at:at + 16] for x in done[b, a // 2])
                        two = tuple(x[a * 16:(a + 1) * 16] for x in (accs[r],) + soft[r][1:])
                        acc, peak, total = joined((one, two))
                        acc1[b, a, r] = acc
                        peak1[b, a, r] = jnp.broadcast_to(peak, (16, HEAD_DIM))
                        sum1[b, a, r] = jnp.broadcast_to(total, (16, HEAD_DIM))
            return scores, finish

        pipelined([narrow(1, 0), narrow(1, 1), middle(1)] + [wide(r, (1,), range(1, NBLK - 1), bias_mid) for r in range(4)])
        in_order(s, 1)
        for copy in x_sends(s, 0):
            copy.start()
        for b in (0, 2):
            jobs += [narrow(b, 0), narrow(b, 1), middle(b)]
        pipelined(jobs)

    def wide(r, q_blocks, k_blocks, bias):
        keys_in = slice(k_blocks[0], k_blocks[-1] + 1)

        def scores():
            every = []
            for a in range(4):
                keys = kvp[keys_in, a, r, :, :HEAD_DIM].reshape(16 * len(k_blocks), HEAD_DIM)
                queries = jnp.concatenate([qp[b, a, r] for b in q_blocks], axis=0)
                every.append(dot_nt(queries, keys) + bias[...])
            return every

        def finish(every):
            soft = [softened(scores) for scores in every]
            accs = []
            for a in range(4):
                values = kvp[keys_in, a, r, :, HEAD_DIM:].reshape(16 * len(k_blocks), HEAD_DIM)
                accs.append(dot(soft[a][0], values))
            for a in range(4):
                for i, b in enumerate(q_blocks):
                    one = (acc1[b, a, r], peak1[b, a, r], sum1[b, a, r])
                    two = tuple(x[i * 16:(i + 1) * 16] for x in (accs[a],) + soft[a][1:])
                    merged, peak, total = joined((one, two))
                    mperm[b, a, r] = (merged / total).astype(BF16)
                    lperm[b, a, r] = peak * SCALE + jnp.log(total)
        return scores, finish

    def in_order(s, b):
        mnat[s, pl.ds(b * BLK, BLK), :] = dot(perm[...], mperm[b].reshape(BLK, HEAD_DIM)).astype(BF16)

    def far(s):
        put_in_order(s, (0, NBLK - 1))
        pipelined([wide(r, (0, 2), range(NBLK), bias_out) for r in range(4)])
        for b in (0, 2):
            in_order(s, b)
        for copy in x_sends(s, 1):
            copy.start()
        x_local(s).start()
        for b in range(OWN):
            column = lperm[b].reshape(BLK, HEAD_DIM)
            for half in range(2):
                hit = perm[:, half * 128:(half + 1) * 128].astype(F32)
                line = jnp.sum(jnp.where(hit > 0.5, column, 0.0), axis=0, keepdims=True)
                piece = 2 * b + half
                lnat[s, piece // 3, piece % 3:piece % 3 + 1, :] = line
        log_send(s).start()

    def finish(s):
        x_local(s).wait()
        for copy in x_arrivals(s):
            copy.wait_recv()
        log_send(s).wait_recv()
        lifted = mg[s].astype(F32)
        square = jnp.mean(lifted * lifted, axis=-1, keepdims=True)
        scaled = (lifted * gain[...]).astype(BF16)
        projected = dot(scaled, wo_v[...])
        out_v[s] = (projected * lax.rsqrt(square + NORM_FLOOR)).astype(BF16)
        pltpu.make_async_copy(out_v.at[s], out.at[s], out_sem.at[s]).start()
        mine, theirs = lnat[s, core], lrx[s]
        upper = jnp.where(core == 0, mine, theirs)
        lower = jnp.where(core == 0, theirs, mine)
        for piece in range(3):
            lanes = pl.ds(piece * 128, 128)
            logs[s, 0:1, lanes] = upper[piece:piece + 1]
            logs[s, 1:2, lanes] = lower[piece:piece + 1]

    for has, at, size in ((has_left, BLK, CHIP), (has_far_left, 0, BLK),
                          (has_right, WIDE + CHIP, CHIP), (has_far_right, ROWS - BLK, BLK)):
        @pl.when(jnp.logical_not(has))
        def _():
            def clear(s, _):
                kvbuf[s, pl.ds(at, size), :] = jnp.zeros((size, 2 * HEAD_DIM), BF16)
                return 0
            lax.fori_loop(0, seqs, clear, 0)

    def stage(s, _):
        for way in range(2):
            @pl.when(hears_from[way])
            def _():
                near_arrival(s, way, 0, 1 - way).wait_recv()

            @pl.when(jnp.logical_and(hears_from[way], sends_to[way]))
            def _():
                far_send(s, way).start()

        @pl.when(s + 1 < seqs)
        def _():
            start_near(s + 1)

        for copy in local_copies(s):
            copy.wait()
        for copy in own_arrivals(s):
            copy.wait_recv()
        for way in range(2):
            @pl.when(hears_from[way])
            def _():
                near_arrival(s, way, 0, way).wait_recv()
                for c in range(2):
                    near_arrival(s, way, 1, c).wait_recv()
        near(s)
        for way in range(2):
            @pl.when(hears_far[way])
            def _():
                far_send(s, way).wait_recv()
        far(s)

        @pl.when(s > 0)
        def _():
            finish(s - 1)
        return 0

    lax.fori_loop(0, seqs, stage, 0)
    finish(seqs - 1)

    def drain(s, _):
        for copy in own_sends(s):
            copy.wait_send()
        for way in range(2):
            @pl.when(sends_to[way])
            def _():
                for copy in near_sends(s, way):
                    copy.wait_send()

            @pl.when(jnp.logical_and(hears_from[way], sends_to[way]))
            def _():
                far_send(s, way).wait_send()
        for copy in x_sends(s, 0) + x_sends(s, 1):
            copy.wait_send()
        log_send(s).wait_send()
        pltpu.make_async_copy(out_v.at[s], out.at[s], out_sem.at[s]).wait()
        return 0
    lax.fori_loop(0, seqs, drain, 0)


def shards(chips, tps, tokens, query_weight, key_weight, value_weight, out_gain, out_weight):
    seqs, length, model_dim = tokens.shape
    channels, out_cols = out_weight.shape
    any_spec = pl.BlockSpec(memory_space=pl.ANY)
    vmem = pl.BlockSpec(memory_space=pltpu.VMEM)
    dma = pltpu.SemaphoreType.DMA
    grid4 = (OWN, 4, 4, 16, HEAD_DIM)
    return pl.pallas_call(
        functools.partial(kernel, chips, tps, seqs),
        out_shape=(pltpu.VMEM((seqs, length, out_cols), BF16),
                   jax.ShapeDtypeStruct((seqs, 2, length), F32)),
        in_specs=[any_spec] * 6,
        out_specs=(any_spec, vmem),
        scratch_shapes=[
            pltpu.VMEM((TOK, HEAD_DIM), F32),
            pltpu.VMEM((TOK, HEAD_DIM), F32),
            pltpu.VMEM((1, channels), F32),
            pltpu.VMEM((seqs, TOK, model_dim), BF16),
            pltpu.VMEM((model_dim, 256), BF16),
            pltpu.VMEM((2, model_dim, 256), BF16),
            pltpu.VMEM((channels, out_cols), BF16),
            pltpu.VMEM((seqs, 2, TOK, 256), BF16),
            pltpu.VMEM((seqs, 2, TOK, 128), BF16),
            pltpu.VMEM((seqs, ROWS, 256), BF16),
            pltpu.VMEM((seqs, CHIP, 128), BF16),
            pltpu.VMEM((NBLK, 4, 4, 16, 256), BF16),
            pltpu.VMEM(grid4, BF16),
            pltpu.VMEM((BLK, BLK), BF16),
            pltpu.VMEM((OWN, BLK, BLK + 2 * REACH), F32),
            pltpu.VMEM((OWN, 64, 192), F32),
            pltpu.VMEM((16, 16 * (NBLK - 2)), F32),
            pltpu.VMEM((32, 16 * NBLK), F32),
            pltpu.VMEM(grid4, F32),
            pltpu.VMEM(grid4, F32),
            pltpu.VMEM(grid4, F32),
            pltpu.VMEM(grid4, BF16),
            pltpu.VMEM(grid4, F32),
            pltpu.VMEM((seqs, CHIP, 128), BF16),
            pltpu.VMEM((seqs, 2, 3, 128), F32),
            pltpu.VMEM((seqs, 3, 128), F32),
            pltpu.VMEM((seqs, TOK, channels), BF16),
            pltpu.VMEM((seqs, TOK, out_cols), BF16),
            dma((7 + seqs,)),
            dma((seqs, 2)),
            dma((seqs, 12)),
            dma((seqs, 12)),
            dma((seqs, 16)),
            dma((seqs, 16)),
            dma((seqs,)),
            dma((seqs,)),
            dma((seqs,)),
            dma((seqs,)),
        ],
        compiler_params=pltpu.CompilerParams(
            collective_id=0, has_side_effects=True, vmem_limit_bytes=62 * 1024 * 1024
        ),
    )(tokens, query_weight, key_weight, value_weight, out_gain.reshape(1, channels), out_weight)


def solution(mesh):
    return jax.shard_map(
        functools.partial(shards, mesh.shape["sp"] // 2, mesh.shape["tp"]),
        mesh=mesh,
        in_specs=(
            P(None, "sp", None),
            P(None, "tp"),
            P(None, "tp"),
            P(None, "tp"),
            P(),
            P(None, "tp"),
        ),
        out_specs=(P(None, "sp", "tp"), P(None, "tp", "sp")),
        check_vma=False,
    )
```

```python
import functools
import math

import jax
import jax.numpy as jnp
from jax import lax
from jax.experimental import pallas as pl
from jax.experimental.pallas import tpu as pltpu
from jax.sharding import PartitionSpec as P

HEAD_DIM = 128
REACH = 64
ROPE_BASE = 10000.0
MASK_FILL = -1e30
NORM_FLOOR = 1e-6
LOG2E = 1.4426950408889634
SCALE = HEAD_DIM ** (-0.5)
RATE = SCALE * LOG2E

TOK = 384
CHIP = 2 * TOK
BLK = 256
WIDE = 1024
HALO = WIDE // BLK
OWN = CHIP // BLK
NBLK = 2 * HALO + OWN
ROWS = NBLK * BLK
MESH = pl.DeviceIdType.MESH
F32 = jnp.float32
BF16 = jnp.bfloat16


def dot_nt(a, b):
    return lax.dot_general(a, b, (((1,), (1,)), ((), ())), preferred_element_type=F32)


def dot(a, b):
    return jnp.dot(a, b, preferred_element_type=F32)


def softened(scores):
    peak = jnp.max(scores, axis=-1, keepdims=True)
    probs = jnp.exp2((scores - peak) * RATE)
    return probs.astype(BF16), peak, jnp.sum(probs, axis=-1, keepdims=True)


def pipelined(jobs):
    ahead = jobs[0][0]()
    for i, (_, finish) in enumerate(jobs):
        now = ahead
        if i + 1 < len(jobs):
            ahead = jobs[i + 1][0]()
        finish(now)


def joined(parts):
    peak = functools.reduce(jnp.maximum, [part[1] for part in parts])
    merged, total = 0.0, 0.0
    for acc_g, peak_g, sum_g in parts:
        share = jnp.exp2((peak_g - peak) * RATE)
        merged = merged + share * acc_g
        total = total + share * sum_g
    return merged, peak, total


def iota(shape, dim):
    return lax.broadcasted_iota(jnp.int32, shape, dim)


def kernel(chips, tps, seqs, tokens, wq, wk, wv, gain_in, wo, out, logs,
           cos, sin, gain, tok_v, wq_v, wkv_v, wo_v, kvown, qown, kvbuf, qbuf, kvp, qp, perm,
           bias1, bias4, bias_mid, bias_out, acc1, peak1, sum1, mperm, lperm, mnat, lnat, lrx, mg, out_v,
           in_sem, loc_sem, kv_send, kv_recv, x_send, x_recv, l_send, l_recv, x_loc, out_sem):
    sp, tp = lax.axis_index("sp"), lax.axis_index("tp")
    chip, core = sp // 2, sp % 2

    def token_load(s):
        return pltpu.make_async_copy(tokens.at[s], tok_v.at[s], in_sem.at[s])

    def pair_loads(h):
        lanes = pl.ds(h * HEAD_DIM, HEAD_DIM)
        return [pltpu.make_async_copy(w.at[:, lanes], wkv_v.at[h, :, pl.ds(i * HEAD_DIM, HEAD_DIM)],
                                      in_sem.at[seqs + 2 * h + i]) for i, w in enumerate((wk, wv))]

    query_load = pltpu.make_async_copy(wq, wq_v, in_sem.at[seqs + 4])
    last_loads = [pltpu.make_async_copy(wo, wo_v, in_sem.at[seqs + 5]),
                  pltpu.make_async_copy(gain_in, gain, in_sem.at[seqs + 6])]
    token_load(0).start()
    for load in pair_loads(0) + pair_loads(1):
        load.start()

    barrier = pltpu.get_barrier_semaphore()
    partners = [(2 * chip + 1 - core, tp)]
    for dx in range(1, tps):
        for c in range(2):
            partners.append((2 * chip + c, (tp + dx) % tps))
    has_left, has_right = chip > 0, chip < chips - 1
    has_far_left, has_far_right = chip > 1, chip < chips - 2
    after, before = jnp.minimum(chip + 1, chips - 1), jnp.maximum(chip - 1, 0)
    for partner in partners:
        pl.semaphore_signal(barrier, inc=1, device_id=partner, device_id_type=MESH)
    for has, neighbour in ((has_left, before), (has_right, after)):
        @pl.when(has)
        def _():
            for c in range(2):
                pl.semaphore_signal(barrier, inc=1, device_id=(2 * neighbour + c, tp), device_id_type=MESH)

    pair = iota((1, HEAD_DIM), 1) % (HEAD_DIM // 2)
    frequency = jnp.exp2(pair.astype(F32) * (-math.log2(ROPE_BASE) / (HEAD_DIM // 2)))
    angles = (sp * TOK + iota((TOK, HEAD_DIM), 0)).astype(F32) * frequency
    cos[...] = jnp.cos(angles)
    sine = jnp.sin(angles)
    sin[...] = jnp.where(iota((TOK, HEAD_DIM), 1) < HEAD_DIM // 2, -sine, sine)

    def row_of(at, size):
        return pl.ds(pl.multiple_of(at, 128), size)

    def remote(src, dst, send, recv, device):
        return pltpu.make_async_remote_copy(src_ref=src, dst_ref=dst, send_sem=send, recv_sem=recv,
                                            device_id=device, device_id_type=MESH)


    def near_sends(s, way):
        copies = []
        base, to = ((BLK, after), (WIDE + CHIP, before))[way]
        for piece, (src, at, size) in enumerate(((128 * core, 512 * core, BLK), (BLK * (1 - core), BLK + 128 * core, 128))):
            for h in range(2):
                copies.append(remote(kvown.at[s, h, row_of(src, size)], kvbuf.at[s, row_of(base + at, size)],
                                     kv_send.at[s, 4 * piece + 2 * h + way],
                                     kv_recv.at[s, 4 * way + 2 * piece + core], (2 * to + h, tp)))
        return copies

    def far_send(s, way):
        src, dst, to = ((WIDE - BLK, 0, after), (WIDE + CHIP, ROWS - BLK, before))[way]
        return remote(kvbuf.at[s, pl.ds(src, BLK)], kvbuf.at[s, pl.ds(dst, BLK)],
                      kv_send.at[s, 8 + way], kv_recv.at[s, 8 + way], (2 * to + core, tp))

    sends_to = (has_right, has_left)
    hears_from = (has_left, has_right)
    hears_far = (has_far_left, has_far_right)

    def start_near(s, which=slice(0, 4)):
        for way in range(2):
            @pl.when(sends_to[way])
            def _():
                for copy in near_sends(s, way)[which]:
                    copy.start()

    def own_sends(s):
        return [remote(kvown.at[s, 1 - core], kvbuf.at[s, row_of(WIDE + TOK * core, TOK)],
                       kv_send.at[s, 10], kv_recv.at[s, 10], (2 * chip + 1 - core, tp)),
                remote(qown.at[s, 1 - core], qbuf.at[s, row_of(TOK * core, TOK)],
                       kv_send.at[s, 11], kv_recv.at[s, 11], (2 * chip + 1 - core, tp))]

    def local_copies(s):
        return [pltpu.make_async_copy(kvown.at[s, core], kvbuf.at[s, row_of(WIDE + TOK * core, TOK)], loc_sem.at[s, 0]),
                pltpu.make_async_copy(qown.at[s, core], qbuf.at[s, row_of(TOK * core, TOK)], loc_sem.at[s, 1])]

    def near_arrival(s, way, piece, c):
        at, size = ((512 * c, BLK), (BLK + 128 * c, 128))[piece]
        at += (BLK, WIDE + CHIP)[way]
        return remote(kvown.at[s, 0, pl.ds(0, size)], kvbuf.at[s, pl.ds(at, size)], kv_send.at[s, 0],
                      kv_recv.at[s, 4 * way + 2 * piece + c], (2 * chip + 1 - core, tp))

    def own_arrivals(s):
        return [remote(kvown.at[s, 0], kvbuf.at[s, row_of(WIDE + TOK * (1 - core), TOK)], kv_send.at[s, 0],
                       kv_recv.at[s, 10], (2 * chip + 1 - core, tp)),
                remote(qown.at[s, 0], qbuf.at[s, row_of(TOK * (1 - core), TOK)], kv_send.at[s, 0],
                       kv_recv.at[s, 11], (2 * chip + 1 - core, tp))]

    head = 2 * tp + core

    def column_of(h):
        return pl.ds(pl.multiple_of(h * HEAD_DIM, HEAD_DIM), HEAD_DIM)

    def piece_of(piece, c):
        return ((BLK * (1 - c), 128), (128 * c, BLK))[piece]

    def x_sends(s, piece):
        copies = []
        for dx in [tps // 2] + [d for d in range(1, tps) if d != tps // 2]:
            for c in range(2) if tps > 1 else ():
                at, size = piece_of(piece, c)
                copies.append(remote(mnat.at[s, pl.ds(TOK * c + at, size)], mg.at[s, pl.ds(at, size), column_of(head)],
                                     x_send.at[s, 8 * piece + 2 * dx + c], x_recv.at[s, 8 * piece + head],
                                     (2 * chip + c, (tp + dx) % tps)))
        at, size = piece_of(piece, 1 - core)
        copies.append(remote(mnat.at[s, row_of(TOK * (1 - core) + at, size)], mg.at[s, row_of(at, size), column_of(head)],
                             x_send.at[s, 8 * piece], x_recv.at[s, 8 * piece + head], (2 * chip + 1 - core, tp)))
        return copies

    def log_send(s):
        return remote(lnat.at[s, 1 - core], lrx.at[s], l_send.at[s], l_recv.at[s], (2 * chip + 1 - core, tp))

    def x_local(s):
        return pltpu.make_async_copy(mnat.at[s, row_of(TOK * core, TOK)], mg.at[s, :, column_of(head)], x_loc.at[s])

    def x_arrivals(s):
        waits = []
        for piece in range(2):
            at, size = piece_of(piece, core)
            for o in range(1, 2 * tps):
                other = (head + o) % (2 * tps)
                waits.append(remote(mnat.at[s, pl.ds(0, size)], mg.at[s, row_of(at, size), column_of(other)],
                                    x_send.at[s, 0], x_recv.at[s, 8 * piece + other], (2 * chip + 1 - core, tp)))
        return waits

    def turned(x):
        return (x * cos[...] + pltpu.roll(x, HEAD_DIM // 2, 1) * sin[...]).astype(BF16)

    def project(s, _):
        token_load(s).wait()
        for h in range(2):
            @pl.when(s == 0)
            def _():
                for load in pair_loads(h):
                    load.wait()
                if h == 1:
                    for t in range(1, seqs):
                        token_load(t).start()
                    for load in last_loads:
                        load.start()
                else:
                    query_load.start()
            both = dot(tok_v[s], wkv_v[h])
            kvown[s, h, :, :HEAD_DIM] = turned(both[:, :HEAD_DIM])
            kvown[s, h, :, HEAD_DIM:] = both[:, HEAD_DIM:].astype(BF16)

            @pl.when(s == 0)
            def _():
                if h == 0:
                    pl.semaphore_wait(barrier, len(partners) + 2 * (jnp.where(has_left, 1, 0) + jnp.where(has_right, 1, 0)))
                    start_near(0, slice(0, 1))
                else:
                    start_near(0, slice(1, 4))
        own_sends(s)[0].start()
        local_copies(s)[0].start()

        @pl.when(s == 0)
        def _():
            query_load.wait()
        queries = dot(tok_v[s], wq_v[...])
        for h in range(2):
            qown[s, h] = turned(queries[:, h * HEAD_DIM:(h + 1) * HEAD_DIM])
        own_sends(s)[1].start()
        local_copies(s)[1].start()
        return 0

    lax.fori_loop(0, seqs, project, 0)
    for load in last_loads:
        load.wait()

    row, col = iota((BLK, BLK), 0), iota((BLK, BLK), 1)
    perm[...] = jnp.where(col == (row % 16) * 16 + row // 16, 1.0, 0.0).astype(BF16)
    first = chip * CHIP
    limit = chips * CHIP
    for b in range(OWN):
        row, col = iota((BLK, BLK + 2 * REACH), 0), iota((BLK, BLK + 2 * REACH), 1)
        gap = (row % 16) * 16 + row // 16 - (col - REACH)
        at = first + b * BLK - REACH + col
        good = (gap >= -REACH) & (gap <= REACH) & (at >= 0) & (at < limit)
        bias1[b] = jnp.where(good, 0.0, MASK_FILL)
        row, col = iota((64, 192), 0), iota((64, 192), 1)
        gap = (row % 16) * 4 + row // 16 - ((col // 64 - 1) * 64 + (col % 16) * 4 + (col % 64) // 16)
        at = first + (b + col // 64 - 1) * BLK
        good = (gap >= -REACH) & (gap <= REACH) & (at >= 0) & (at < limit)
        bias4[b] = jnp.where(good, 0.0, MASK_FILL)
    for ref, q_blocks, k_blocks in ((bias_mid, (1,), range(1, NBLK - 1)), (bias_out, (0, 2), range(NBLK))):
        dims = (16 * len(q_blocks), 16 * len(k_blocks))
        row, col = iota(dims, 0), iota(dims, 1)
        q_at = row % 16 + 16 * (q_blocks[0] + 2 * (row // 16))
        block = col // 16 + k_blocks[0] - HALO
        gap = q_at - (col % 16 + 16 * block)
        at = first + block * BLK
        good = (gap >= -REACH) & (gap <= REACH) & (at >= 0) & (at < limit)
        ref[...] = jnp.where(good, 0.0, MASK_FILL)

    def put_in_order(s, blocks):
        for b in blocks:
            kvp[b] = dot(perm[...], kvbuf[s, pl.ds(b * BLK, BLK), :]).astype(BF16).reshape(4, 4, 16, 2 * HEAD_DIM)

    def near(s):
        for b in range(OWN):
            block = dot(perm[...], qbuf[s, pl.ds(b * BLK, BLK), :]).astype(BF16)
            qp[b] = block.reshape(4, 4, 16, HEAD_DIM)
        put_in_order(s, range(1, NBLK - 1))
        jobs, done = [], {}

        def narrow(b, half):
            around = pl.ds(WIDE + b * BLK - REACH, BLK + 2 * REACH)

            def scores():
                queries = qp[b, 2 * half:2 * half + 2].reshape(128, HEAD_DIM)
                return dot_nt(queries, kvbuf[s, around, :HEAD_DIM]) + bias1[b, half * 128:(half + 1) * 128]

            def finish(scores):
                probs, peak, total = softened(scores)
                done[b, half] = dot(probs, kvbuf[s, around, HEAD_DIM:]), peak, total
            return scores, finish

        def middle(b):
            def scores():
                every = []
                for r in range(4):
                    keys = kvp[b + HALO - 1:b + HALO + 2, :, r, :, :HEAD_DIM].reshape(192, HEAD_DIM)
                    every.append(dot_nt(qp[b, :, r].reshape(64, HEAD_DIM), keys) + bias4[b])
                return every

            def finish(every):
                soft = [softened(scores) for scores in every]
                accs = []
                for r in range(4):
                    values = kvp[b + HALO - 1:b + HALO + 2, :, r, :, HEAD_DIM:].reshape(192, HEAD_DIM)
                    accs.append(dot(soft[r][0], values))
                for a in range(4):
                    for r in range(4):
                        at = (a % 2) * 64 + r * 16
                        one = tuple(x[at:at + 16] for x in done[b, a // 2])
                        two = tuple(x[a * 16:(a + 1) * 16] for x in (accs[r],) + soft[r][1:])
                        acc, peak, total = joined((one, two))
                        acc1[b, a, r] = acc
                        peak1[b, a, r] = jnp.broadcast_to(peak, (16, HEAD_DIM))
                        sum1[b, a, r] = jnp.broadcast_to(total, (16, HEAD_DIM))
            return scores, finish

        pipelined([narrow(1, 0), narrow(1, 1), middle(1)] + [wide(r, (1,), range(1, NBLK - 1), bias_mid) for r in range(4)])
        in_order(s, 1)
        for copy in x_sends(s, 0):
            copy.start()
        for b in (0, 2):
            jobs += [narrow(b, 0), narrow(b, 1), middle(b)]
        pipelined(jobs)

    def wide(r, q_blocks, k_blocks, bias):
        keys_in = slice(k_blocks[0], k_blocks[-1] + 1)

        def scores():
            every = []
            for a in range(4):
                keys = kvp[keys_in, a, r, :, :HEAD_DIM].reshape(16 * len(k_blocks), HEAD_DIM)
                queries = jnp.concatenate([qp[b, a, r] for b in q_blocks], axis=0)
                every.append(dot_nt(queries, keys) + bias[...])
            return every

        def finish(every):
            soft = [softened(scores) for scores in every]
            accs = []
            for a in range(4):
                values = kvp[keys_in, a, r, :, HEAD_DIM:].reshape(16 * len(k_blocks), HEAD_DIM)
                accs.append(dot(soft[a][0], values))
            for a in range(4):
                for i, b in enumerate(q_blocks):
                    one = (acc1[b, a, r], peak1[b, a, r], sum1[b, a, r])
                    two = tuple(x[i * 16:(i + 1) * 16] for x in (accs[a],) + soft[a][1:])
                    merged, peak, total = joined((one, two))
                    mperm[b, a, r] = (merged / total).astype(BF16)
                    lperm[b, a, r] = peak * SCALE + jnp.log(total)
        return scores, finish

    def in_order(s, b):
        mnat[s, pl.ds(b * BLK, BLK), :] = dot(perm[...], mperm[b].reshape(BLK, HEAD_DIM)).astype(BF16)

    def far(s):
        put_in_order(s, (0, NBLK - 1))
        pipelined([wide(r, (0, 2), range(NBLK), bias_out) for r in range(4)])
        for b in (0, 2):
            in_order(s, b)
        for copy in x_sends(s, 1):
            copy.start()
        x_local(s).start()
        for b in range(OWN):
            column = lperm[b].reshape(BLK, HEAD_DIM)
            for half in range(2):
                hit = perm[:, half * 128:(half + 1) * 128].astype(F32)
                line = jnp.sum(jnp.where(hit > 0.5, column, 0.0), axis=0, keepdims=True)
                piece = 2 * b + half
                lnat[s, piece // 3, piece % 3:piece % 3 + 1, :] = line
        log_send(s).start()

    def finish(s):
        x_local(s).wait()
        for copy in x_arrivals(s):
            copy.wait_recv()
        log_send(s).wait_recv()
        lifted = mg[s].astype(F32)
        square = jnp.mean(lifted * lifted, axis=-1, keepdims=True)
        scaled = (lifted * gain[...]).astype(BF16)
        projected = dot(scaled, wo_v[...])
        out_v[s] = (projected * lax.rsqrt(square + NORM_FLOOR)).astype(BF16)
        pltpu.make_async_copy(out_v.at[s], out.at[s], out_sem.at[s]).start()
        mine, theirs = lnat[s, core], lrx[s]
        upper = jnp.where(core == 0, mine, theirs)
        lower = jnp.where(core == 0, theirs, mine)
        for piece in range(3):
            lanes = pl.ds(piece * 128, 128)
            logs[s, 0:1, lanes] = upper[piece:piece + 1]
            logs[s, 1:2, lanes] = lower[piece:piece + 1]

    for has, at, size in ((has_left, BLK, CHIP), (has_far_left, 0, BLK),
                          (has_right, WIDE + CHIP, CHIP), (has_far_right, ROWS - BLK, BLK)):
        @pl.when(jnp.logical_not(has))
        def _():
            def clear(s, _):
                kvbuf[s, pl.ds(at, size), :] = jnp.zeros((size, 2 * HEAD_DIM), BF16)
                return 0
            lax.fori_loop(0, seqs, clear, 0)

    def stage(s, _):
        @pl.when(s + 1 < seqs)
        def _():
            start_near(s + 1, slice(0, 1))

        for way in range(2):
            @pl.when(hears_from[way])
            def _():
                near_arrival(s, way, 0, 1 - way).wait_recv()

            @pl.when(jnp.logical_and(hears_from[way], sends_to[way]))
            def _():
                far_send(s, way).start()

        @pl.when(s + 1 < seqs)
        def _():
            start_near(s + 1, slice(1, 4))

        for copy in local_copies(s):
            copy.wait()
        for copy in own_arrivals(s):
            copy.wait_recv()
        for way in range(2):
            @pl.when(hears_from[way])
            def _():
                near_arrival(s, way, 0, way).wait_recv()
                for c in range(2):
                    near_arrival(s, way, 1, c).wait_recv()
        near(s)
        for way in range(2):
            @pl.when(hears_far[way])
            def _():
                far_send(s, way).wait_recv()
        far(s)

        @pl.when(s > 0)
        def _():
            finish(s - 1)
        return 0

    lax.fori_loop(0, seqs, stage, 0)
    finish(seqs - 1)

    def drain(s, _):
        for copy in own_sends(s):
            copy.wait_send()
        for way in range(2):
            @pl.when(sends_to[way])
            def _():
                for copy in near_sends(s, way):
                    copy.wait_send()

            @pl.when(jnp.logical_and(hears_from[way], sends_to[way]))
            def _():
                far_send(s, way).wait_send()
        for copy in x_sends(s, 0) + x_sends(s, 1):
            copy.wait_send()
        log_send(s).wait_send()
        pltpu.make_async_copy(out_v.at[s], out.at[s], out_sem.at[s]).wait()
        return 0
    lax.fori_loop(0, seqs, drain, 0)


def shards(chips, tps, tokens, query_weight, key_weight, value_weight, out_gain, out_weight):
    seqs, length, model_dim = tokens.shape
    channels, out_cols = out_weight.shape
    any_spec = pl.BlockSpec(memory_space=pl.ANY)
    vmem = pl.BlockSpec(memory_space=pltpu.VMEM)
    dma = pltpu.SemaphoreType.DMA
    grid4 = (OWN, 4, 4, 16, HEAD_DIM)
    return pl.pallas_call(
        functools.partial(kernel, chips, tps, seqs),
        out_shape=(pltpu.VMEM((seqs, length, out_cols), BF16),
                   jax.ShapeDtypeStruct((seqs, 2, length), F32)),
        in_specs=[any_spec] * 6,
        out_specs=(any_spec, vmem),
        scratch_shapes=[
            pltpu.VMEM((TOK, HEAD_DIM), F32),
            pltpu.VMEM((TOK, HEAD_DIM), F32),
            pltpu.VMEM((1, channels), F32),
            pltpu.VMEM((seqs, TOK, model_dim), BF16),
            pltpu.VMEM((model_dim, 256), BF16),
            pltpu.VMEM((2, model_dim, 256), BF16),
            pltpu.VMEM((channels, out_cols), BF16),
            pltpu.VMEM((seqs, 2, TOK, 256), BF16),
            pltpu.VMEM((seqs, 2, TOK, 128), BF16),
            pltpu.VMEM((seqs, ROWS, 256), BF16),
            pltpu.VMEM((seqs, CHIP, 128), BF16),
            pltpu.VMEM((NBLK, 4, 4, 16, 256), BF16),
            pltpu.VMEM(grid4, BF16),
            pltpu.VMEM((BLK, BLK), BF16),
            pltpu.VMEM((OWN, BLK, BLK + 2 * REACH), F32),
            pltpu.VMEM((OWN, 64, 192), F32),
            pltpu.VMEM((16, 16 * (NBLK - 2)), F32),
            pltpu.VMEM((32, 16 * NBLK), F32),
            pltpu.VMEM(grid4, F32),
            pltpu.VMEM(grid4, F32),
            pltpu.VMEM(grid4, F32),
            pltpu.VMEM(grid4, BF16),
            pltpu.VMEM(grid4, F32),
            pltpu.VMEM((seqs, CHIP, 128), BF16),
            pltpu.VMEM((seqs, 2, 3, 128), F32),
            pltpu.VMEM((seqs, 3, 128), F32),
            pltpu.VMEM((seqs, TOK, channels), BF16),
            pltpu.VMEM((seqs, TOK, out_cols), BF16),
            dma((7 + seqs,)),
            dma((seqs, 2)),
            dma((seqs, 12)),
            dma((seqs, 12)),
            dma((seqs, 16)),
            dma((seqs, 16)),
            dma((seqs,)),
            dma((seqs,)),
            dma((seqs,)),
            dma((seqs,)),
        ],
        compiler_params=pltpu.CompilerParams(
            collective_id=0, has_side_effects=True, vmem_limit_bytes=62 * 1024 * 1024
        ),
    )(tokens, query_weight, key_weight, value_weight, out_gain.reshape(1, channels), out_weight)


def solution(mesh):
    return jax.shard_map(
        functools.partial(shards, mesh.shape["sp"] // 2, mesh.shape["tp"]),
        mesh=mesh,
        in_specs=(
            P(None, "sp", None),
            P(None, "tp"),
            P(None, "tp"),
            P(None, "tp"),
            P(),
            P(None, "tp"),
        ),
        out_specs=(P(None, "sp", "tp"), P(None, "tp", "sp")),
        check_vma=False,
    )
```

```python
import functools
import math

import jax
import jax.numpy as jnp
from jax import lax
from jax.experimental import pallas as pl
from jax.experimental.pallas import tpu as pltpu
from jax.sharding import PartitionSpec as P

HEAD_DIM = 128
REACH = 64
ROPE_BASE = 10000.0
MASK_FILL = -1e30
NORM_FLOOR = 1e-6
LOG2E = 1.4426950408889634
SCALE = HEAD_DIM ** (-0.5)
RATE = SCALE * LOG2E

TOK = 384
CHIP = 2 * TOK
BLK = 256
WIDE = 1024
HALO = WIDE // BLK
OWN = CHIP // BLK
NBLK = 2 * HALO + OWN
ROWS = NBLK * BLK
HAND_OVER = 1024 * 1024
MESH = pl.DeviceIdType.MESH
F32 = jnp.float32
BF16 = jnp.bfloat16


def dot_nt(a, b):
    return lax.dot_general(a, b, (((1,), (1,)), ((), ())), preferred_element_type=F32)


def dot(a, b):
    return jnp.dot(a, b, preferred_element_type=F32)


def softened(scores):
    peak = jnp.max(scores, axis=-1, keepdims=True)
    probs = jnp.exp2((scores - peak) * RATE)
    return probs.astype(BF16), peak, jnp.sum(probs, axis=-1, keepdims=True)


def pipelined(jobs):
    ahead = jobs[0][0]()
    for i, (_, finish) in enumerate(jobs):
        now = ahead
        if i + 1 < len(jobs):
            ahead = jobs[i + 1][0]()
        finish(now)


def joined(parts):
    peak = functools.reduce(jnp.maximum, [part[1] for part in parts])
    merged, total = 0.0, 0.0
    for acc_g, peak_g, sum_g in parts:
        share = jnp.exp2((peak_g - peak) * RATE)
        merged = merged + share * acc_g
        total = total + share * sum_g
    return merged, peak, total


def iota(shape, dim):
    return lax.broadcasted_iota(jnp.int32, shape, dim)


def kernel(chips, tps, seqs, tokens, wq, wk, wv, gain_in, wo, out, logs,
           cos, sin, gain, tok_v, wq_v, wkv_v, wo_v, kvown, qown, kvbuf, qbuf, kvp, qp, perm,
           bias1, bias4, bias_mid, bias_out, acc1, peak1, sum1, mperm, lperm, mnat, lnat, lrx, mg,
           in_sem, loc_sem, kv_send, kv_recv, x_send, x_recv, l_send, l_recv, x_loc):
    sp, tp = lax.axis_index("sp"), lax.axis_index("tp")
    chip, core = sp // 2, sp % 2

    def token_load(s):
        return pltpu.make_async_copy(tokens.at[s], tok_v.at[s], in_sem.at[s])

    def pair_loads(h):
        lanes = pl.ds(h * HEAD_DIM, HEAD_DIM)
        return [pltpu.make_async_copy(w.at[:, lanes], wkv_v.at[h, :, pl.ds(i * HEAD_DIM, HEAD_DIM)],
                                      in_sem.at[seqs + 2 * h + i]) for i, w in enumerate((wk, wv))]

    query_load = pltpu.make_async_copy(wq, wq_v, in_sem.at[seqs + 4])
    last_loads = [pltpu.make_async_copy(wo, wo_v, in_sem.at[seqs + 5]),
                  pltpu.make_async_copy(gain_in, gain, in_sem.at[seqs + 6])]
    token_load(0).start()
    for load in pair_loads(0) + pair_loads(1):
        load.start()

    barrier = pltpu.get_barrier_semaphore()
    partners = [(2 * chip + 1 - core, tp)]
    for dx in range(1, tps):
        for c in range(2):
            partners.append((2 * chip + c, (tp + dx) % tps))
    has_left, has_right = chip > 0, chip < chips - 1
    has_far_left, has_far_right = chip > 1, chip < chips - 2
    after, before = jnp.minimum(chip + 1, chips - 1), jnp.maximum(chip - 1, 0)
    for partner in partners:
        pl.semaphore_signal(barrier, inc=1, device_id=partner, device_id_type=MESH)
    for has, neighbour in ((has_left, before), (has_right, after)):
        @pl.when(has)
        def _():
            for c in range(2):
                pl.semaphore_signal(barrier, inc=1, device_id=(2 * neighbour + c, tp), device_id_type=MESH)

    pair = iota((1, HEAD_DIM), 1) % (HEAD_DIM // 2)
    frequency = jnp.exp2(pair.astype(F32) * (-math.log2(ROPE_BASE) / (HEAD_DIM // 2)))
    angles = (sp * TOK + iota((TOK, HEAD_DIM), 0)).astype(F32) * frequency
    cos[...] = jnp.cos(angles)
    sine = jnp.sin(angles)
    sin[...] = jnp.where(iota((TOK, HEAD_DIM), 1) < HEAD_DIM // 2, -sine, sine)

    def row_of(at, size):
        return pl.ds(pl.multiple_of(at, 128), size)

    def remote(src, dst, send, recv, device):
        return pltpu.make_async_remote_copy(src_ref=src, dst_ref=dst, send_sem=send, recv_sem=recv,
                                            device_id=device, device_id_type=MESH)


    def near_sends(s, way):
        copies = []
        base, to = ((BLK, after), (WIDE + CHIP, before))[way]
        for piece, (src, at, size) in enumerate(((128 * core, 512 * core, BLK), (BLK * (1 - core), BLK + 128 * core, 128))):
            for h in range(2):
                copies.append(remote(kvown.at[s, h, row_of(src, size)], kvbuf.at[s, row_of(base + at, size)],
                                     kv_send.at[s, 4 * piece + 2 * h + way],
                                     kv_recv.at[s, 4 * way + 2 * piece + core], (2 * to + h, tp)))
        return copies

    def far_send(s, way):
        src, dst, to = ((WIDE - BLK, 0, after), (WIDE + CHIP, ROWS - BLK, before))[way]
        return remote(kvbuf.at[s, pl.ds(src, BLK)], kvbuf.at[s, pl.ds(dst, BLK)],
                      kv_send.at[s, 8 + way], kv_recv.at[s, 8 + way], (2 * to + core, tp))

    sends_to = (has_right, has_left)
    hears_from = (has_left, has_right)
    hears_far = (has_far_left, has_far_right)

    def start_near(s, which=slice(0, 4)):
        for way in range(2):
            @pl.when(sends_to[way])
            def _():
                for copy in near_sends(s, way)[which]:
                    copy.start()

    def own_sends(s):
        return [remote(kvown.at[s, 1 - core], kvbuf.at[s, row_of(WIDE + TOK * core, TOK)],
                       kv_send.at[s, 10], kv_recv.at[s, 10], (2 * chip + 1 - core, tp)),
                remote(qown.at[s, 1 - core], qbuf.at[s, row_of(TOK * core, TOK)],
                       kv_send.at[s, 11], kv_recv.at[s, 11], (2 * chip + 1 - core, tp))]

    def local_copies(s):
        return [pltpu.make_async_copy(kvown.at[s, core], kvbuf.at[s, row_of(WIDE + TOK * core, TOK)], loc_sem.at[s, 0]),
                pltpu.make_async_copy(qown.at[s, core], qbuf.at[s, row_of(TOK * core, TOK)], loc_sem.at[s, 1])]

    def near_arrival(s, way, piece, c):
        at, size = ((512 * c, BLK), (BLK + 128 * c, 128))[piece]
        at += (BLK, WIDE + CHIP)[way]
        return remote(kvown.at[s, 0, pl.ds(0, size)], kvbuf.at[s, pl.ds(at, size)], kv_send.at[s, 0],
                      kv_recv.at[s, 4 * way + 2 * piece + c], (2 * chip + 1 - core, tp))

    def own_arrivals(s):
        return [remote(kvown.at[s, 0], kvbuf.at[s, row_of(WIDE + TOK * (1 - core), TOK)], kv_send.at[s, 0],
                       kv_recv.at[s, 10], (2 * chip + 1 - core, tp)),
                remote(qown.at[s, 0], qbuf.at[s, row_of(TOK * (1 - core), TOK)], kv_send.at[s, 0],
                       kv_recv.at[s, 11], (2 * chip + 1 - core, tp))]

    head = 2 * tp + core

    def column_of(h):
        return pl.ds(pl.multiple_of(h * HEAD_DIM, HEAD_DIM), HEAD_DIM)

    def piece_of(piece, c):
        return ((BLK * (1 - c), 128), (128 * c, BLK))[piece]

    def x_sends(s, piece):
        copies = []
        for dx in [tps // 2] + [d for d in range(1, tps) if d != tps // 2]:
            for c in range(2) if tps > 1 else ():
                at, size = piece_of(piece, c)
                copies.append(remote(mnat.at[s, pl.ds(TOK * c + at, size)], mg.at[s, pl.ds(at, size), column_of(head)],
                                     x_send.at[s, 8 * piece + 2 * dx + c], x_recv.at[s, 8 * piece + head],
                                     (2 * chip + c, (tp + dx) % tps)))
        at, size = piece_of(piece, 1 - core)
        copies.append(remote(mnat.at[s, row_of(TOK * (1 - core) + at, size)], mg.at[s, row_of(at, size), column_of(head)],
                             x_send.at[s, 8 * piece], x_recv.at[s, 8 * piece + head], (2 * chip + 1 - core, tp)))
        return copies

    def log_send(s):
        return remote(lnat.at[s, 1 - core], lrx.at[s], l_send.at[s], l_recv.at[s], (2 * chip + 1 - core, tp))

    def x_local(s):
        return pltpu.make_async_copy(mnat.at[s, row_of(TOK * core, TOK)], mg.at[s, :, column_of(head)], x_loc.at[s])

    def x_arrivals(s):
        waits = []
        for piece in range(2):
            at, size = piece_of(piece, core)
            for o in range(1, 2 * tps):
                other = (head + o) % (2 * tps)
                waits.append(remote(mnat.at[s, pl.ds(0, size)], mg.at[s, row_of(at, size), column_of(other)],
                                    x_send.at[s, 0], x_recv.at[s, 8 * piece + other], (2 * chip + 1 - core, tp)))
        return waits

    def turned(x):
        return (x * cos[...] + pltpu.roll(x, HEAD_DIM // 2, 1) * sin[...]).astype(BF16)

    def project(s, _):
        token_load(s).wait()
        for h in range(2):
            @pl.when(s == 0)
            def _():
                for load in pair_loads(h):
                    load.wait()
                if h == 1:
                    for t in range(1, seqs):
                        token_load(t).start()
                    for load in last_loads:
                        load.start()
                else:
                    query_load.start()
            both = dot(tok_v[s], wkv_v[h])
            kvown[s, h, :, :HEAD_DIM] = turned(both[:, :HEAD_DIM])
            kvown[s, h, :, HEAD_DIM:] = both[:, HEAD_DIM:].astype(BF16)

            @pl.when(s == 0)
            def _():
                if h == 0:
                    pl.semaphore_wait(barrier, len(partners) + 2 * (jnp.where(has_left, 1, 0) + jnp.where(has_right, 1, 0)))
                    start_near(0, slice(0, 1))
                else:
                    start_near(0, slice(1, 4))
        own_sends(s)[0].start()
        local_copies(s)[0].start()

        @pl.when(s == 0)
        def _():
            query_load.wait()
        queries = dot(tok_v[s], wq_v[...])
        for h in range(2):
            qown[s, h] = turned(queries[:, h * HEAD_DIM:(h + 1) * HEAD_DIM])
        own_sends(s)[1].start()
        local_copies(s)[1].start()
        return 0

    lax.fori_loop(0, seqs, project, 0)
    for load in last_loads:
        load.wait()

    row, col = iota((BLK, BLK), 0), iota((BLK, BLK), 1)
    perm[...] = jnp.where(col == (row % 16) * 16 + row // 16, 1.0, 0.0).astype(BF16)
    first = chip * CHIP
    limit = chips * CHIP
    for b in range(OWN):
        row, col = iota((BLK, BLK + 2 * REACH), 0), iota((BLK, BLK + 2 * REACH), 1)
        gap = (row % 16) * 16 + row // 16 - (col - REACH)
        at = first + b * BLK - REACH + col
        good = (gap >= -REACH) & (gap <= REACH) & (at >= 0) & (at < limit)
        bias1[b] = jnp.where(good, 0.0, MASK_FILL)
        row, col = iota((64, 192), 0), iota((64, 192), 1)
        gap = (row % 16) * 4 + row // 16 - ((col // 64 - 1) * 64 + (col % 16) * 4 + (col % 64) // 16)
        at = first + (b + col // 64 - 1) * BLK
        good = (gap >= -REACH) & (gap <= REACH) & (at >= 0) & (at < limit)
        bias4[b] = jnp.where(good, 0.0, MASK_FILL)
    for ref, q_blocks, k_blocks in ((bias_mid, (1,), range(1, NBLK - 1)), (bias_out, (0, 2), range(NBLK))):
        dims = (16 * len(q_blocks), 16 * len(k_blocks))
        row, col = iota(dims, 0), iota(dims, 1)
        q_at = row % 16 + 16 * (q_blocks[0] + 2 * (row // 16))
        block = col // 16 + k_blocks[0] - HALO
        gap = q_at - (col % 16 + 16 * block)
        at = first + block * BLK
        good = (gap >= -REACH) & (gap <= REACH) & (at >= 0) & (at < limit)
        ref[...] = jnp.where(good, 0.0, MASK_FILL)

    def put_in_order(s, blocks):
        for b in blocks:
            kvp[b] = dot(perm[...], kvbuf[s, pl.ds(b * BLK, BLK), :]).astype(BF16).reshape(4, 4, 16, 2 * HEAD_DIM)

    def near(s):
        for b in range(OWN):
            block = dot(perm[...], qbuf[s, pl.ds(b * BLK, BLK), :]).astype(BF16)
            qp[b] = block.reshape(4, 4, 16, HEAD_DIM)
        put_in_order(s, range(1, NBLK - 1))
        jobs, done = [], {}

        def narrow(b, half):
            around = pl.ds(WIDE + b * BLK - REACH, BLK + 2 * REACH)

            def scores():
                queries = qp[b, 2 * half:2 * half + 2].reshape(128, HEAD_DIM)
                return dot_nt(queries, kvbuf[s, around, :HEAD_DIM]) + bias1[b, half * 128:(half + 1) * 128]

            def finish(scores):
                probs, peak, total = softened(scores)
                done[b, half] = dot(probs, kvbuf[s, around, HEAD_DIM:]), peak, total
            return scores, finish

        def middle(b):
            def scores():
                every = []
                for r in range(4):
                    keys = kvp[b + HALO - 1:b + HALO + 2, :, r, :, :HEAD_DIM].reshape(192, HEAD_DIM)
                    every.append(dot_nt(qp[b, :, r].reshape(64, HEAD_DIM), keys) + bias4[b])
                return every

            def finish(every):
                soft = [softened(scores) for scores in every]
                accs = []
                for r in range(4):
                    values = kvp[b + HALO - 1:b + HALO + 2, :, r, :, HEAD_DIM:].reshape(192, HEAD_DIM)
                    accs.append(dot(soft[r][0], values))
                for a in range(4):
                    for r in range(4):
                        at = (a % 2) * 64 + r * 16
                        one = tuple(x[at:at + 16] for x in done[b, a // 2])
                        two = tuple(x[a * 16:(a + 1) * 16] for x in (accs[r],) + soft[r][1:])
                        acc, peak, total = joined((one, two))
                        acc1[b, a, r] = acc
                        peak1[b, a, r] = jnp.broadcast_to(peak, (16, HEAD_DIM))
                        sum1[b, a, r] = jnp.broadcast_to(total, (16, HEAD_DIM))
            return scores, finish

        pipelined([narrow(1, 0), narrow(1, 1), middle(1)] + [wide(r, (1,), range(1, NBLK - 1), bias_mid) for r in range(4)])
        in_order(s, 1)
        for copy in x_sends(s, 0):
            copy.start()
        for b in (0, 2):
            jobs += [narrow(b, 0), narrow(b, 1), middle(b)]
        pipelined(jobs)

    def wide(r, q_blocks, k_blocks, bias):
        keys_in = slice(k_blocks[0], k_blocks[-1] + 1)

        def scores():
            every = []
            for a in range(4):
                keys = kvp[keys_in, a, r, :, :HEAD_DIM].reshape(16 * len(k_blocks), HEAD_DIM)
                queries = jnp.concatenate([qp[b, a, r] for b in q_blocks], axis=0)
                every.append(dot_nt(queries, keys) + bias[...])
            return every

        def finish(every):
            soft = [softened(scores) for scores in every]
            accs = []
            for a in range(4):
                values = kvp[keys_in, a, r, :, HEAD_DIM:].reshape(16 * len(k_blocks), HEAD_DIM)
                accs.append(dot(soft[a][0], values))
            for a in range(4):
                for i, b in enumerate(q_blocks):
                    one = (acc1[b, a, r], peak1[b, a, r], sum1[b, a, r])
                    two = tuple(x[i * 16:(i + 1) * 16] for x in (accs[a],) + soft[a][1:])
                    merged, peak, total = joined((one, two))
                    mperm[b, a, r] = (merged / total).astype(BF16)
                    lperm[b, a, r] = peak * SCALE + jnp.log(total)
        return scores, finish

    def in_order(s, b):
        mnat[s, pl.ds(b * BLK, BLK), :] = dot(perm[...], mperm[b].reshape(BLK, HEAD_DIM)).astype(BF16)

    def far(s):
        put_in_order(s, (0, NBLK - 1))
        pipelined([wide(r, (0, 2), range(NBLK), bias_out) for r in range(4)])
        for b in (0, 2):
            in_order(s, b)
        for copy in x_sends(s, 1):
            copy.start()
        x_local(s).start()
        for b in range(OWN):
            column = lperm[b].reshape(BLK, HEAD_DIM)
            for half in range(2):
                hit = perm[:, half * 128:(half + 1) * 128].astype(F32)
                line = jnp.sum(jnp.where(hit > 0.5, column, 0.0), axis=0, keepdims=True)
                piece = 2 * b + half
                lnat[s, piece // 3, piece % 3:piece % 3 + 1, :] = line
        log_send(s).start()

    def finish(s):
        x_local(s).wait()
        for copy in x_arrivals(s):
            copy.wait_recv()
        log_send(s).wait_recv()
        lifted = mg[s].astype(F32)
        square = jnp.mean(lifted * lifted, axis=-1, keepdims=True)
        scaled = (lifted * gain[...]).astype(BF16)
        projected = dot(scaled, wo_v[...])
        out[s] = (projected * lax.rsqrt(square + NORM_FLOOR)).astype(BF16)
        mine, theirs = lnat[s, core], lrx[s]
        upper = jnp.where(core == 0, mine, theirs)
        lower = jnp.where(core == 0, theirs, mine)
        for piece in range(3):
            lanes = pl.ds(piece * 128, 128)
            logs[s, 0:1, lanes] = upper[piece:piece + 1]
            logs[s, 1:2, lanes] = lower[piece:piece + 1]

    for has, at, size in ((has_left, BLK, CHIP), (has_far_left, 0, BLK),
                          (has_right, WIDE + CHIP, CHIP), (has_far_right, ROWS - BLK, BLK)):
        @pl.when(jnp.logical_not(has))
        def _():
            def clear(s, _):
                kvbuf[s, pl.ds(at, size), :] = jnp.zeros((size, 2 * HEAD_DIM), BF16)
                return 0
            lax.fori_loop(0, seqs, clear, 0)

    def stage(s, _):
        for way in range(2):
            @pl.when(hears_from[way])
            def _():
                near_arrival(s, way, 0, 1 - way).wait_recv()

            @pl.when(jnp.logical_and(hears_from[way], sends_to[way]))
            def _():
                far_send(s, way).start()

        @pl.when(s + 1 < seqs)
        def _():
            start_near(s + 1)

        for copy in local_copies(s):
            copy.wait()
        for copy in own_arrivals(s):
            copy.wait_recv()
        for way in range(2):
            @pl.when(hears_from[way])
            def _():
                near_arrival(s, way, 0, way).wait_recv()
                for c in range(2):
                    near_arrival(s, way, 1, c).wait_recv()
        near(s)
        for way in range(2):
            @pl.when(hears_far[way])
            def _():
                far_send(s, way).wait_recv()
        far(s)

        @pl.when(s > 0)
        def _():
            finish(s - 1)
        return 0

    lax.fori_loop(0, seqs, stage, 0)
    finish(seqs - 1)

    def drain(s, _):
        for copy in own_sends(s):
            copy.wait_send()
        for way in range(2):
            @pl.when(sends_to[way])
            def _():
                for copy in near_sends(s, way):
                    copy.wait_send()

            @pl.when(jnp.logical_and(hears_from[way], sends_to[way]))
            def _():
                far_send(s, way).wait_send()
        for copy in x_sends(s, 0) + x_sends(s, 1):
            copy.wait_send()
        log_send(s).wait_send()
        return 0
    lax.fori_loop(0, seqs, drain, 0)


def hand_over(mixed, logs, out, out_logs, sem):
    seqs = mixed.shape[0]
    copies = [pltpu.make_async_copy(mixed.at[s], out.at[s], sem.at[s]) for s in range(seqs)]
    copies.append(pltpu.make_async_copy(logs, out_logs, sem.at[seqs]))
    for copy in copies:
        copy.start()
    for copy in copies:
        copy.wait()


def shards(chips, tps, tokens, query_weight, key_weight, value_weight, out_gain, out_weight):
    seqs, length, model_dim = tokens.shape
    channels, out_cols = out_weight.shape
    any_spec = pl.BlockSpec(memory_space=pl.ANY)
    vmem = pl.BlockSpec(memory_space=pltpu.VMEM)
    dma = pltpu.SemaphoreType.DMA
    grid4 = (OWN, 4, 4, 16, HEAD_DIM)
    mixed, logs = pl.pallas_call(
        functools.partial(kernel, chips, tps, seqs),
        out_shape=(pltpu.VMEM((seqs, length, out_cols), BF16),
                   pltpu.VMEM((seqs, 2, length), F32)),
        in_specs=[any_spec] * 6,
        out_specs=(vmem, vmem),
        scratch_shapes=[
            pltpu.VMEM((TOK, HEAD_DIM), F32),
            pltpu.VMEM((TOK, HEAD_DIM), F32),
            pltpu.VMEM((1, channels), F32),
            pltpu.VMEM((seqs, TOK, model_dim), BF16),
            pltpu.VMEM((model_dim, 256), BF16),
            pltpu.VMEM((2, model_dim, 256), BF16),
            pltpu.VMEM((channels, out_cols), BF16),
            pltpu.VMEM((seqs, 2, TOK, 256), BF16),
            pltpu.VMEM((seqs, 2, TOK, 128), BF16),
            pltpu.VMEM((seqs, ROWS, 256), BF16),
            pltpu.VMEM((seqs, CHIP, 128), BF16),
            pltpu.VMEM((NBLK, 4, 4, 16, 256), BF16),
            pltpu.VMEM(grid4, BF16),
            pltpu.VMEM((BLK, BLK), BF16),
            pltpu.VMEM((OWN, BLK, BLK + 2 * REACH), F32),
            pltpu.VMEM((OWN, 64, 192), F32),
            pltpu.VMEM((16, 16 * (NBLK - 2)), F32),
            pltpu.VMEM((32, 16 * NBLK), F32),
            pltpu.VMEM(grid4, F32),
            pltpu.VMEM(grid4, F32),
            pltpu.VMEM(grid4, F32),
            pltpu.VMEM(grid4, BF16),
            pltpu.VMEM(grid4, F32),
            pltpu.VMEM((seqs, CHIP, 128), BF16),
            pltpu.VMEM((seqs, 2, 3, 128), F32),
            pltpu.VMEM((seqs, 3, 128), F32),
            pltpu.VMEM((seqs, TOK, channels), BF16),
            dma((7 + seqs,)),
            dma((seqs, 2)),
            dma((seqs, 12)),
            dma((seqs, 12)),
            dma((seqs, 16)),
            dma((seqs, 16)),
            dma((seqs,)),
            dma((seqs,)),
            dma((seqs,)),
        ],
        compiler_params=pltpu.CompilerParams(
            collective_id=0, has_side_effects=True, vmem_limit_bytes=62 * 1024 * 1024
        ),
    )(tokens, query_weight, key_weight, value_weight, out_gain.reshape(1, channels), out_weight)
    return pl.pallas_call(
        hand_over,
        out_shape=(jax.ShapeDtypeStruct(mixed.shape, BF16), jax.ShapeDtypeStruct(logs.shape, F32)),
        in_specs=[vmem, vmem],
        out_specs=(any_spec, any_spec),
        scratch_shapes=[dma((seqs + 1,))],
        compiler_params=pltpu.CompilerParams(vmem_limit_bytes=HAND_OVER),
    )(mixed, logs)


def solution(mesh):
    return jax.shard_map(
        functools.partial(shards, mesh.shape["sp"] // 2, mesh.shape["tp"]),
        mesh=mesh,
        in_specs=(
            P(None, "sp", None),
            P(None, "tp"),
            P(None, "tp"),
            P(None, "tp"),
            P(),
            P(None, "tp"),
        ),
        out_specs=(P(None, "sp", "tp"), P(None, "tp", "sp")),
        check_vma=False,
    )
```

```python
import functools
import math

import jax
import jax.numpy as jnp
from jax import lax
from jax.experimental import pallas as pl
from jax.experimental.pallas import tpu as pltpu
from jax.sharding import PartitionSpec as P

HEAD_DIM = 128
REACH = 64
ROPE_BASE = 10000.0
MASK_FILL = -1e30
NORM_FLOOR = 1e-6
LOG2E = 1.4426950408889634
SCALE = HEAD_DIM ** (-0.5)
RATE = SCALE * LOG2E

TOK = 384
CHIP = 2 * TOK
BLK = 256
WIDE = 1024
HALO = WIDE // BLK
OWN = CHIP // BLK
NBLK = 2 * HALO + OWN
ROWS = NBLK * BLK
HAND_OVER = 1024 * 1024
MESH = pl.DeviceIdType.MESH
F32 = jnp.float32
BF16 = jnp.bfloat16


def dot_nt(a, b):
    return lax.dot_general(a, b, (((1,), (1,)), ((), ())), preferred_element_type=F32)


def dot(a, b):
    return jnp.dot(a, b, preferred_element_type=F32)


def softened(scores):
    peak = jnp.max(scores, axis=-1, keepdims=True)
    probs = jnp.exp2((scores - peak) * RATE)
    return probs.astype(BF16), peak, jnp.sum(probs, axis=-1, keepdims=True)


def pipelined(jobs):
    ahead = jobs[0][0]()
    for i, (_, finish) in enumerate(jobs):
        now = ahead
        if i + 1 < len(jobs):
            ahead = jobs[i + 1][0]()
        finish(now)


def joined(parts):
    peak = functools.reduce(jnp.maximum, [part[1] for part in parts])
    merged, total = 0.0, 0.0
    for acc_g, peak_g, sum_g in parts:
        share = jnp.exp2((peak_g - peak) * RATE)
        merged = merged + share * acc_g
        total = total + share * sum_g
    return merged, peak, total


def iota(shape, dim):
    return lax.broadcasted_iota(jnp.int32, shape, dim)


def kernel(chips, tps, seqs, tokens, wq, wk, wv, gain_in, wo, out, logs,
           cos, sin, gain, tok_v, wq_v, wkv_v, wo_v, kvown, qown, kvbuf, qbuf, kvp, qp, perm,
           bias1, bias4, bias_mid, bias_out, acc1, peak1, sum1, mperm, lperm, mnat, lnat, lrx, mg,
           in_sem, loc_sem, kv_send, kv_recv, x_send, x_recv, l_send, l_recv, x_loc):
    sp, tp = lax.axis_index("sp"), lax.axis_index("tp")
    chip, core = sp // 2, sp % 2

    def token_load(s):
        return pltpu.make_async_copy(tokens.at[s], tok_v.at[s], in_sem.at[s])

    def pair_loads(h):
        lanes = pl.ds(h * HEAD_DIM, HEAD_DIM)
        return [pltpu.make_async_copy(w.at[:, lanes], wkv_v.at[h, :, pl.ds(i * HEAD_DIM, HEAD_DIM)],
                                      in_sem.at[seqs + 2 * h + i]) for i, w in enumerate((wk, wv))]

    query_load = pltpu.make_async_copy(wq, wq_v, in_sem.at[seqs + 4])
    last_loads = [pltpu.make_async_copy(wo, wo_v, in_sem.at[seqs + 5]),
                  pltpu.make_async_copy(gain_in, gain, in_sem.at[seqs + 6])]
    token_load(0).start()
    for load in pair_loads(0) + pair_loads(1):
        load.start()

    barrier = pltpu.get_barrier_semaphore()
    partners = [(2 * chip + 1 - core, tp)]
    for dx in range(1, tps):
        for c in range(2):
            partners.append((2 * chip + c, (tp + dx) % tps))
    has_left, has_right = chip > 0, chip < chips - 1
    has_far_left, has_far_right = chip > 1, chip < chips - 2
    after, before = jnp.minimum(chip + 1, chips - 1), jnp.maximum(chip - 1, 0)
    for partner in partners:
        pl.semaphore_signal(barrier, inc=1, device_id=partner, device_id_type=MESH)
    for has, neighbour in ((has_left, before), (has_right, after)):
        @pl.when(has)
        def _():
            for c in range(2):
                pl.semaphore_signal(barrier, inc=1, device_id=(2 * neighbour + c, tp), device_id_type=MESH)

    pair = iota((1, HEAD_DIM), 1) % (HEAD_DIM // 2)
    frequency = jnp.exp2(pair.astype(F32) * (-math.log2(ROPE_BASE) / (HEAD_DIM // 2)))
    angles = (sp * TOK + iota((TOK, HEAD_DIM), 0)).astype(F32) * frequency
    cos[...] = jnp.cos(angles)
    sine = jnp.sin(angles)
    sin[...] = jnp.where(iota((TOK, HEAD_DIM), 1) < HEAD_DIM // 2, -sine, sine)

    def row_of(at, size):
        return pl.ds(pl.multiple_of(at, 128), size)

    def remote(src, dst, send, recv, device):
        return pltpu.make_async_remote_copy(src_ref=src, dst_ref=dst, send_sem=send, recv_sem=recv,
                                            device_id=device, device_id_type=MESH)


    def near_sends(s, way):
        copies = []
        base, to = ((BLK, after), (WIDE + CHIP, before))[way]
        for piece, (src, at, size) in enumerate(((128 * core, 512 * core, BLK), (BLK * (1 - core), BLK + 128 * core, 128))):
            for h in range(2):
                copies.append(remote(kvown.at[s, h, row_of(src, size)], kvbuf.at[s, row_of(base + at, size)],
                                     kv_send.at[s, 4 * piece + 2 * h + way],
                                     kv_recv.at[s, 4 * way + 2 * piece + core], (2 * to + h, tp)))
        return copies

    def far_send(s, way):
        src, dst, to = ((WIDE - BLK, 0, after), (WIDE + CHIP, ROWS - BLK, before))[way]
        return remote(kvbuf.at[s, pl.ds(src, BLK)], kvbuf.at[s, pl.ds(dst, BLK)],
                      kv_send.at[s, 8 + way], kv_recv.at[s, 8 + way], (2 * to + core, tp))

    sends_to = (has_right, has_left)
    hears_from = (has_left, has_right)
    hears_far = (has_far_left, has_far_right)

    def start_near(s, which=slice(0, 4)):
        for way in range(2):
            @pl.when(sends_to[way])
            def _():
                for copy in near_sends(s, way)[which]:
                    copy.start()

    def own_sends(s):
        return [remote(kvown.at[s, 1 - core], kvbuf.at[s, row_of(WIDE + TOK * core, TOK)],
                       kv_send.at[s, 10], kv_recv.at[s, 10], (2 * chip + 1 - core, tp)),
                remote(qown.at[s, 1 - core], qbuf.at[s, row_of(TOK * core, TOK)],
                       kv_send.at[s, 11], kv_recv.at[s, 11], (2 * chip + 1 - core, tp))]

    def local_copies(s):
        return [pltpu.make_async_copy(kvown.at[s, core], kvbuf.at[s, row_of(WIDE + TOK * core, TOK)], loc_sem.at[s, 0]),
                pltpu.make_async_copy(qown.at[s, core], qbuf.at[s, row_of(TOK * core, TOK)], loc_sem.at[s, 1])]

    def near_arrival(s, way, piece, c):
        at, size = ((512 * c, BLK), (BLK + 128 * c, 128))[piece]
        at += (BLK, WIDE + CHIP)[way]
        return remote(kvown.at[s, 0, pl.ds(0, size)], kvbuf.at[s, pl.ds(at, size)], kv_send.at[s, 0],
                      kv_recv.at[s, 4 * way + 2 * piece + c], (2 * chip + 1 - core, tp))

    def own_arrivals(s):
        return [remote(kvown.at[s, 0], kvbuf.at[s, row_of(WIDE + TOK * (1 - core), TOK)], kv_send.at[s, 0],
                       kv_recv.at[s, 10], (2 * chip + 1 - core, tp)),
                remote(qown.at[s, 0], qbuf.at[s, row_of(TOK * (1 - core), TOK)], kv_send.at[s, 0],
                       kv_recv.at[s, 11], (2 * chip + 1 - core, tp))]

    head = 2 * tp + core

    def column_of(h):
        return pl.ds(pl.multiple_of(h * HEAD_DIM, HEAD_DIM), HEAD_DIM)

    def piece_of(piece, c):
        return ((BLK * (1 - c), 128), (128 * c, BLK))[piece]

    def x_sends(s, piece):
        copies = []
        for dx in [tps // 2] + [d for d in range(1, tps) if d != tps // 2]:
            for c in range(2) if tps > 1 else ():
                at, size = piece_of(piece, c)
                copies.append(remote(mnat.at[s, pl.ds(TOK * c + at, size)], mg.at[s, pl.ds(at, size), column_of(head)],
                                     x_send.at[s, 8 * piece + 2 * dx + c], x_recv.at[s, 8 * piece + head],
                                     (2 * chip + c, (tp + dx) % tps)))
        at, size = piece_of(piece, 1 - core)
        copies.append(remote(mnat.at[s, row_of(TOK * (1 - core) + at, size)], mg.at[s, row_of(at, size), column_of(head)],
                             x_send.at[s, 8 * piece], x_recv.at[s, 8 * piece + head], (2 * chip + 1 - core, tp)))
        return copies

    def log_send(s):
        return remote(lnat.at[s, 1 - core], lrx.at[s], l_send.at[s], l_recv.at[s], (2 * chip + 1 - core, tp))

    def x_local(s):
        return pltpu.make_async_copy(mnat.at[s, row_of(TOK * core, TOK)], mg.at[s, :, column_of(head)], x_loc.at[s])

    def x_arrivals(s, piece):
        waits = []
        at, size = piece_of(piece, core)
        for o in range(1, 2 * tps):
            other = (head + o) % (2 * tps)
            waits.append(remote(mnat.at[s, pl.ds(0, size)], mg.at[s, row_of(at, size), column_of(other)],
                                x_send.at[s, 0], x_recv.at[s, 8 * piece + other], (2 * chip + 1 - core, tp)))
        return waits

    def turned(x):
        return (x * cos[...] + pltpu.roll(x, HEAD_DIM // 2, 1) * sin[...]).astype(BF16)

    def project(s, _):
        token_load(s).wait()
        for h in range(2):
            @pl.when(s == 0)
            def _():
                for load in pair_loads(h):
                    load.wait()
                if h == 1:
                    for t in range(1, seqs):
                        token_load(t).start()
                    for load in last_loads:
                        load.start()
                else:
                    query_load.start()
            both = dot(tok_v[s], wkv_v[h])
            kvown[s, h, :, :HEAD_DIM] = turned(both[:, :HEAD_DIM])
            kvown[s, h, :, HEAD_DIM:] = both[:, HEAD_DIM:].astype(BF16)

            @pl.when(s == 0)
            def _():
                if h == 0:
                    pl.semaphore_wait(barrier, len(partners) + 2 * (jnp.where(has_left, 1, 0) + jnp.where(has_right, 1, 0)))
                    start_near(0, slice(0, 1))
                else:
                    start_near(0, slice(1, 4))
        own_sends(s)[0].start()
        local_copies(s)[0].start()

        @pl.when(s == 0)
        def _():
            query_load.wait()
        queries = dot(tok_v[s], wq_v[...])
        for h in range(2):
            qown[s, h] = turned(queries[:, h * HEAD_DIM:(h + 1) * HEAD_DIM])
        own_sends(s)[1].start()
        local_copies(s)[1].start()
        return 0

    lax.fori_loop(0, seqs, project, 0)
    for load in last_loads:
        load.wait()

    row, col = iota((BLK, BLK), 0), iota((BLK, BLK), 1)
    perm[...] = jnp.where(col == (row % 16) * 16 + row // 16, 1.0, 0.0).astype(BF16)
    first = chip * CHIP
    limit = chips * CHIP
    for b in range(OWN):
        row, col = iota((BLK, BLK + 2 * REACH), 0), iota((BLK, BLK + 2 * REACH), 1)
        gap = (row % 16) * 16 + row // 16 - (col - REACH)
        at = first + b * BLK - REACH + col
        good = (gap >= -REACH) & (gap <= REACH) & (at >= 0) & (at < limit)
        bias1[b] = jnp.where(good, 0.0, MASK_FILL)
        row, col = iota((64, 192), 0), iota((64, 192), 1)
        gap = (row % 16) * 4 + row // 16 - ((col // 64 - 1) * 64 + (col % 16) * 4 + (col % 64) // 16)
        at = first + (b + col // 64 - 1) * BLK
        good = (gap >= -REACH) & (gap <= REACH) & (at >= 0) & (at < limit)
        bias4[b] = jnp.where(good, 0.0, MASK_FILL)
    for ref, q_blocks, k_blocks in ((bias_mid, (1,), range(1, NBLK - 1)), (bias_out, (0, 2), range(NBLK))):
        dims = (16 * len(q_blocks), 16 * len(k_blocks))
        row, col = iota(dims, 0), iota(dims, 1)
        q_at = row % 16 + 16 * (q_blocks[0] + 2 * (row // 16))
        block = col // 16 + k_blocks[0] - HALO
        gap = q_at - (col % 16 + 16 * block)
        at = first + block * BLK
        good = (gap >= -REACH) & (gap <= REACH) & (at >= 0) & (at < limit)
        ref[...] = jnp.where(good, 0.0, MASK_FILL)

    def put_in_order(s, blocks):
        for b in blocks:
            kvp[b] = dot(perm[...], kvbuf[s, pl.ds(b * BLK, BLK), :]).astype(BF16).reshape(4, 4, 16, 2 * HEAD_DIM)

    def near(s):
        for b in range(OWN):
            block = dot(perm[...], qbuf[s, pl.ds(b * BLK, BLK), :]).astype(BF16)
            qp[b] = block.reshape(4, 4, 16, HEAD_DIM)
        put_in_order(s, range(1, NBLK - 1))
        jobs, done = [], {}

        def narrow(b, half):
            around = pl.ds(WIDE + b * BLK - REACH, BLK + 2 * REACH)

            def scores():
                queries = qp[b, 2 * half:2 * half + 2].reshape(128, HEAD_DIM)
                return dot_nt(queries, kvbuf[s, around, :HEAD_DIM]) + bias1[b, half * 128:(half + 1) * 128]

            def finish(scores):
                probs, peak, total = softened(scores)
                done[b, half] = dot(probs, kvbuf[s, around, HEAD_DIM:]), peak, total
            return scores, finish

        def middle(b):
            def scores():
                every = []
                for r in range(4):
                    keys = kvp[b + HALO - 1:b + HALO + 2, :, r, :, :HEAD_DIM].reshape(192, HEAD_DIM)
                    every.append(dot_nt(qp[b, :, r].reshape(64, HEAD_DIM), keys) + bias4[b])
                return every

            def finish(every):
                soft = [softened(scores) for scores in every]
                accs = []
                for r in range(4):
                    values = kvp[b + HALO - 1:b + HALO + 2, :, r, :, HEAD_DIM:].reshape(192, HEAD_DIM)
                    accs.append(dot(soft[r][0], values))
                for a in range(4):
                    for r in range(4):
                        at = (a % 2) * 64 + r * 16
                        one = tuple(x[at:at + 16] for x in done[b, a // 2])
                        two = tuple(x[a * 16:(a + 1) * 16] for x in (accs[r],) + soft[r][1:])
                        acc, peak, total = joined((one, two))
                        acc1[b, a, r] = acc
                        peak1[b, a, r] = jnp.broadcast_to(peak, (16, HEAD_DIM))
                        sum1[b, a, r] = jnp.broadcast_to(total, (16, HEAD_DIM))
            return scores, finish

        pipelined([narrow(1, 0), narrow(1, 1), middle(1)] + [wide(r, (1,), range(1, NBLK - 1), bias_mid) for r in range(4)])
        in_order(s, 1)
        for copy in x_sends(s, 0):
            copy.start()
        for b in (0, 2):
            jobs += [narrow(b, 0), narrow(b, 1), middle(b)]
        pipelined(jobs)

    def wide(r, q_blocks, k_blocks, bias):
        keys_in = slice(k_blocks[0], k_blocks[-1] + 1)

        def scores():
            every = []
            for a in range(4):
                keys = kvp[keys_in, a, r, :, :HEAD_DIM].reshape(16 * len(k_blocks), HEAD_DIM)
                queries = jnp.concatenate([qp[b, a, r] for b in q_blocks], axis=0)
                every.append(dot_nt(queries, keys) + bias[...])
            return every

        def finish(every):
            soft = [softened(scores) for scores in every]
            accs = []
            for a in range(4):
                values = kvp[keys_in, a, r, :, HEAD_DIM:].reshape(16 * len(k_blocks), HEAD_DIM)
                accs.append(dot(soft[a][0], values))
            for a in range(4):
                for i, b in enumerate(q_blocks):
                    one = (acc1[b, a, r], peak1[b, a, r], sum1[b, a, r])
                    two = tuple(x[i * 16:(i + 1) * 16] for x in (accs[a],) + soft[a][1:])
                    merged, peak, total = joined((one, two))
                    mperm[b, a, r] = (merged / total).astype(BF16)
                    lperm[b, a, r] = peak * SCALE + jnp.log(total)
        return scores, finish

    def in_order(s, b):
        mnat[s, pl.ds(b * BLK, BLK), :] = dot(perm[...], mperm[b].reshape(BLK, HEAD_DIM)).astype(BF16)

    def far(s):
        put_in_order(s, (0, NBLK - 1))
        pipelined([wide(r, (0, 2), range(NBLK), bias_out) for r in range(4)])
        for b in (0, 2):
            in_order(s, b)
        for copy in x_sends(s, 1):
            copy.start()
        x_local(s).start()
        for b in range(OWN):
            column = lperm[b].reshape(BLK, HEAD_DIM)
            for half in range(2):
                hit = perm[:, half * 128:(half + 1) * 128].astype(F32)
                line = jnp.sum(jnp.where(hit > 0.5, column, 0.0), axis=0, keepdims=True)
                piece = 2 * b + half
                lnat[s, piece // 3, piece % 3:piece % 3 + 1, :] = line
        log_send(s).start()

    def finish(s):
        x_local(s).wait()
        for piece in range(2):
            for copy in x_arrivals(s, piece):
                copy.wait_recv()
            at, size = piece_of(piece, core)
            rows = row_of(at, size)
            lifted = mg[s, rows, :].astype(F32)
            square = jnp.mean(lifted * lifted, axis=-1, keepdims=True)
            scaled = (lifted * gain[...]).astype(BF16)
            projected = dot(scaled, wo_v[...])
            out[s, rows, :] = (projected * lax.rsqrt(square + NORM_FLOOR)).astype(BF16)
        log_send(s).wait_recv()
        mine, theirs = lnat[s, core], lrx[s]
        upper = jnp.where(core == 0, mine, theirs)
        lower = jnp.where(core == 0, theirs, mine)
        for piece in range(3):
            lanes = pl.ds(piece * 128, 128)
            logs[s, 0:1, lanes] = upper[piece:piece + 1]
            logs[s, 1:2, lanes] = lower[piece:piece + 1]

    for has, at, size in ((has_left, BLK, CHIP), (has_far_left, 0, BLK),
                          (has_right, WIDE + CHIP, CHIP), (has_far_right, ROWS - BLK, BLK)):
        @pl.when(jnp.logical_not(has))
        def _():
            def clear(s, _):
                kvbuf[s, pl.ds(at, size), :] = jnp.zeros((size, 2 * HEAD_DIM), BF16)
                return 0
            lax.fori_loop(0, seqs, clear, 0)

    def stage(s, _):
        for way in range(2):
            @pl.when(hears_from[way])
            def _():
                near_arrival(s, way, 0, 1 - way).wait_recv()

            @pl.when(jnp.logical_and(hears_from[way], sends_to[way]))
            def _():
                far_send(s, way).start()

            @pl.when(jnp.logical_and(sends_to[way], s + 1 < seqs))
            def _():
                for copy in near_sends(s + 1, way):
                    copy.start()

        for copy in local_copies(s):
            copy.wait()
        for copy in own_arrivals(s):
            copy.wait_recv()
        for way in range(2):
            @pl.when(hears_from[way])
            def _():
                near_arrival(s, way, 0, way).wait_recv()
                for c in range(2):
                    near_arrival(s, way, 1, c).wait_recv()
        near(s)
        for way in range(2):
            @pl.when(hears_far[way])
            def _():
                far_send(s, way).wait_recv()
        far(s)

        @pl.when(s > 0)
        def _():
            finish(s - 1)
        return 0

    lax.fori_loop(0, seqs, stage, 0)
    finish(seqs - 1)

    def drain(s, _):
        for copy in own_sends(s):
            copy.wait_send()
        for way in range(2):
            @pl.when(sends_to[way])
            def _():
                for copy in near_sends(s, way):
                    copy.wait_send()

            @pl.when(jnp.logical_and(hears_from[way], sends_to[way]))
            def _():
                far_send(s, way).wait_send()
        for copy in x_sends(s, 0) + x_sends(s, 1):
            copy.wait_send()
        log_send(s).wait_send()
        return 0
    lax.fori_loop(0, seqs, drain, 0)


def hand_over(mixed, logs, out, out_logs, sem):
    seqs = mixed.shape[0]
    copies = [pltpu.make_async_copy(mixed.at[s], out.at[s], sem.at[s]) for s in range(seqs)]
    copies.append(pltpu.make_async_copy(logs, out_logs, sem.at[seqs]))
    for copy in copies:
        copy.start()
    for copy in copies:
        copy.wait()


def shards(chips, tps, tokens, query_weight, key_weight, value_weight, out_gain, out_weight):
    seqs, length, model_dim = tokens.shape
    channels, out_cols = out_weight.shape
    any_spec = pl.BlockSpec(memory_space=pl.ANY)
    vmem = pl.BlockSpec(memory_space=pltpu.VMEM)
    dma = pltpu.SemaphoreType.DMA
    grid4 = (OWN, 4, 4, 16, HEAD_DIM)
    mixed, logs = pl.pallas_call(
        functools.partial(kernel, chips, tps, seqs),
        out_shape=(pltpu.VMEM((seqs, length, out_cols), BF16),
                   pltpu.VMEM((seqs, 2, length), F32)),
        in_specs=[any_spec] * 6,
        out_specs=(vmem, vmem),
        scratch_shapes=[
            pltpu.VMEM((TOK, HEAD_DIM), F32),
            pltpu.VMEM((TOK, HEAD_DIM), F32),
            pltpu.VMEM((1, channels), F32),
            pltpu.VMEM((seqs, TOK, model_dim), BF16),
            pltpu.VMEM((model_dim, 256), BF16),
            pltpu.VMEM((2, model_dim, 256), BF16),
            pltpu.VMEM((channels, out_cols), BF16),
            pltpu.VMEM((seqs, 2, TOK, 256), BF16),
            pltpu.VMEM((seqs, 2, TOK, 128), BF16),
            pltpu.VMEM((seqs, ROWS, 256), BF16),
            pltpu.VMEM((seqs, CHIP, 128), BF16),
            pltpu.VMEM((NBLK, 4, 4, 16, 256), BF16),
            pltpu.VMEM(grid4, BF16),
            pltpu.VMEM((BLK, BLK), BF16),
            pltpu.VMEM((OWN, BLK, BLK + 2 * REACH), F32),
            pltpu.VMEM((OWN, 64, 192), F32),
            pltpu.VMEM((16, 16 * (NBLK - 2)), F32),
            pltpu.VMEM((32, 16 * NBLK), F32),
            pltpu.VMEM(grid4, F32),
            pltpu.VMEM(grid4, F32),
            pltpu.VMEM(grid4, F32),
            pltpu.VMEM(grid4, BF16),
            pltpu.VMEM(grid4, F32),
            pltpu.VMEM((seqs, CHIP, 128), BF16),
            pltpu.VMEM((seqs, 2, 3, 128), F32),
            pltpu.VMEM((seqs, 3, 128), F32),
            pltpu.VMEM((seqs, TOK, channels), BF16),
            dma((7 + seqs,)),
            dma((seqs, 2)),
            dma((seqs, 12)),
            dma((seqs, 12)),
            dma((seqs, 16)),
            dma((seqs, 16)),
            dma((seqs,)),
            dma((seqs,)),
            dma((seqs,)),
        ],
        compiler_params=pltpu.CompilerParams(
            collective_id=0, has_side_effects=True, vmem_limit_bytes=62 * 1024 * 1024
        ),
    )(tokens, query_weight, key_weight, value_weight, out_gain.reshape(1, channels), out_weight)
    return pl.pallas_call(
        hand_over,
        out_shape=(jax.ShapeDtypeStruct(mixed.shape, BF16), jax.ShapeDtypeStruct(logs.shape, F32)),
        in_specs=[vmem, vmem],
        out_specs=(any_spec, any_spec),
        scratch_shapes=[dma((seqs + 1,))],
        compiler_params=pltpu.CompilerParams(vmem_limit_bytes=HAND_OVER),
    )(mixed, logs)


def solution(mesh):
    return jax.shard_map(
        functools.partial(shards, mesh.shape["sp"] // 2, mesh.shape["tp"]),
        mesh=mesh,
        in_specs=(
            P(None, "sp", None),
            P(None, "tp"),
            P(None, "tp"),
            P(None, "tp"),
            P(),
            P(None, "tp"),
        ),
        out_specs=(P(None, "sp", "tp"), P(None, "tp", "sp")),
        check_vma=False,
    )
```

```python
import functools
import math

import jax
import jax.numpy as jnp
from jax import lax
from jax.experimental import pallas as pl
from jax.experimental.pallas import tpu as pltpu
from jax.sharding import PartitionSpec as P

HEAD_DIM = 128
REACH = 64
ROPE_BASE = 10000.0
MASK_FILL = -1e30
NORM_FLOOR = 1e-6
LOG2E = 1.4426950408889634
SCALE = HEAD_DIM ** (-0.5)
RATE = SCALE * LOG2E

TOK = 384
CHIP = 2 * TOK
BLK = 256
WIDE = 1024
HALO = WIDE // BLK
OWN = CHIP // BLK
NBLK = 2 * HALO + OWN
ROWS = NBLK * BLK
HAND_OVER = 1024 * 1024
MESH = pl.DeviceIdType.MESH
F32 = jnp.float32
BF16 = jnp.bfloat16


def dot_nt(a, b):
    return lax.dot_general(a, b, (((1,), (1,)), ((), ())), preferred_element_type=F32)


def dot(a, b):
    return jnp.dot(a, b, preferred_element_type=F32)


def softened(scores):
    peak = jnp.max(scores, axis=-1, keepdims=True)
    probs = jnp.exp2((scores - peak) * RATE)
    return probs.astype(BF16), peak, jnp.sum(probs, axis=-1, keepdims=True)


def pipelined(jobs):
    ahead = jobs[0][0]()
    for i, (_, finish) in enumerate(jobs):
        now = ahead
        if i + 1 < len(jobs):
            ahead = jobs[i + 1][0]()
        finish(now)


def joined(parts):
    peak = functools.reduce(jnp.maximum, [part[1] for part in parts])
    merged, total = 0.0, 0.0
    for acc_g, peak_g, sum_g in parts:
        share = jnp.exp2((peak_g - peak) * RATE)
        merged = merged + share * acc_g
        total = total + share * sum_g
    return merged, peak, total


def iota(shape, dim):
    return lax.broadcasted_iota(jnp.int32, shape, dim)


def kernel(chips, tps, seqs, tokens, wq, wk, wv, gain_in, wo, out, logs,
           cos, sin, gain, tok_v, wq_v, wkv_v, wo_v, kvown, qown, kvbuf, qbuf, kvp, qp, perm,
           bias1, bias4, bias_mid, bias_out, acc1, peak1, sum1, mperm, lperm, mnat, lnat, lrx, mg,
           in_sem, loc_sem, kv_send, kv_recv, x_send, x_recv, l_send, l_recv, x_loc):
    sp, tp = lax.axis_index("sp"), lax.axis_index("tp")
    chip, core = sp // 2, sp % 2

    def token_load(s):
        return pltpu.make_async_copy(tokens.at[s], tok_v.at[s], in_sem.at[s])

    def pair_loads(h):
        lanes = pl.ds(h * HEAD_DIM, HEAD_DIM)
        return [pltpu.make_async_copy(w.at[:, lanes], wkv_v.at[h, :, pl.ds(i * HEAD_DIM, HEAD_DIM)],
                                      in_sem.at[seqs + 2 * h + i]) for i, w in enumerate((wk, wv))]

    query_load = pltpu.make_async_copy(wq, wq_v, in_sem.at[seqs + 4])
    last_loads = [pltpu.make_async_copy(wo, wo_v, in_sem.at[seqs + 5]),
                  pltpu.make_async_copy(gain_in, gain, in_sem.at[seqs + 6])]
    token_load(0).start()
    for load in pair_loads(0) + pair_loads(1):
        load.start()

    barrier = pltpu.get_barrier_semaphore()
    partners = [(2 * chip + 1 - core, tp)]
    for dx in range(1, tps):
        for c in range(2):
            partners.append((2 * chip + c, (tp + dx) % tps))
    has_left, has_right = chip > 0, chip < chips - 1
    has_far_left, has_far_right = chip > 1, chip < chips - 2
    after, before = jnp.minimum(chip + 1, chips - 1), jnp.maximum(chip - 1, 0)
    for partner in partners:
        pl.semaphore_signal(barrier, inc=1, device_id=partner, device_id_type=MESH)
    for has, neighbour in ((has_left, before), (has_right, after)):
        @pl.when(has)
        def _():
            for c in range(2):
                pl.semaphore_signal(barrier, inc=1, device_id=(2 * neighbour + c, tp), device_id_type=MESH)

    pair = iota((1, HEAD_DIM), 1) % (HEAD_DIM // 2)
    frequency = jnp.exp2(pair.astype(F32) * (-math.log2(ROPE_BASE) / (HEAD_DIM // 2)))
    angles = (sp * TOK + iota((TOK, HEAD_DIM), 0)).astype(F32) * frequency
    cos[...] = jnp.cos(angles)
    sine = jnp.sin(angles)
    sin[...] = jnp.where(iota((TOK, HEAD_DIM), 1) < HEAD_DIM // 2, -sine, sine)

    def row_of(at, size):
        return pl.ds(pl.multiple_of(at, 128), size)

    def remote(src, dst, send, recv, device):
        return pltpu.make_async_remote_copy(src_ref=src, dst_ref=dst, send_sem=send, recv_sem=recv,
                                            device_id=device, device_id_type=MESH)


    def near_sends(s, way):
        copies = []
        base, to = ((BLK, after), (WIDE + CHIP, before))[way]
        for piece, (src, at, size) in enumerate(((128 * core, 512 * core, BLK), (BLK * (1 - core), BLK + 128 * core, 128))):
            for h in range(2):
                copies.append(remote(kvown.at[s, h, row_of(src, size)], kvbuf.at[s, row_of(base + at, size)],
                                     kv_send.at[s, 4 * piece + 2 * h + way],
                                     kv_recv.at[s, 4 * way + 2 * piece + core], (2 * to + h, tp)))
        return copies

    def far_send(s, way):
        src, dst, to = ((WIDE - BLK, 0, after), (WIDE + CHIP, ROWS - BLK, before))[way]
        return remote(kvbuf.at[s, pl.ds(src, BLK)], kvbuf.at[s, pl.ds(dst, BLK)],
                      kv_send.at[s, 8 + way], kv_recv.at[s, 8 + way], (2 * to + core, tp))

    sends_to = (has_right, has_left)
    hears_from = (has_left, has_right)
    hears_far = (has_far_left, has_far_right)

    def start_near(s, which=slice(0, 4)):
        for way in range(2):
            @pl.when(sends_to[way])
            def _():
                for copy in near_sends(s, way)[which]:
                    copy.start()

    def own_sends(s):
        return [remote(kvown.at[s, 1 - core], kvbuf.at[s, row_of(WIDE + TOK * core, TOK)],
                       kv_send.at[s, 10], kv_recv.at[s, 10], (2 * chip + 1 - core, tp)),
                remote(qown.at[s, 1 - core], qbuf.at[s, row_of(TOK * core, TOK)],
                       kv_send.at[s, 11], kv_recv.at[s, 11], (2 * chip + 1 - core, tp))]

    def local_copies(s):
        return [pltpu.make_async_copy(kvown.at[s, core], kvbuf.at[s, row_of(WIDE + TOK * core, TOK)], loc_sem.at[s, 0]),
                pltpu.make_async_copy(qown.at[s, core], qbuf.at[s, row_of(TOK * core, TOK)], loc_sem.at[s, 1])]

    def near_arrival(s, way, piece, c):
        at, size = ((512 * c, BLK), (BLK + 128 * c, 128))[piece]
        at += (BLK, WIDE + CHIP)[way]
        return remote(kvown.at[s, 0, pl.ds(0, size)], kvbuf.at[s, pl.ds(at, size)], kv_send.at[s, 0],
                      kv_recv.at[s, 4 * way + 2 * piece + c], (2 * chip + 1 - core, tp))

    def own_arrivals(s):
        return [remote(kvown.at[s, 0], kvbuf.at[s, row_of(WIDE + TOK * (1 - core), TOK)], kv_send.at[s, 0],
                       kv_recv.at[s, 10], (2 * chip + 1 - core, tp)),
                remote(qown.at[s, 0], qbuf.at[s, row_of(TOK * (1 - core), TOK)], kv_send.at[s, 0],
                       kv_recv.at[s, 11], (2 * chip + 1 - core, tp))]

    head = 2 * tp + core

    def column_of(h):
        return pl.ds(pl.multiple_of(h * HEAD_DIM, HEAD_DIM), HEAD_DIM)

    def piece_of(piece, c):
        return ((BLK * (1 - c), 128), (128 * c, BLK))[piece]

    def x_sends(s, piece):
        copies = []
        for dx in [tps // 2] + [d for d in range(1, tps) if d != tps // 2]:
            for c in range(2) if tps > 1 else ():
                at, size = piece_of(piece, c)
                copies.append(remote(mnat.at[s, pl.ds(TOK * c + at, size)], mg.at[s, pl.ds(at, size), column_of(head)],
                                     x_send.at[s, 8 * piece + 2 * dx + c], x_recv.at[s, 8 * piece + head],
                                     (2 * chip + c, (tp + dx) % tps)))
        at, size = piece_of(piece, 1 - core)
        copies.append(remote(mnat.at[s, row_of(TOK * (1 - core) + at, size)], mg.at[s, row_of(at, size), column_of(head)],
                             x_send.at[s, 8 * piece], x_recv.at[s, 8 * piece + head], (2 * chip + 1 - core, tp)))
        return copies

    def log_send(s):
        return remote(lnat.at[s, 1 - core], lrx.at[s], l_send.at[s], l_recv.at[s], (2 * chip + 1 - core, tp))

    def x_local(s):
        return pltpu.make_async_copy(mnat.at[s, row_of(TOK * core, TOK)], mg.at[s, :, column_of(head)], x_loc.at[s])

    def x_arrivals(s, piece):
        waits = []
        at, size = piece_of(piece, core)
        for o in range(1, 2 * tps):
            other = (head + o) % (2 * tps)
            waits.append(remote(mnat.at[s, pl.ds(0, size)], mg.at[s, row_of(at, size), column_of(other)],
                                x_send.at[s, 0], x_recv.at[s, 8 * piece + other], (2 * chip + 1 - core, tp)))
        return waits

    def turned(x):
        return (x * cos[...] + pltpu.roll(x, HEAD_DIM // 2, 1) * sin[...]).astype(BF16)

    def project(s, _):
        token_load(s).wait()
        for h in range(2):
            @pl.when(s == 0)
            def _():
                for load in pair_loads(h):
                    load.wait()
                if h == 1:
                    for t in range(1, seqs):
                        token_load(t).start()
                    for load in last_loads:
                        load.start()
                else:
                    query_load.start()
            both = dot(tok_v[s], wkv_v[h])
            kvown[s, h, :, :HEAD_DIM] = turned(both[:, :HEAD_DIM])
            kvown[s, h, :, HEAD_DIM:] = both[:, HEAD_DIM:].astype(BF16)

            @pl.when(s == 0)
            def _():
                if h == 0:
                    pl.semaphore_wait(barrier, len(partners) + 2 * (jnp.where(has_left, 1, 0) + jnp.where(has_right, 1, 0)))
                    start_near(0, slice(0, 1))
                else:
                    start_near(0, slice(1, 4))
        own_sends(s)[0].start()
        local_copies(s)[0].start()

        @pl.when(s == 0)
        def _():
            query_load.wait()
        queries = dot(tok_v[s], wq_v[...])
        for h in range(2):
            qown[s, h] = turned(queries[:, h * HEAD_DIM:(h + 1) * HEAD_DIM])
        own_sends(s)[1].start()
        local_copies(s)[1].start()
        return 0

    lax.fori_loop(0, seqs, project, 0)
    for load in last_loads:
        load.wait()

    row, col = iota((BLK, BLK), 0), iota((BLK, BLK), 1)
    perm[...] = jnp.where(col == (row % 16) * 16 + row // 16, 1.0, 0.0).astype(BF16)
    first = chip * CHIP
    limit = chips * CHIP
    for b in range(OWN):
        row, col = iota((BLK, BLK + 2 * REACH), 0), iota((BLK, BLK + 2 * REACH), 1)
        gap = (row % 16) * 16 + row // 16 - (col - REACH)
        at = first + b * BLK - REACH + col
        good = (gap >= -REACH) & (gap <= REACH) & (at >= 0) & (at < limit)
        bias1[b] = jnp.where(good, 0.0, MASK_FILL)
        row, col = iota((64, 192), 0), iota((64, 192), 1)
        gap = (row % 16) * 4 + row // 16 - ((col // 64 - 1) * 64 + (col % 16) * 4 + (col % 64) // 16)
        at = first + (b + col // 64 - 1) * BLK
        good = (gap >= -REACH) & (gap <= REACH) & (at >= 0) & (at < limit)
        bias4[b] = jnp.where(good, 0.0, MASK_FILL)
    for ref, q_blocks, k_blocks in ((bias_mid, (1,), range(1, NBLK - 1)), (bias_out.at[0], (0,), range(NBLK - 2)),
                                   (bias_out.at[1], (2,), range(2, NBLK))):
        dims = (16 * len(q_blocks), 16 * len(k_blocks))
        row, col = iota(dims, 0), iota(dims, 1)
        q_at = row % 16 + 16 * (q_blocks[0] + 2 * (row // 16))
        block = col // 16 + k_blocks[0] - HALO
        gap = q_at - (col % 16 + 16 * block)
        at = first + block * BLK
        good = (gap >= -REACH) & (gap <= REACH) & (at >= 0) & (at < limit)
        ref[...] = jnp.where(good, 0.0, MASK_FILL)

    def put_in_order(s, blocks):
        for b in blocks:
            kvp[b] = dot(perm[...], kvbuf[s, pl.ds(b * BLK, BLK), :]).astype(BF16).reshape(4, 4, 16, 2 * HEAD_DIM)

    def near(s):
        for b in range(OWN):
            block = dot(perm[...], qbuf[s, pl.ds(b * BLK, BLK), :]).astype(BF16)
            qp[b] = block.reshape(4, 4, 16, HEAD_DIM)
        put_in_order(s, range(1, NBLK - 1))
        jobs, done = [], {}

        def narrow(b, half):
            around = pl.ds(WIDE + b * BLK - REACH, BLK + 2 * REACH)

            def scores():
                queries = qp[b, 2 * half:2 * half + 2].reshape(128, HEAD_DIM)
                return dot_nt(queries, kvbuf[s, around, :HEAD_DIM]) + bias1[b, half * 128:(half + 1) * 128]

            def finish(scores):
                probs, peak, total = softened(scores)
                done[b, half] = dot(probs, kvbuf[s, around, HEAD_DIM:]), peak, total
            return scores, finish

        def middle(b):
            def scores():
                every = []
                for r in range(4):
                    keys = kvp[b + HALO - 1:b + HALO + 2, :, r, :, :HEAD_DIM].reshape(192, HEAD_DIM)
                    every.append(dot_nt(qp[b, :, r].reshape(64, HEAD_DIM), keys) + bias4[b])
                return every

            def finish(every):
                soft = [softened(scores) for scores in every]
                accs = []
                for r in range(4):
                    values = kvp[b + HALO - 1:b + HALO + 2, :, r, :, HEAD_DIM:].reshape(192, HEAD_DIM)
                    accs.append(dot(soft[r][0], values))
                for a in range(4):
                    for r in range(4):
                        at = (a % 2) * 64 + r * 16
                        one = tuple(x[at:at + 16] for x in done[b, a // 2])
                        two = tuple(x[a * 16:(a + 1) * 16] for x in (accs[r],) + soft[r][1:])
                        acc, peak, total = joined((one, two))
                        acc1[b, a, r] = acc
                        peak1[b, a, r] = jnp.broadcast_to(peak, (16, HEAD_DIM))
                        sum1[b, a, r] = jnp.broadcast_to(total, (16, HEAD_DIM))
            return scores, finish

        pipelined([narrow(1, 0), narrow(1, 1), middle(1)] + [wide(r, (1,), range(1, NBLK - 1), bias_mid) for r in range(4)])
        in_order(s, 1)
        for copy in x_sends(s, 0):
            copy.start()
        for b in (0, 2):
            jobs += [narrow(b, 0), narrow(b, 1), middle(b)]
        pipelined(jobs)

    def wide(r, q_blocks, k_blocks, bias):
        keys_in = slice(k_blocks[0], k_blocks[-1] + 1)

        def scores():
            every = []
            for a in range(4):
                keys = kvp[keys_in, a, r, :, :HEAD_DIM].reshape(16 * len(k_blocks), HEAD_DIM)
                queries = jnp.concatenate([qp[b, a, r] for b in q_blocks], axis=0)
                every.append(dot_nt(queries, keys) + bias[...])
            return every

        def finish(every):
            soft = [softened(scores) for scores in every]
            accs = []
            for a in range(4):
                values = kvp[keys_in, a, r, :, HEAD_DIM:].reshape(16 * len(k_blocks), HEAD_DIM)
                accs.append(dot(soft[a][0], values))
            for a in range(4):
                for i, b in enumerate(q_blocks):
                    one = (acc1[b, a, r], peak1[b, a, r], sum1[b, a, r])
                    two = tuple(x[i * 16:(i + 1) * 16] for x in (accs[a],) + soft[a][1:])
                    merged, peak, total = joined((one, two))
                    mperm[b, a, r] = (merged / total).astype(BF16)
                    lperm[b, a, r] = peak * SCALE + jnp.log(total)
        return scores, finish

    def in_order(s, b):
        mnat[s, pl.ds(b * BLK, BLK), :] = dot(perm[...], mperm[b].reshape(BLK, HEAD_DIM)).astype(BF16)

    def far(s):
        put_in_order(s, (0, NBLK - 1))
        sends = x_sends(s, 1)
        for half in range(2):
            b = 2 * half
            pipelined([wide(r, (b,), range(b, b + NBLK - 2), bias_out.at[half]) for r in range(4)])
            in_order(s, b)
            for copy in sends[half:-1:2]:
                copy.start()
        sends[-1].start()
        x_local(s).start()
        for b in range(OWN):
            column = lperm[b].reshape(BLK, HEAD_DIM)
            for half in range(2):
                hit = perm[:, half * 128:(half + 1) * 128].astype(F32)
                line = jnp.sum(jnp.where(hit > 0.5, column, 0.0), axis=0, keepdims=True)
                piece = 2 * b + half
                lnat[s, piece // 3, piece % 3:piece % 3 + 1, :] = line
        log_send(s).start()

    def finish(s):
        x_local(s).wait()
        for piece in range(2):
            for copy in x_arrivals(s, piece):
                copy.wait_recv()
            at, size = piece_of(piece, core)
            rows = row_of(at, size)
            lifted = mg[s, rows, :].astype(F32)
            square = jnp.mean(lifted * lifted, axis=-1, keepdims=True)
            scaled = (lifted * gain[...]).astype(BF16)
            projected = dot(scaled, wo_v[...])
            out[s, rows, :] = (projected * lax.rsqrt(square + NORM_FLOOR)).astype(BF16)
        log_send(s).wait_recv()
        mine, theirs = lnat[s, core], lrx[s]
        upper = jnp.where(core == 0, mine, theirs)
        lower = jnp.where(core == 0, theirs, mine)
        for piece in range(3):
            lanes = pl.ds(piece * 128, 128)
            logs[s, 0:1, lanes] = upper[piece:piece + 1]
            logs[s, 1:2, lanes] = lower[piece:piece + 1]

    for has, at, size in ((has_left, BLK, CHIP), (has_far_left, 0, BLK),
                          (has_right, WIDE + CHIP, CHIP), (has_far_right, ROWS - BLK, BLK)):
        @pl.when(jnp.logical_not(has))
        def _():
            def clear(s, _):
                kvbuf[s, pl.ds(at, size), :] = jnp.zeros((size, 2 * HEAD_DIM), BF16)
                return 0
            lax.fori_loop(0, seqs, clear, 0)

    def stage(s, _):
        for way in range(2):
            @pl.when(hears_from[way])
            def _():
                near_arrival(s, way, 0, 1 - way).wait_recv()

            @pl.when(jnp.logical_and(hears_from[way], sends_to[way]))
            def _():
                far_send(s, way).start()

            @pl.when(jnp.logical_and(sends_to[way], s + 1 < seqs))
            def _():
                for copy in near_sends(s + 1, way):
                    copy.start()

        for copy in local_copies(s):
            copy.wait()
        for copy in own_arrivals(s):
            copy.wait_recv()
        for way in range(2):
            @pl.when(hears_from[way])
            def _():
                near_arrival(s, way, 0, way).wait_recv()
                for c in range(2):
                    near_arrival(s, way, 1, c).wait_recv()
        near(s)
        for way in range(2):
            @pl.when(hears_far[way])
            def _():
                far_send(s, way).wait_recv()
        far(s)

        @pl.when(s > 0)
        def _():
            finish(s - 1)
        return 0

    lax.fori_loop(0, seqs, stage, 0)
    finish(seqs - 1)

    def drain(s, _):
        for copy in own_sends(s):
            copy.wait_send()
        for way in range(2):
            @pl.when(sends_to[way])
            def _():
                for copy in near_sends(s, way):
                    copy.wait_send()

            @pl.when(jnp.logical_and(hears_from[way], sends_to[way]))
            def _():
                far_send(s, way).wait_send()
        for copy in x_sends(s, 0) + x_sends(s, 1):
            copy.wait_send()
        log_send(s).wait_send()
        return 0
    lax.fori_loop(0, seqs, drain, 0)


def hand_over(mixed, logs, out, out_logs, sem):
    seqs = mixed.shape[0]
    copies = [pltpu.make_async_copy(mixed.at[s], out.at[s], sem.at[s]) for s in range(seqs)]
    copies.append(pltpu.make_async_copy(logs, out_logs, sem.at[seqs]))
    for copy in copies:
        copy.start()
    for copy in copies:
        copy.wait()


def shards(chips, tps, tokens, query_weight, key_weight, value_weight, out_gain, out_weight):
    seqs, length, model_dim = tokens.shape
    channels, out_cols = out_weight.shape
    any_spec = pl.BlockSpec(memory_space=pl.ANY)
    vmem = pl.BlockSpec(memory_space=pltpu.VMEM)
    dma = pltpu.SemaphoreType.DMA
    grid4 = (OWN, 4, 4, 16, HEAD_DIM)
    mixed, logs = pl.pallas_call(
        functools.partial(kernel, chips, tps, seqs),
        out_shape=(pltpu.VMEM((seqs, length, out_cols), BF16),
                   pltpu.VMEM((seqs, 2, length), F32)),
        in_specs=[any_spec] * 6,
        out_specs=(vmem, vmem),
        scratch_shapes=[
            pltpu.VMEM((TOK, HEAD_DIM), F32),
            pltpu.VMEM((TOK, HEAD_DIM), F32),
            pltpu.VMEM((1, channels), F32),
            pltpu.VMEM((seqs, TOK, model_dim), BF16),
            pltpu.VMEM((model_dim, 256), BF16),
            pltpu.VMEM((2, model_dim, 256), BF16),
            pltpu.VMEM((channels, out_cols), BF16),
            pltpu.VMEM((seqs, 2, TOK, 256), BF16),
            pltpu.VMEM((seqs, 2, TOK, 128), BF16),
            pltpu.VMEM((seqs, ROWS, 256), BF16),
            pltpu.VMEM((seqs, CHIP, 128), BF16),
            pltpu.VMEM((NBLK, 4, 4, 16, 256), BF16),
            pltpu.VMEM(grid4, BF16),
            pltpu.VMEM((BLK, BLK), BF16),
            pltpu.VMEM((OWN, BLK, BLK + 2 * REACH), F32),
            pltpu.VMEM((OWN, 64, 192), F32),
            pltpu.VMEM((16, 16 * (NBLK - 2)), F32),
            pltpu.VMEM((2, 16, 16 * (NBLK - 2)), F32),
            pltpu.VMEM(grid4, F32),
            pltpu.VMEM(grid4, F32),
            pltpu.VMEM(grid4, F32),
            pltpu.VMEM(grid4, BF16),
            pltpu.VMEM(grid4, F32),
            pltpu.VMEM((seqs, CHIP, 128), BF16),
            pltpu.VMEM((seqs, 2, 3, 128), F32),
            pltpu.VMEM((seqs, 3, 128), F32),
            pltpu.VMEM((seqs, TOK, channels), BF16),
            dma((7 + seqs,)),
            dma((seqs, 2)),
            dma((seqs, 12)),
            dma((seqs, 12)),
            dma((seqs, 16)),
            dma((seqs, 16)),
            dma((seqs,)),
            dma((seqs,)),
            dma((seqs,)),
        ],
        compiler_params=pltpu.CompilerParams(
            collective_id=0, has_side_effects=True, vmem_limit_bytes=62 * 1024 * 1024
        ),
    )(tokens, query_weight, key_weight, value_weight, out_gain.reshape(1, channels), out_weight)
    return pl.pallas_call(
        hand_over,
        out_shape=(jax.ShapeDtypeStruct(mixed.shape, BF16), jax.ShapeDtypeStruct(logs.shape, F32)),
        in_specs=[vmem, vmem],
        out_specs=(any_spec, any_spec),
        scratch_shapes=[dma((seqs + 1,))],
        compiler_params=pltpu.CompilerParams(vmem_limit_bytes=HAND_OVER),
    )(mixed, logs)


def solution(mesh):
    return jax.shard_map(
        functools.partial(shards, mesh.shape["sp"] // 2, mesh.shape["tp"]),
        mesh=mesh,
        in_specs=(
            P(None, "sp", None),
            P(None, "tp"),
            P(None, "tp"),
            P(None, "tp"),
            P(),
            P(None, "tp"),
        ),
        out_specs=(P(None, "sp", "tp"), P(None, "tp", "sp")),
        check_vma=False,
    )
```
